32 devices in a mesh: sp: 4 (over y, x), tp: 8 (over z, core).
Axes of the slice: x: 2, y: 2, z: 4, core: 2. Of those that a mesh axis runs over, the one named last changes fastest.
Arguments:
- queries: bfloat16 [3072, 16, 128], P('sp', 'tp'), may hold values from -240 to 240
- key_pairs: bfloat16 [3072, 16, 128], P('sp', 'tp'), may hold values from -11 to 11
- head_values: bfloat16 [3072, 16, 128], P('sp', 'tp'), may hold values from -6 to 6
- lambdas: float32 [16], P('tp'), may hold values from 0.3 to 0.8
- head_gain: float32 [128], replicated, may hold values from 0.1 to 1.9
- out_weight: bfloat16 [2048, 2048], replicated, may hold values from -0.125 to 0.125
- residual: bfloat16 [3072, 2048], P(('sp', 'tp')), may hold values from -6 to 6
- norm_gain: float32 [2048], replicated, may hold values from 0.1 to 1.9
- expert_ids: int32 [3072, 2], P(('sp', 'tp')), may hold values from 0 to 7, all different within a row; in each aligned block of 96 rows (0 to 95, 96 to 191, ...) at most 32 rows name the same one
- route_weights: float32 [3072, 2], P(('sp', 'tp')), may hold values from 0.2 to 1
- gate_weight: bfloat16 [8, 2048, 2048], P('sp', None, 'tp'), may hold values from -0.125 to 0.125
- up_weight: bfloat16 [8, 2048, 2048], P('sp', None, 'tp'), may hold values from -0.125 to 0.125
- down_weight: bfloat16 [8, 2048, 2048], P('sp', 'tp'), may hold values from -0.125 to 0.125
Outputs:
- merged: bfloat16 [3072, 2048], P(('sp', 'tp'))
The draws below stay inside these ranges and needn't reach their ends.
Inputs may be any that keep to these rules, and one draw needn't show every extreme that they name: `expert_ids`: within the rows of one device each expert is named at most 32 times, and exactly 32 times in some device.
All inputs are finite; a program needn't handle non-finite values.
Results may differ from the reference program's by a relative error of at most 0.019.
Values may be sent and summed in bfloat16 or wider, within the bound.
A program may use at most 128 MiB of HBM per device.

```python
import math
import jax
import jax.numpy as jnp
import numpy as np
from jax import lax

D = 2048
HEADS = 16
HD = 64
VD = 128
FF = 2048
TOPK = 2
LENGTH = 3072
ROWS = 96
EXPERTS = 8
CAP = 32
N_TP = 8


def base_field(key, salt_value):
    return jnp.clip(jax.random.normal(jax.random.fold_in(key, salt_value), (LENGTH, HEADS, 2 * HD), jnp.float32), -4.0, 4.0) * 1.3


def draw_key_pairs(key, part):
    drawn_field = base_field(key, 11)
    return drawn_field.astype(jnp.bfloat16)


def draw_queries(key, part):
    drawn_field = base_field(key, 12)
    return drawn_field.astype(jnp.bfloat16)


def block_levels(rng, dims, shards, smallest, largest):
    loudness = 1.0
    for dim, blocks in shards:
        draws = jax.random.uniform(jax.random.fold_in(jax.random.fold_in(rng, 6), dim), (blocks,), jnp.float32, smallest / len(shards), largest / len(shards))
        loudness = loudness * jnp.repeat(jnp.exp(draws), dims[dim] // blocks).reshape((-1,) + (1,) * (len(dims) - 1 - dim))
    return loudness


def shared_out(own_key, own, number, rows, amount, top, limit, lean):
    order = jax.random.permutation(own_key, amount)
    crowded, common = load_shares(amount, rows * top, limit, lean, True), load_shares(amount, rows * top, limit, lean, False)
    places = jnp.arange(amount)

    def named(sizes, rotation):
        used = int((sizes > 0).sum())
        fixed = max(1, used // 4)
        passed = fixed + (places - fixed + rotation * (used - fixed)) % max(1, amount - fixed)
        return jnp.zeros((amount,), jnp.int32).at[order[jnp.where(places < fixed, places, passed)]].set(jnp.asarray(sizes, jnp.int32))

    sizes = jnp.where(number % 4 == 0, named(crowded, number // 4), named(common, number - number // 4 - 1))
    mixed = jax.random.permutation(jax.random.fold_in(own, 3), amount)
    source_of, sink = mixed[0:amount // 2 * 2:2], mixed[1:amount // 2 * 2:2]
    room = jnp.minimum(sizes[source_of] - 1, limit - sizes[sink]) // 2
    room = jnp.where((source_of == order[0]) | (sink == order[0]) | (sizes[sink] == 0), 0, jnp.maximum(room, 0))
    passed = jax.random.randint(jax.random.fold_in(own, 4), (amount // 2,), 0, 1 << 20) % (room + 1)
    sizes = sizes.at[source_of].add(-passed).at[sink].add(passed)
    items = jnp.searchsorted(jnp.cumsum(sizes), jnp.arange(rows * top), side="right").astype(jnp.int32)
    table = items.reshape(top, rows).T
    table = table[jax.random.permutation(jax.random.fold_in(own, 1), rows)]
    rotation = jax.random.randint(jax.random.fold_in(own, 2), (rows, 1), 0, top)
    return jnp.take_along_axis(table, (jnp.arange(top)[None, :] + rotation) % top, axis=1)


def load_shares(count, total, limit, skew, full):
    portions = [(1 << 20) // math.isqrt(grade ** skew) + 1 for grade in range(1, count + 1)]
    largest = limit if full else min(limit, max(-(-total // count), total * portions[0] // sum(portions)))
    least = 1 if total - largest >= count - 1 else 0
    holding, surplus = [largest] + [least] * (count - 1), total - largest - least * (count - 1)
    while surplus > 0:
        free = [i for i in range(1, count) if holding[i] < largest] or [i for i in range(1, count) if holding[i] < limit]
        mass, budget = sum([portions[i] for i in free]), surplus
        for i in free:
            more = min(limit - holding[i], max(1, budget * portions[i] // mass), surplus)
            holding[i] = holding[i] + more
            surplus = surplus - more
    return np.array(holding)


def centred(own_key, extent, scale, most, cuts=(), kind=jnp.bfloat16):
    loudness = block_levels(own_key, extent, cuts, -0.22, 0.18) if cuts else 1.0
    values = jax.random.normal(own_key, extent, jnp.float32) * scale * loudness
    return jnp.minimum(jnp.maximum(values, -most), most).astype(kind)


def setup_inputs(seed: int = 0) -> dict:
    key_list = jax.random.split(jax.random.key(seed), 14)
    queries = draw_queries(jax.random.fold_in(key_list[13], 71), 0)
    key_pairs = draw_key_pairs(jax.random.fold_in(key_list[13], 71), 0)
    head_values = centred(key_list[2], (LENGTH, HEADS, VD), 1.0, 6.0, ((0, 4), (1, 8)))
    lambdas = jnp.clip(0.3 + 0.5 * jax.random.uniform(key_list[3], (HEADS,), jnp.float32) ** block_levels(key_list[3], (HEADS,), ((0, 8),), -0.2, 0.2), 0.3, 0.8)
    head_gain = jnp.clip(1.0 + 0.18 * jax.random.normal(key_list[4], (VD,), jnp.float32), 0.1, 1.9)
    out_weight = centred(key_list[5], (HEADS * VD, D), (HEADS * VD) ** -0.5, 0.125)
    residual = centred(key_list[6], (LENGTH, D), 1.0, 6.0, ((0, 32),))
    norm_gain = jnp.clip(1.0 + 0.18 * jax.random.normal(key_list[7], (D,), jnp.float32), 0.1, 1.9)
    expert_ids_keys = jax.random.split(jax.random.fold_in(key_list[8], 1), LENGTH // ROWS)
    expert_ids_turns = jax.random.permutation(jax.random.fold_in(key_list[8], 3), LENGTH // ROWS)
    expert_ids = jax.vmap(lambda own, number: shared_out(jax.random.fold_in(key_list[8], 2), own, number, ROWS, EXPERTS, TOPK, CAP, 1))(expert_ids_keys, expert_ids_turns).reshape((LENGTH, TOPK))
    route_weights = jnp.clip(0.2 + 0.8 * jax.random.uniform(key_list[9], (LENGTH, TOPK), jnp.float32) ** block_levels(key_list[9], (LENGTH, TOPK), ((0, 32),), -0.2, 0.2), 0.2, 1.0)
    gate_weight = centred(key_list[10], (EXPERTS, D, FF), D ** -0.5, 0.125, ((0, 4), (2, 8)))
    up_weight = centred(key_list[11], (EXPERTS, D, FF), D ** -0.5, 0.125, ((0, 4), (2, 8)))
    down_weight = centred(key_list[12], (EXPERTS, FF, D), FF ** -0.5, 0.125, ((0, 4), (1, 8)))
    return {"queries": queries, "key_pairs": key_pairs, "head_values": head_values, "lambdas": lambdas, "head_gain": head_gain, "out_weight": out_weight, "residual": residual, "norm_gain": norm_gain, "expert_ids": expert_ids, "route_weights": route_weights, "gate_weight": gate_weight, "up_weight": up_weight, "down_weight": down_weight}


def attend_head(query_rows, key_rows, value_rows, weight_two):
    block_rows = min(512, LENGTH)
    columns = jnp.arange(LENGTH, dtype=jnp.int32)

    def one_block(block_index):
        offset = block_index * block_rows
        query_block = lax.dynamic_slice_in_dim(query_rows, offset, block_rows, 0)
        positions = offset + jnp.arange(block_rows, dtype=jnp.int32)
        allowed = columns[None, :] <= positions[:, None]
        results = []
        for member in range(2):
            first_col = member * HD
            scores = jnp.dot(query_block[:, first_col:first_col + HD], key_rows[:, first_col:first_col + HD].T, preferred_element_type=jnp.float32) * HD ** (-0.5)
            scores = jnp.where(allowed, scores, -jnp.inf)
            highest = lax.optimization_barrier(jnp.max(scores, axis=1, keepdims=True))
            weights = jnp.exp(scores - highest)
            totals = lax.optimization_barrier(jnp.sum(weights, axis=1, keepdims=True))
            summed = jnp.dot(weights.astype(jnp.bfloat16), value_rows, preferred_element_type=jnp.float32)
            results.append(summed / totals)
        return results[0] - weight_two * results[1]
    blocks = lax.map(one_block, jnp.arange(LENGTH // block_rows, dtype=jnp.int32))
    return blocks.reshape(LENGTH, VD)

def reference(queries, key_pairs, head_values, lambdas, head_gain, out_weight, residual, norm_gain, expert_ids, route_weights, gate_weight, up_weight, down_weight):

    def one_head(packed):
        query_rows, key_rows, value_rows, weight_two = packed
        mixed = attend_head(query_rows, key_rows, value_rows, weight_two)
        row_scale = lax.rsqrt(lax.optimization_barrier(jnp.mean(mixed * mixed, axis=1, keepdims=True)) + 1e-06)
        return (mixed * row_scale * head_gain).astype(jnp.bfloat16)
    per_head = lax.map(one_head, (jnp.transpose(queries, (1, 0, 2)), jnp.transpose(key_pairs, (1, 0, 2)), jnp.transpose(head_values, (1, 0, 2)), lambdas))
    attended = jnp.transpose(per_head, (1, 0, 2)).reshape(LENGTH, HEADS * VD)
    projected = jnp.dot(attended, out_weight, preferred_element_type=jnp.float32)
    updated = (residual.astype(jnp.float32) + projected).astype(jnp.bfloat16)
    widened = updated.astype(jnp.float32)
    normed = (widened * lax.rsqrt(lax.optimization_barrier(jnp.mean(widened * widened, axis=1, keepdims=True)) + 1e-06) * norm_gain).astype(jnp.bfloat16)
    flat_ids = expert_ids.reshape(-1)
    flat_weights = route_weights.reshape(-1)
    owners = jnp.arange(LENGTH * TOPK, dtype=jnp.int32) // TOPK
    most_rows = LENGTH // ROWS * CAP
    slice_width = FF // N_TP

    def expert_step(gathered, expert):
        matches = flat_ids == expert
        chosen = jnp.nonzero(matches, size=most_rows, fill_value=0)[0].astype(jnp.int32)
        filled = (jnp.arange(most_rows, dtype=jnp.int32) < jnp.sum(matches.astype(jnp.int32))).astype(jnp.float32)
        targets = owners[chosen]
        inputs = normed[targets]
        gate_part = jnp.dot(inputs, gate_weight[expert], preferred_element_type=jnp.float32)
        up_part = jnp.dot(inputs, up_weight[expert], preferred_element_type=jnp.float32)
        inner_rows = (jax.nn.silu(gate_part) * up_part).astype(jnp.bfloat16)
        pieces = jnp.einsum('mtf,tfd->mtd', inner_rows.reshape(most_rows, N_TP, slice_width).astype(jnp.float32), down_weight[expert].reshape(N_TP, slice_width, D).astype(jnp.float32))
        pieces = lax.optimization_barrier(pieces.astype(jnp.bfloat16)).astype(jnp.float32)
        result = lax.optimization_barrier(lax.optimization_barrier(jnp.sum(pieces, axis=1)).astype(jnp.bfloat16)).astype(jnp.float32)
        scaled = result * (flat_weights[chosen] * filled)[:, None]
        return (gathered.at[targets].add(scaled), None)
    moe_sum, leftover = lax.scan(expert_step, jnp.zeros((LENGTH, D), jnp.float32), jnp.arange(EXPERTS, dtype=jnp.int32))
    return (updated.astype(jnp.float32) + moe_sum).astype(jnp.bfloat16)
```

```python
import functools
import math

import jax
import jax.numpy as jnp
from jax import lax
from jax.experimental import pallas as pl
from jax.experimental.pallas import tpu as pltpu
from jax.sharding import PartitionSpec as P

MESH = pl.DeviceIdType.MESH
LOG2E = 1.4426950408889634
CORES = 2
PLANE = 4
HEADS_HERE = 2
VMEM_BYTES = 67043328


def attend_kernel(
    n_sp,
    n_tp,
    scale,
    lam_ref,
    q_ref,
    kv_ref,
    gain_ref,
    meta_ref,
    base_ref,
    norm_ref,
    w_hbm,
    updated_ref,
    normed_ref,
    zmeta_ref,
    weight,
    gathered,
    kvbuf,
    acc,
    top,
    tot,
    att,
    kv_send,
    kv_recv,
    at_send,
    at_recv,
    me_send,
    me_recv,
    own_sem,
    w_sem,
):
    heads, tiles, wide, _ = q_ref.shape
    tile = wide // 2
    rows = base_ref.shape[0]
    n_z = n_tp // CORES
    c = lax.axis_index("sp")
    t = lax.axis_index("tp")
    load = pltpu.make_async_copy(w_hbm, weight, w_sem)
    load.start()
    barrier = pltpu.get_barrier_semaphore()
    for d in range(1, n_sp):
        pl.semaphore_signal(barrier, inc=1, device_id=((c + d) % n_sp, t), device_id_type=MESH)
    for d in range(1, n_tp):
        pl.semaphore_signal(barrier, inc=1, device_id=(c, (t + d) % n_tp), device_id_type=MESH)
    pl.semaphore_wait(barrier, n_sp + n_tp - 2)

    def kv_copy(d, h):
        return pltpu.make_async_remote_copy(
            src_ref=kv_ref.at[h],
            dst_ref=kvbuf.at[d - 1, h],
            send_sem=kv_send.at[d - 1, h],
            recv_sem=kv_recv.at[d - 1, h],
            device_id=((c + d) % n_sp, t),
            device_id_type=MESH,
        )

    def meta_copy(d):
        return pltpu.make_async_remote_copy(
            src_ref=meta_ref,
            dst_ref=zmeta_ref.at[d],
            send_sem=me_send.at[d],
            recv_sem=me_recv.at[d],
            device_id=(c, (t + CORES * d) % n_tp),
            device_id_type=MESH,
        )

    for d in range(1, n_sp):
        @pl.when(c + d < n_sp)
        def _():
            for h in range(heads):
                kv_copy(d, h).start()

    for d in range(1, n_z):
        meta_copy(d).start()
    zmeta_ref[0] = meta_ref[...]

    factor = scale * LOG2E

    def scores_of(h, i, keys):
        return (
            lax.dot_general(
                q_ref[h, i], keys, (((1,), (1,)), ((), ())), preferred_element_type=jnp.float32
            )
            * factor
        )

    for i in range(tiles):
        extent = (i + 1) * tile
        for h in range(heads):
            s = scores_of(h, i, kv_ref[h, 0, :extent])
            row = lax.rem(lax.broadcasted_iota(jnp.int32, (wide, extent), 0), tile) + i * tile
            col = lax.broadcasted_iota(jnp.int32, (wide, extent), 1)
            s = jnp.where(col <= row, s, -jnp.inf)
            high = jnp.max(s, axis=1, keepdims=True)
            p = jnp.exp2(s - high)
            top[h, i] = high
            tot[h, i] = jnp.sum(p, axis=1, keepdims=True)
            acc[h, i] = jnp.dot(
                p.astype(jnp.bfloat16), kv_ref[h, 1, :extent], preferred_element_type=jnp.float32
            )

    def span_step(step, carry):
        for h in range(heads):
            kv_copy(step, h).wait_recv()

        def tile_step(i, inner):
            for h in range(heads):
                s = scores_of(h, i, kvbuf[step - 1, h, 0])
                before = top[h, i]
                high = jnp.maximum(before, jnp.max(s, axis=1, keepdims=True))
                p = jnp.exp2(s - high)
                decay = jnp.exp2(before - high)
                top[h, i] = high
                tot[h, i] = tot[h, i] * decay + jnp.sum(p, axis=1, keepdims=True)
                acc[h, i] = acc[h, i] * decay + jnp.dot(
                    p.astype(jnp.bfloat16),
                    kvbuf[step - 1, h, 1],
                    preferred_element_type=jnp.float32,
                )
            return inner

        return lax.fori_loop(0, tiles, tile_step, carry)

    lax.fori_loop(1, c + 1, span_step, 0)

    for h in range(heads):
        width = acc.shape[3]
        for i in range(tiles):
            both = acc[h, i] / tot[h, i]
            mixed = both[:tile] - lam_ref[h] * both[tile:]
            mean = jnp.mean(mixed * mixed, axis=1, keepdims=True)
            normed = mixed * lax.rsqrt(mean + 1e-06) * gain_ref[...]
            att[i * tile : (i + 1) * tile, h * width : (h + 1) * width] = normed.astype(att.dtype)

    def att_copy(d):
        to = (t + d) % n_tp
        return pltpu.make_async_remote_copy(
            src_ref=att.at[pl.ds(pl.multiple_of(to * rows, rows), rows)],
            dst_ref=gathered.at[t],
            send_sem=at_send.at[d],
            recv_sem=at_recv.at[d],
            device_id=(c, to),
            device_id_type=MESH,
        )

    for d in range(1, n_tp):
        att_copy(d).start()
    own = pltpu.make_async_copy(
        att.at[pl.ds(pl.multiple_of(t * rows, rows), rows)], gathered.at[t], own_sem
    )
    own.start()
    own.wait()
    load.wait()
    span = att.shape[1]
    projected = jnp.zeros(base_ref.shape, jnp.float32)
    for d in range(n_tp):
        if d:
            att_copy(d).wait_recv()
        source = (t - d + n_tp) % n_tp
        projected = projected + jnp.dot(
            gathered[source],
            weight[pl.ds(pl.multiple_of(source * span, span), span), :],
            preferred_element_type=jnp.float32,
        )
    updated = (base_ref[...].astype(jnp.float32) + projected).astype(jnp.bfloat16)
    updated_ref[...] = updated
    widened = updated.astype(jnp.float32)
    mean = jnp.mean(widened * widened, axis=1, keepdims=True)
    normed_ref[...] = (widened * lax.rsqrt(mean + 1e-06) * norm_ref[...]).astype(jnp.bfloat16)
    for d in range(1, n_tp):
        att_copy(d).wait_send()
    for d in range(1, n_z):
        meta_copy(d).wait()
    for d in range(1, n_sp):
        @pl.when(c + d < n_sp)
        def _():
            for h in range(heads):
                kv_copy(d, h).wait_send()


def attend(queries, key_pairs, head_values, lambdas, head_gain, meta, residual, norm_gain, out_weight, n_sp, n_tp):
    tokens, heads, pair = queries.shape
    rows = residual.shape[0]
    width = head_values.shape[2]
    half = pair // 2
    tile = math.gcd(tokens, 256)
    tiles = tokens // tile
    first = (jnp.arange(pair) < half)[None, :]
    q = jnp.transpose(queries, (1, 0, 2)).reshape(heads, tiles, 1, tile, pair)
    sides = jnp.stack([first, ~first])
    q = jnp.where(sides, q, jnp.zeros((), q.dtype)).reshape(heads, tiles, 2 * tile, pair)
    kv = jnp.transpose(jnp.stack([key_pairs, head_values]), (2, 0, 1, 3))
    dma = pltpu.SemaphoreType.DMA
    vmem = pl.BlockSpec(memory_space=pltpu.VMEM)
    n_z = n_tp // CORES
    return pl.pallas_call(
        functools.partial(attend_kernel, n_sp, n_tp, half ** (-0.5)),
        out_shape=(
            jax.ShapeDtypeStruct(residual.shape, jnp.bfloat16),
            jax.ShapeDtypeStruct(residual.shape, jnp.bfloat16),
            jax.ShapeDtypeStruct((n_z,) + meta.shape, meta.dtype),
        ),
        in_specs=[pl.BlockSpec(memory_space=pltpu.SMEM)] + [vmem] * 6
        + [pl.BlockSpec(memory_space=pl.ANY)],
        out_specs=(vmem, vmem, vmem),
        scratch_shapes=[
            pltpu.VMEM(out_weight.shape, out_weight.dtype),
            pltpu.VMEM((n_tp, rows, heads * width), jnp.bfloat16),
            pltpu.VMEM((n_sp - 1,) + kv.shape, kv.dtype),
            pltpu.VMEM((heads, tiles, 2 * tile, width), jnp.float32),
            pltpu.VMEM((heads, tiles, 2 * tile, 1), jnp.float32),
            pltpu.VMEM((heads, tiles, 2 * tile, 1), jnp.float32),
            pltpu.VMEM((tokens, heads * width), jnp.bfloat16),
            dma((n_sp - 1, heads)),
            dma((n_sp - 1, heads)),
            dma((n_tp,)),
            dma((n_tp,)),
            dma((n_z,)),
            dma((n_z,)),
            dma,
            dma,
        ],
        compiler_params=pltpu.CompilerParams(
            collective_id=0, has_side_effects=True, vmem_limit_bytes=48 * 1024 * 1024
        ),
        name="attend",
    )(lambdas, q, kv, head_gain.reshape(1, -1), meta, residual, norm_gain.reshape(1, -1), out_weight)


def experts_kernel(
    n_sp,
    n_z,
    x_ref,
    meta_ref,
    base_ref,
    gate_hbm,
    up_hbm,
    down_hbm,
    out_ref,
    gate,
    up,
    down,
    zrows,
    pack,
    arrived,
    psend,
    own,
    precv,
    ret,
    zsend,
    zret,
    mine,
    w_sem,
    zs_send,
    zs_recv,
    ps_send,
    ps_recv,
    fw_send,
    fw_recv,
    pp_send,
    pp_recv,
    rt_send,
    rt_recv,
    zr_send,
    zr_recv,
):
    rows, model = x_ref.shape
    local, cap = pack.shape[2], pack.shape[3]
    slots = n_sp * local * cap
    c = lax.axis_index("sp")
    t = lax.axis_index("tp")
    n_tp = n_z * CORES
    core = t % CORES
    partner = (c, t + 1 - 2 * core)
    loads = [
        pltpu.make_async_copy(a, b, w_sem.at[i])
        for i, (a, b) in enumerate(((gate_hbm, gate), (up_hbm, up), (down_hbm, down)))
    ]
    for load in loads:
        load.start()

    def column(d):
        return ((c + d) % n_sp, t)

    def layer(d):
        return (c, (t + CORES * d) % n_tp)

    barrier = pltpu.get_barrier_semaphore()
    for d in range(1, n_sp):
        pl.semaphore_signal(barrier, inc=1, device_id=column(d), device_id_type=MESH)
    for d in range(1, n_z):
        pl.semaphore_signal(barrier, inc=1, device_id=layer(d), device_id_type=MESH)
    pl.semaphore_signal(barrier, inc=1, device_id=partner, device_id_type=MESH)
    pl.semaphore_wait(barrier, n_sp + n_z - 1)

    def remote(src, dst, send, recv, target):
        return pltpu.make_async_remote_copy(
            src_ref=src,
            dst_ref=dst,
            send_sem=send,
            recv_sem=recv,
            device_id=target,
            device_id_type=MESH,
        )

    def z_copy(d):
        return remote(x_ref, zrows.at[d - 1], zs_send.at[d], zs_recv.at[d], layer(d))

    def pack_copy(d, s):
        return remote(
            pack.at[s, d - 1], arrived.at[0, s, d], ps_send.at[d, s], ps_recv.at[d, s], column(d)
        )

    def share_copy(d, s):
        return remote(
            arrived.at[0, s, d], arrived.at[1, s, d], fw_send.at[d, s], fw_recv.at[d, s], partner
        )

    def pair_copy(s):
        return remote(psend.at[s], precv.at[s], pp_send.at[s], pp_recv.at[s], partner)

    def back_copy(d, s):
        return remote(
            own.at[s, d], ret.at[s, d], rt_send.at[d, s], rt_recv.at[d, s], column(n_sp - d)
        )

    def z_back(d):
        return remote(
            zsend.at[d], zret.at[d], zr_send.at[d], zr_recv.at[d], layer(n_z - d)
        )

    for d in range(1, n_z):
        z_copy(d).start()

    def route_hits(s, r):
        target = lax.broadcasted_iota(jnp.int32, (slots, rows), 0).astype(jnp.float32)
        return target == meta_ref[s, r : r + 1, :rows]

    def pack_rows(s):
        if s:
            z_copy(s).wait_recv()
        hits = route_hits(s, 0) | route_hits(s, 1)
        pick = jnp.where(hits, 1.0, 0.0).astype(jnp.bfloat16)
        source = x_ref[...] if s == 0 else zrows[s - 1]
        packed = (
            jnp.dot(pick, source, preferred_element_type=jnp.float32)
            .astype(jnp.bfloat16)
            .reshape(n_sp, local, cap, model)
        )
        for d in range(1, n_sp):
            pack[s, d - 1] = packed[d]
            pack_copy(d, s).start()
        arrived[0, s, 0] = packed[0]
        share_copy(0, s).start()

    def run_experts(s):
        for d in range(1, n_sp):
            pack_copy(d, s).wait_recv()
            share_copy(d, s).start()
        for d in range(n_sp):
            share_copy(d, s).wait_recv()

        def expert_step(e, carry):
            x = arrived[:, s, :, e].reshape(2 * n_sp * cap, model)
            gated = jnp.dot(x, gate[e], preferred_element_type=jnp.float32)
            lifted = jnp.dot(x, up[e], preferred_element_type=jnp.float32)
            inner = (gated / (1.0 + jnp.exp(-gated)) * lifted).astype(jnp.bfloat16)
            y = jnp.dot(inner, down[e], preferred_element_type=jnp.float32)
            y = y.astype(jnp.bfloat16).reshape(2, n_sp, cap, model)
            own[s, :, e] = y[0]
            psend[s, :, e] = y[1]
            return carry

        lax.fori_loop(0, local, expert_step, 0)
        pair_copy(s).start()

    def reduce_pair(s):
        pair_copy(s).wait_recv()
        for d in list(range(1, n_sp)) + [0]:
            total = own[s, d].astype(jnp.float32) + precv[s, d].astype(jnp.float32)
            total = total.astype(jnp.bfloat16)
            if d == 0:
                ret[s, 0] = total
            else:
                own[s, d] = total
                back_copy(d, s).start()

    def mix_rows(s):
        for d in range(1, n_sp):
            back_copy(d, s).wait_recv()
        mixing = jnp.where(route_hits(s, 0), meta_ref[s, 2:3, :rows], 0.0) + jnp.where(
            route_hits(s, 1), meta_ref[s, 3:4, :rows], 0.0
        )
        high = mixing.astype(jnp.bfloat16)
        low = (mixing - high.astype(jnp.float32)).astype(jnp.bfloat16)
        back = ret[s].reshape(slots, model)
        numbers = (((0,), (0,)), ((), ()))
        merged = lax.dot_general(
            high, back, numbers, preferred_element_type=jnp.float32
        ) + lax.dot_general(low, back, numbers, preferred_element_type=jnp.float32)
        if s:
            zsend[s] = merged.astype(jnp.bfloat16)
            z_back(s).start()
        else:
            mine[...] = merged

    pack_rows(0)
    for load in loads:
        load.wait()
    if n_z > 1:
        pack_rows(1)
    for s in range(n_z):
        run_experts(s)
        if s + 2 < n_z:
            pack_rows(s + 2)
        elif s + 2 - n_z < n_z - 2:
            mix_rows(s + 2 - n_z)
        reduce_pair(s)
    for s in range(max(0, n_z - 2), n_z):
        mix_rows(s)
    merged = mine[...]
    for s in range(1, n_z):
        z_back(s).wait_recv()
        merged = merged + zret[s].astype(jnp.float32)
    out_ref[...] = (base_ref[...].astype(jnp.float32) + merged).astype(jnp.bfloat16)

    for d in range(1, n_z):
        z_copy(d).wait_send()
        z_back(d).wait_send()
    for s in range(n_z):
        for d in range(n_sp):
            if d:
                pack_copy(d, s).wait_send()
                back_copy(d, s).wait_send()
            share_copy(d, s).wait_send()
        pair_copy(s).wait_send()


def experts(normed, zmeta, updated, gate_weight, up_weight, down_weight, n_sp, n_z, cap):
    rows, model = normed.shape
    local = gate_weight.shape[0]
    dma = pltpu.SemaphoreType.DMA
    vmem = pl.BlockSpec(memory_space=pltpu.VMEM)
    hbm = pl.BlockSpec(memory_space=pl.ANY)
    block = (local, cap, model)

    def buffer(*shape):
        return pltpu.VMEM(shape, jnp.bfloat16)

    return pl.pallas_call(
        functools.partial(experts_kernel, n_sp, n_z),
        out_shape=jax.ShapeDtypeStruct((rows, model), jnp.bfloat16),
        in_specs=[vmem] * 3 + [hbm] * 3,
        out_specs=vmem,
        scratch_shapes=[
            buffer(*gate_weight.shape),
            buffer(*up_weight.shape),
            buffer(*down_weight.shape),
            buffer(n_z - 1, rows, model),
            buffer(n_z, n_sp - 1, *block),
            buffer(2, n_z, n_sp, *block),
            buffer(n_z, n_sp, *block),
            buffer(n_z, n_sp, *block),
            buffer(n_z, n_sp, *block),
            buffer(n_z, n_sp, *block),
            buffer(n_z, rows, model),
            buffer(n_z, rows, model),
            pltpu.VMEM((rows, model), jnp.float32),
            dma((3,)),
            dma((n_z,)),
            dma((n_z,)),
            dma((n_sp, n_z)),
            dma((n_sp, n_z)),
            dma((n_sp, n_z)),
            dma((n_sp, n_z)),
            dma((n_z,)),
            dma((n_z,)),
            dma((n_sp, n_z)),
            dma((n_sp, n_z)),
            dma((n_z,)),
            dma((n_z,)),
        ],
        compiler_params=pltpu.CompilerParams(
            collective_id=1, has_side_effects=True, vmem_limit_bytes=VMEM_BYTES
        ),
        name="experts",
    )(normed, zmeta, updated, gate_weight, up_weight, down_weight)


def layer_kernel(
    n_sp,
    n_tp,
    scale,
    lam_ref,
    q_ref,
    kv_ref,
    gain_ref,
    meta_ref,
    base_ref,
    norm_ref,
    w_hbm,
    gate_hbm,
    up_hbm,
    down_hbm,
    out_ref,
    weight,
    gathered,
    kvbuf,
    acc,
    top,
    tot,
    att,
    updated,
    x_ref,
    zmeta,
    gate,
    up,
    down,
    zrows,
    pack,
    arrived,
    psend,
    own,
    precv,
    ret,
    zsend,
    zret,
    mine,
    kv_send,
    kv_recv,
    at_send,
    at_recv,
    me_send,
    me_recv,
    w_sem,
    zs_send,
    zs_recv,
    ps_send,
    ps_recv,
    fw_send,
    fw_recv,
    pp_send,
    pp_recv,
    rt_send,
    rt_recv,
    zr_send,
    zr_recv,
    go,
):
    heads, tiles, wide, _ = q_ref.shape
    tile = wide // 2
    rows, model = base_ref.shape
    width = kv_ref.shape[3]
    n_z = n_tp // CORES
    local, cap = pack.shape[2], pack.shape[3]
    slots = n_sp * local * cap
    c = lax.axis_index("sp")
    t = lax.axis_index("tp")
    core = t % CORES
    partner = (c, t + 1 - 2 * core)

    def column(d):
        return ((c + d) % n_sp, t)

    def layer(d):
        return (c, (t + CORES * d) % n_tp)

    loads = [
        pltpu.make_async_copy(a, b, w_sem.at[i])
        for i, (a, b) in enumerate(
            [(w_hbm.at[:, h], weight.at[h]) for h in range(heads)]
            + [(gate_hbm, gate), (up_hbm, up), (down_hbm, down)]
        )
    ]
    for load in loads:
        load.start()
    barrier = pltpu.get_barrier_semaphore()
    for d in range(1, n_sp):
        pl.semaphore_signal(barrier, inc=1, device_id=column(d), device_id_type=MESH)
    for d in range(1, n_tp):
        pl.semaphore_signal(barrier, inc=1, device_id=(c, (t + d) % n_tp), device_id_type=MESH)
    pl.semaphore_wait(barrier, n_sp + n_tp - 2)

    def remote(src, dst, send, recv, target):
        return pltpu.make_async_remote_copy(
            src_ref=src,
            dst_ref=dst,
            send_sem=send,
            recv_sem=recv,
            device_id=target,
            device_id_type=MESH,
        )

    def kv_copies(slot, source, h, to, mine_too, parts=(0, 1)):
        return [
            remote(
                kv_ref.at[h, part] if mine_too else kvbuf.at[source, h, part],
                kvbuf.at[source, h, part],
                kv_send.at[slot, part],
                kv_recv.at[source, h, part],
                (to, t),
            )
            for part in parts
        ]

    def kv_wait(source, h):
        for part in range(2):
            remote(
                kvbuf.at[source, h, part],
                kvbuf.at[source, h, part],
                kv_send.at[0, part],
                kv_recv.at[source, h, part],
                partner,
            ).wait_recv()

    first_sends = [
        kv_copies(0, 0, 0, 2, True)
        + kv_copies(1, 0, 1, 1, True)
        + kv_copies(2, 0, 1, 2, True)
        + kv_copies(3, 0, 0, 1, True),
        kv_copies(0, 1, 0, 3, True) + kv_copies(1, 1, 1, 0, True) + kv_copies(2, 1, 1, 3, True),
        kv_copies(0, 2, 0, 3, True) + kv_copies(1, 2, 1, 3, True, (0,)),
        [],
    ]
    relayed = [(1, 1), (0, 1), (0, 0), (1, 0)]
    late_sends = [
        kv_copies(4, 1, 1, 2, False),
        kv_copies(3, 0, 1, 3, False),
        kv_copies(2, 0, 0, 3, False) + kv_copies(1, 2, 1, 3, True, (1,)),
        kv_copies(0, 1, 0, 2, False),
    ]

    def meta_copy(d):
        return remote(meta_ref, zmeta.at[d], me_send.at[d], me_recv.at[d], layer(d))

    for k in range(n_sp):
        @pl.when(c == k)
        def _():
            for copy in first_sends[k]:
                copy.start()

    for d in range(1, n_z):
        meta_copy(d).start()
    zmeta[0] = meta_ref[...]

    factor = scale * LOG2E

    def scores_of(h, i, keys):
        return (
            lax.dot_general(
                q_ref[h, i], keys, (((1,), (1,)), ((), ())), preferred_element_type=jnp.float32
            )
            * factor
        )

    for i in range(tiles):
        extent = (i + 1) * tile
        for h in range(heads):
            s = scores_of(h, i, kv_ref[h, 0, :extent])
            row = lax.rem(lax.broadcasted_iota(jnp.int32, (wide, extent), 0), tile) + i * tile
            col = lax.broadcasted_iota(jnp.int32, (wide, extent), 1)
            s = jnp.where(col <= row, s, -jnp.inf)
            high = jnp.max(s, axis=1, keepdims=True)
            p = jnp.exp2(s - high)
            top[h, i] = high
            tot[h, i] = jnp.sum(p, axis=1, keepdims=True)
            acc[h, i] = jnp.dot(
                p.astype(jnp.bfloat16), kv_ref[h, 1, :extent], preferred_element_type=jnp.float32
            )

    for k in range(n_sp):
        @pl.when(c == k)
        def _():
            kv_wait(*relayed[k])
            for copy in late_sends[k]:
                copy.start()

    def order_of(orders):
        codes = [sum((2 * s + h) * 8**j for j, (s, h) in enumerate(o)) for o in orders]
        code, count = jnp.int32(codes[0]), jnp.int32(len(orders[0]))
        for k in range(1, n_sp):
            code = jnp.where(c == k, codes[k], code)
            count = jnp.where(c == k, len(orders[k]), count)
        return code, count

    def absorb(orders, waited):
        code, count = order_of(orders)

        def piece_step(j, code):
            piece = code % 8
            source, h = piece // 2, piece % 2

            @pl.when(j >= waited)
            def _():
                kv_wait(source, h)

            def tile_step(i, inner):
                s = scores_of(h, i, kvbuf[source, h, 0])
                before = top[h, i]
                high = jnp.maximum(before, jnp.max(s, axis=1, keepdims=True))
                p = jnp.exp2(s - high)
                decay = jnp.exp2(before - high)
                top[h, i] = high
                tot[h, i] = tot[h, i] * decay + jnp.sum(p, axis=1, keepdims=True)
                acc[h, i] = acc[h, i] * decay + jnp.dot(
                    p.astype(jnp.bfloat16),
                    kvbuf[source, h, 1],
                    preferred_element_type=jnp.float32,
                )
                return inner

            lax.fori_loop(0, tiles, tile_step, 0)
            return code // 8

        lax.fori_loop(0, count, piece_step, code)

    def att_copy(h, d):
        to = (t + d) % n_tp
        return remote(
            att.at[h, pl.ds(pl.multiple_of(to * rows, rows), rows)],
            gathered.at[h, :, pl.ds(pl.multiple_of(t * width, width), width)],
            at_send.at[h, d],
            at_recv.at[h, d],
            (c, to),
        )

    def finish(h):
        for i in range(tiles):
            both = acc[h, i] / tot[h, i]
            mixed = both[:tile] - lam_ref[h] * both[tile:]
            mean = jnp.mean(mixed * mixed, axis=1, keepdims=True)
            normed = mixed * lax.rsqrt(mean + 1e-06) * gain_ref[...]
            att[h, i * tile : (i + 1) * tile] = normed.astype(att.dtype)
        for d in range(1, n_tp):
            att_copy(h, d).start()
        gathered[h, :, pl.ds(pl.multiple_of(t * width, width), width)] = att[
            h, pl.ds(pl.multiple_of(t * rows, rows), rows)
        ]

    def project(h):
        loads[h].wait()
        for d in range(1, n_tp):
            att_copy(h, d).wait_recv()
        return jnp.dot(
            gathered[h],
            weight[h].reshape(n_tp * width, model),
            preferred_element_type=jnp.float32,
        )

    absorb([[], [(0, 1), (0, 0)], [(0, 0), (0, 1), (1, 0)], [(1, 0), (2, 0), (1, 1), (0, 0)]], 1)
    finish(0)
    absorb([[], [], [(1, 1)], [(2, 1), (0, 1)]], 0)

    @pl.when(c == n_sp - 1)
    def _():
        for d in range(1, n_sp):
            pl.semaphore_signal(go, inc=1, device_id=column(d), device_id_type=MESH)

    finish(1)
    mine[...] = project(0)
    new = (base_ref[...].astype(jnp.float32) + mine[...] + project(1)).astype(jnp.bfloat16)
    updated[...] = new
    widened = new.astype(jnp.float32)
    mean = jnp.mean(widened * widened, axis=1, keepdims=True)
    x_ref[...] = (widened * lax.rsqrt(mean + 1e-06) * norm_ref[...]).astype(jnp.bfloat16)

    def z_copy(d):
        return remote(x_ref, zrows.at[d - 1], zs_send.at[d], zs_recv.at[d], layer(d))

    def pack_copy(d, s):
        return remote(
            pack.at[s, d - 1], arrived.at[0, s, d], ps_send.at[d, s], ps_recv.at[d, s], column(d)
        )

    def share_copy(d, s):
        return remote(
            arrived.at[0, s, d], arrived.at[1, s, d], fw_send.at[d, s], fw_recv.at[d, s], partner
        )

    def pair_copy(s):
        return remote(psend.at[s], precv.at[s], pp_send.at[s], pp_recv.at[s], partner)

    def back_copy(d, s):
        return remote(
            own.at[s, d], ret.at[s, d], rt_send.at[d, s], rt_recv.at[d, s], column(n_sp - d)
        )

    def z_back(d):
        return remote(zsend.at[d], zret.at[d], zr_send.at[d], zr_recv.at[d], layer(n_z - d))

    for d in range(1, n_z):
        z_copy(d).start()
    for d in range(1, n_z):
        meta_copy(d).wait()

    def route_hits(s, r):
        target = lax.broadcasted_iota(jnp.int32, (slots, rows), 0).astype(jnp.float32)
        return target == zmeta[s, r : r + 1, :rows]

    def pack_rows(s):
        if s:
            z_copy(s).wait_recv()
        hits = route_hits(s, 0) | route_hits(s, 1)
        pick = jnp.where(hits, 1.0, 0.0).astype(jnp.bfloat16)
        source = x_ref[...] if s == 0 else zrows[s - 1]
        packed = (
            jnp.dot(pick, source, preferred_element_type=jnp.float32)
            .astype(jnp.bfloat16)
            .reshape(n_sp, local, cap, model)
        )
        for d in range(1, n_sp):
            pack[s, d - 1] = packed[d]
            pack_copy(d, s).start()
        arrived[0, s, 0] = packed[0]
        share_copy(0, s).start()

    def run_experts(s):
        for d in range(1, n_sp):
            pack_copy(d, s).wait_recv()
            share_copy(d, s).start()
        for d in range(n_sp):
            share_copy(d, s).wait_recv()

        def expert_step(e, carry):
            x = arrived[:, s, :, e].reshape(2 * n_sp * cap, model)
            gated = jnp.dot(x, gate[e], preferred_element_type=jnp.float32)
            lifted = jnp.dot(x, up[e], preferred_element_type=jnp.float32)
            inner = (gated / (1.0 + jnp.exp(-gated)) * lifted).astype(jnp.bfloat16)
            y = jnp.dot(inner, down[e], preferred_element_type=jnp.float32)
            y = y.astype(jnp.bfloat16).reshape(2, n_sp, cap, model)
            own[s, :, e] = y[0]
            psend[s, :, e] = y[1]
            return carry

        lax.fori_loop(0, local, expert_step, 0)
        pair_copy(s).start()

    def reduce_pair(s):
        pair_copy(s).wait_recv()
        for d in list(range(1, n_sp)) + [0]:
            total = own[s, d].astype(jnp.float32) + precv[s, d].astype(jnp.float32)
            total = total.astype(jnp.bfloat16)
            if d == 0:
                ret[s, 0] = total
            else:
                own[s, d] = total
                back_copy(d, s).start()

    def mix_rows(s):
        for d in range(1, n_sp):
            back_copy(d, s).wait_recv()
        mixing = jnp.where(route_hits(s, 0), zmeta[s, 2:3, :rows], 0.0) + jnp.where(
            route_hits(s, 1), zmeta[s, 3:4, :rows], 0.0
        )
        high = mixing.astype(jnp.bfloat16)
        low = (mixing - high.astype(jnp.float32)).astype(jnp.bfloat16)
        back = ret[s].reshape(slots, model)
        numbers = (((0,), (0,)), ((), ()))
        merged = lax.dot_general(
            high, back, numbers, preferred_element_type=jnp.float32
        ) + lax.dot_general(low, back, numbers, preferred_element_type=jnp.float32)
        if s:
            zsend[s] = merged.astype(jnp.bfloat16)
            z_back(s).start()
        return merged

    @pl.when(c != n_sp - 1)
    def _():
        pl.semaphore_wait(go, 1)

    pack_rows(0)
    for load in loads[heads:]:
        load.wait()
    for s in range(1, n_z):
        pack_rows(s)
        run_experts(s - 1)
        if s > 1:
            reduce_pair(s - 1)
    run_experts(n_z - 1)
    for s in range(1, n_z - 1):
        mix_rows(s)
    reduce_pair(n_z - 1)
    reduce_pair(0)
    mix_rows(n_z - 1)
    merged = updated[...].astype(jnp.float32)
    for s in range(1, n_z):
        z_back(s).wait_recv()
        merged = merged + zret[s].astype(jnp.float32)
    mine[...] = merged
    out_ref[...] = (mine[...] + mix_rows(0)).astype(jnp.bfloat16)

    for k in range(n_sp):
        @pl.when(c == k)
        def _():
            for copy in first_sends[k] + late_sends[k]:
                copy.wait_send()

    for d in range(1, n_tp):
        for h in range(heads):
            att_copy(h, d).wait_send()
    for d in range(1, n_z):
        z_copy(d).wait_send()
        z_back(d).wait_send()
    for s in range(n_z):
        for d in range(n_sp):
            if d:
                pack_copy(d, s).wait_send()
                back_copy(d, s).wait_send()
            share_copy(d, s).wait_send()
        pair_copy(s).wait_send()


def masked_queries(queries, tile):
    tokens, heads, pair = queries.shape
    tiles = tokens // tile
    first = (jnp.arange(pair) < pair // 2)[None, :]
    q = jnp.transpose(queries, (1, 0, 2)).reshape(heads, tiles, 1, tile, pair)
    sides = jnp.stack([first, ~first])
    return jnp.where(sides, q, jnp.zeros((), q.dtype)).reshape(heads, tiles, 2 * tile, pair)


def whole_layer(
    queries,
    key_pairs,
    head_values,
    lambdas,
    head_gain,
    meta,
    residual,
    norm_gain,
    out_weight,
    gate_weight,
    up_weight,
    down_weight,
    n_sp,
    n_tp,
    cap,
):
    tokens, heads, pair = queries.shape
    rows, model = residual.shape
    width = head_values.shape[2]
    local = gate_weight.shape[0]
    n_z = n_tp // CORES
    tile = math.gcd(tokens, 256)
    tiles = tokens // tile
    q = masked_queries(queries, tile)
    kv = jnp.transpose(jnp.stack([key_pairs, head_values]), (2, 0, 1, 3))
    dma = pltpu.SemaphoreType.DMA
    vmem = pl.BlockSpec(memory_space=pltpu.VMEM)
    hbm = pl.BlockSpec(memory_space=pl.ANY)
    block = (local, cap, model)

    def buffer(*shape):
        return pltpu.VMEM(shape, jnp.bfloat16)

    def single(*shape):
        return pltpu.VMEM(shape, jnp.float32)

    return pl.pallas_call(
        functools.partial(layer_kernel, n_sp, n_tp, (pair // 2) ** (-0.5)),
        out_shape=jax.ShapeDtypeStruct((rows, model), jnp.bfloat16),
        in_specs=[pl.BlockSpec(memory_space=pltpu.SMEM)] + [vmem] * 6 + [hbm] * 4,
        out_specs=vmem,
        scratch_shapes=[
            buffer(heads, n_tp, width, model),
            buffer(heads, rows, n_tp * width),
            buffer(n_sp - 1, *kv.shape),
            single(heads, tiles, 2 * tile, width),
            single(heads, tiles, 2 * tile, 1),
            single(heads, tiles, 2 * tile, 1),
            buffer(heads, tokens, width),
            buffer(rows, model),
            buffer(rows, model),
            single(n_z, *meta.shape),
            buffer(*gate_weight.shape),
            buffer(*up_weight.shape),
            buffer(*down_weight.shape),
            buffer(n_z - 1, rows, model),
            buffer(n_z, n_sp - 1, *block),
            buffer(2, n_z, n_sp, *block),
            buffer(n_z, n_sp, *block),
            buffer(n_z, n_sp, *block),
            buffer(n_z, n_sp, *block),
            buffer(n_z, n_sp, *block),
            buffer(n_z, rows, model),
            buffer(n_z, rows, model),
            single(rows, model),
            dma((n_sp + 1, 2)),
            dma((n_sp - 1, heads, 2)),
            dma((heads, n_tp)),
            dma((heads, n_tp)),
            dma((n_z,)),
            dma((n_z,)),
            dma((heads + 3,)),
            dma((n_z,)),
            dma((n_z,)),
            dma((n_sp, n_z)),
            dma((n_sp, n_z)),
            dma((n_sp, n_z)),
            dma((n_sp, n_z)),
            dma((n_z,)),
            dma((n_z,)),
            dma((n_sp, n_z)),
            dma((n_sp, n_z)),
            dma((n_z,)),
            dma((n_z,)),
            pltpu.SemaphoreType.REGULAR,
        ],
        compiler_params=pltpu.CompilerParams(
            collective_id=2, has_side_effects=True, vmem_limit_bytes=VMEM_BYTES
        ),
        name="layer",
    )(
        lambdas,
        q,
        kv,
        head_gain.reshape(1, -1),
        meta,
        residual,
        norm_gain.reshape(1, -1),
        out_weight.reshape(n_tp, heads, width, model),
        gate_weight,
        up_weight,
        down_weight,
    )


def shards(
    queries,
    key_pairs,
    head_values,
    lambdas,
    head_gain,
    out_weight,
    residual,
    norm_gain,
    expert_ids,
    route_weights,
    gate_weight,
    up_weight,
    down_weight,
):
    tokens_here, heads_here, pair_width = queries.shape
    value_width = head_values.shape[2]
    rows_here = residual.shape[0]
    sp_count = lax.axis_size("sp")
    tp_count = lax.axis_size("tp")
    z_count = tp_count // CORES
    route_count = expert_ids.shape[1]
    local_experts = gate_weight.shape[0]
    expert_count = local_experts * sp_count
    capacity = max(2, 4 * rows_here * route_count // (3 * expert_count))
    flat_ids = expert_ids.reshape(-1)
    indicator = (flat_ids[:, None] == jnp.arange(expert_count, dtype=jnp.int32)[None, :]).astype(
        jnp.int32
    )
    ranking = jnp.sum(jnp.cumsum(indicator, axis=0) * indicator, axis=1) - 1
    turned = (flat_ids - lax.axis_index("sp") * local_experts) % expert_count
    near_slots = (turned * capacity + ranking).reshape(rows_here, route_count)
    slots = flat_ids * capacity + ranking
    meta = jnp.concatenate([near_slots.astype(jnp.float32), route_weights], axis=1).T
    meta = jnp.pad(meta, ((0, 8 - 2 * route_count), (0, -rows_here % 128)), constant_values=-1.0)
    model_width = residual.shape[1]
    block_bytes = z_count * local_experts * capacity * model_width * 2
    if sp_count == PLANE and heads_here == HEADS_HERE and pair_width == value_width and (
        capacity % 16 == 0 and rows_here <= 128 and route_count == 2
        and (7 * sp_count - 1) * block_bytes <= 3 * VMEM_BYTES // 5
    ):
        return whole_layer(
            queries,
            key_pairs,
            head_values,
            lambdas,
            head_gain,
            meta,
            residual,
            norm_gain,
            out_weight,
            gate_weight,
            up_weight,
            down_weight,
            sp_count,
            tp_count,
            capacity,
        )
    updated, normed, zmeta = attend(
        queries,
        key_pairs,
        head_values,
        lambdas,
        head_gain,
        meta,
        residual,
        norm_gain,
        out_weight,
        sp_count,
        tp_count,
    )
    if capacity % 16 == 0 and rows_here <= 128 and route_count == 2 and (
        (7 * sp_count - 1) * block_bytes <= 3 * VMEM_BYTES // 5
    ):
        return experts(
            normed, zmeta, updated, gate_weight, up_weight, down_weight, sp_count, z_count, capacity
        )
    sources = jnp.arange(rows_here * route_count, dtype=jnp.int32) // route_count
    outgoing = (
        jnp.zeros((expert_count * capacity, model_width), jnp.bfloat16)
        .at[slots]
        .set(normed[sources])
    )
    arrived = lax.all_to_all(
        outgoing.reshape(sp_count, local_experts, capacity, model_width),
        "sp",
        split_axis=0,
        concat_axis=0,
        tiled=True,
    )
    piece_rows = lax.all_gather(arrived[None], "tp", axis=0, tiled=True)
    gate_part = jnp.einsum(
        "tsecd,edf->tsecf", piece_rows, gate_weight, preferred_element_type=jnp.float32
    )
    up_part = jnp.einsum(
        "tsecd,edf->tsecf", piece_rows, up_weight, preferred_element_type=jnp.float32
    )
    inner_rows = (jax.nn.silu(gate_part) * up_part).astype(jnp.bfloat16)
    partial_value = jnp.einsum(
        "tsecf,efd->tsecd", inner_rows, down_weight, preferred_element_type=jnp.float32
    )
    reduced = lax.psum_scatter(
        partial_value.astype(jnp.bfloat16), "tp", scatter_dimension=0, tiled=True
    )
    returned = lax.all_to_all(reduced[0], "sp", split_axis=0, concat_axis=0, tiled=True)
    picked = (
        returned.reshape(expert_count * capacity, model_width)[slots]
        .astype(jnp.float32)
        .reshape(rows_here, route_count, model_width)
    )
    moe_sum = jnp.sum(picked * route_weights[:, :, None], axis=1)
    return (updated.astype(jnp.float32) + moe_sum).astype(jnp.bfloat16)


def solution(mesh):
    placed = (
        P("sp", "tp", None),
        P("sp", "tp", None),
        P("sp", "tp", None),
        P("tp"),
        P(),
        P(),
        P(("sp", "tp"), None),
        P(),
        P(("sp", "tp"), None),
        P(("sp", "tp"), None),
        P("sp", None, "tp"),
        P("sp", None, "tp"),
        P("sp", "tp", None),
    )
    return jax.shard_map(
        shards, mesh=mesh, in_specs=placed, out_specs=P(("sp", "tp"), None), check_vma=False
    )
```

```python
import functools
import math

import jax
import jax.numpy as jnp
from jax import lax
from jax.experimental import pallas as pl
from jax.experimental.pallas import tpu as pltpu
from jax.sharding import PartitionSpec as P

MESH = pl.DeviceIdType.MESH
LOG2E = 1.4426950408889634
CORES = 2
PLANE = 4
HEADS_HERE = 2
LAYERS = 4
TWIN = 3
VMEM_BYTES = 67043328


def attend_kernel(
    n_sp,
    n_tp,
    scale,
    lam_ref,
    q_ref,
    kv_ref,
    gain_ref,
    meta_ref,
    base_ref,
    norm_ref,
    w_hbm,
    updated_ref,
    normed_ref,
    zmeta_ref,
    weight,
    gathered,
    kvbuf,
    acc,
    top,
    tot,
    att,
    kv_send,
    kv_recv,
    at_send,
    at_recv,
    me_send,
    me_recv,
    own_sem,
    w_sem,
):
    heads, tiles, wide, _ = q_ref.shape
    tile = wide // 2
    rows = base_ref.shape[0]
    n_z = n_tp // CORES
    c = lax.axis_index("sp")
    t = lax.axis_index("tp")
    load = pltpu.make_async_copy(w_hbm, weight, w_sem)
    load.start()
    barrier = pltpu.get_barrier_semaphore()
    for d in range(1, n_sp):
        pl.semaphore_signal(barrier, inc=1, device_id=((c + d) % n_sp, t), device_id_type=MESH)
    for d in range(1, n_tp):
        pl.semaphore_signal(barrier, inc=1, device_id=(c, (t + d) % n_tp), device_id_type=MESH)
    pl.semaphore_wait(barrier, n_sp + n_tp - 2)

    def kv_copy(d, h):
        return pltpu.make_async_remote_copy(
            src_ref=kv_ref.at[h],
            dst_ref=kvbuf.at[d - 1, h],
            send_sem=kv_send.at[d - 1, h],
            recv_sem=kv_recv.at[d - 1, h],
            device_id=((c + d) % n_sp, t),
            device_id_type=MESH,
        )

    def meta_copy(d):
        return pltpu.make_async_remote_copy(
            src_ref=meta_ref,
            dst_ref=zmeta_ref.at[d],
            send_sem=me_send.at[d],
            recv_sem=me_recv.at[d],
            device_id=(c, (t + CORES * d) % n_tp),
            device_id_type=MESH,
        )

    for d in range(1, n_sp):
        @pl.when(c + d < n_sp)
        def _():
            for h in range(heads):
                kv_copy(d, h).start()

    for d in range(1, n_z):
        meta_copy(d).start()
    zmeta_ref[0] = meta_ref[...]

    factor = scale * LOG2E

    def scores_of(h, i, keys):
        return (
            lax.dot_general(
                q_ref[h, i], keys, (((1,), (1,)), ((), ())), preferred_element_type=jnp.float32
            )
            * factor
        )

    for i in range(tiles):
        extent = (i + 1) * tile
        for h in range(heads):
            s = scores_of(h, i, kv_ref[h, 0, :extent])
            row = lax.rem(lax.broadcasted_iota(jnp.int32, (wide, extent), 0), tile) + i * tile
            col = lax.broadcasted_iota(jnp.int32, (wide, extent), 1)
            s = jnp.where(col <= row, s, -jnp.inf)
            high = jnp.max(s, axis=1, keepdims=True)
            p = jnp.exp2(s - high)
            top[h, i] = high
            tot[h, i] = jnp.sum(p, axis=1, keepdims=True)
            acc[h, i] = jnp.dot(
                p.astype(jnp.bfloat16), kv_ref[h, 1, :extent], preferred_element_type=jnp.float32
            )

    def span_step(step, carry):
        for h in range(heads):
            kv_copy(step, h).wait_recv()

        def tile_step(i, inner):
            for h in range(heads):
                s = scores_of(h, i, kvbuf[step - 1, h, 0])
                before = top[h, i]
                high = jnp.maximum(before, jnp.max(s, axis=1, keepdims=True))
                p = jnp.exp2(s - high)
                decay = jnp.exp2(before - high)
                top[h, i] = high
                tot[h, i] = tot[h, i] * decay + jnp.sum(p, axis=1, keepdims=True)
                acc[h, i] = acc[h, i] * decay + jnp.dot(
                    p.astype(jnp.bfloat16),
                    kvbuf[step - 1, h, 1],
                    preferred_element_type=jnp.float32,
                )
            return inner

        return lax.fori_loop(0, tiles, tile_step, carry)

    lax.fori_loop(1, c + 1, span_step, 0)

    for h in range(heads):
        width = acc.shape[3]
        for i in range(tiles):
            both = acc[h, i] / tot[h, i]
            mixed = both[:tile] - lam_ref[h] * both[tile:]
            mean = jnp.mean(mixed * mixed, axis=1, keepdims=True)
            normed = mixed * lax.rsqrt(mean + 1e-06) * gain_ref[...]
            att[i * tile : (i + 1) * tile, h * width : (h + 1) * width] = normed.astype(att.dtype)

    def att_copy(d):
        to = (t + d) % n_tp
        return pltpu.make_async_remote_copy(
            src_ref=att.at[pl.ds(pl.multiple_of(to * rows, rows), rows)],
            dst_ref=gathered.at[t],
            send_sem=at_send.at[d],
            recv_sem=at_recv.at[d],
            device_id=(c, to),
            device_id_type=MESH,
        )

    for d in range(1, n_tp):
        att_copy(d).start()
    own = pltpu.make_async_copy(
        att.at[pl.ds(pl.multiple_of(t * rows, rows), rows)], gathered.at[t], own_sem
    )
    own.start()
    own.wait()
    load.wait()
    span = att.shape[1]
    projected = jnp.zeros(base_ref.shape, jnp.float32)
    for d in range(n_tp):
        if d:
            att_copy(d).wait_recv()
        source = (t - d + n_tp) % n_tp
        projected = projected + jnp.dot(
            gathered[source],
            weight[pl.ds(pl.multiple_of(source * span, span), span), :],
            preferred_element_type=jnp.float32,
        )
    updated = (base_ref[...].astype(jnp.float32) + projected).astype(jnp.bfloat16)
    updated_ref[...] = updated
    widened = updated.astype(jnp.float32)
    mean = jnp.mean(widened * widened, axis=1, keepdims=True)
    normed_ref[...] = (widened * lax.rsqrt(mean + 1e-06) * norm_ref[...]).astype(jnp.bfloat16)
    for d in range(1, n_tp):
        att_copy(d).wait_send()
    for d in range(1, n_z):
        meta_copy(d).wait()
    for d in range(1, n_sp):
        @pl.when(c + d < n_sp)
        def _():
            for h in range(heads):
                kv_copy(d, h).wait_send()


def attend(queries, key_pairs, head_values, lambdas, head_gain, meta, residual, norm_gain, out_weight, n_sp, n_tp):
    tokens, heads, pair = queries.shape
    rows = residual.shape[0]
    width = head_values.shape[2]
    half = pair // 2
    tile = math.gcd(tokens, 256)
    tiles = tokens // tile
    first = (jnp.arange(pair) < half)[None, :]
    q = jnp.transpose(queries, (1, 0, 2)).reshape(heads, tiles, 1, tile, pair)
    sides = jnp.stack([first, ~first])
    q = jnp.where(sides, q, jnp.zeros((), q.dtype)).reshape(heads, tiles, 2 * tile, pair)
    kv = jnp.transpose(jnp.stack([key_pairs, head_values]), (2, 0, 1, 3))
    dma = pltpu.SemaphoreType.DMA
    vmem = pl.BlockSpec(memory_space=pltpu.VMEM)
    n_z = n_tp // CORES
    return pl.pallas_call(
        functools.partial(attend_kernel, n_sp, n_tp, half ** (-0.5)),
        out_shape=(
            jax.ShapeDtypeStruct(residual.shape, jnp.bfloat16),
            jax.ShapeDtypeStruct(residual.shape, jnp.bfloat16),
            jax.ShapeDtypeStruct((n_z,) + meta.shape, meta.dtype),
        ),
        in_specs=[pl.BlockSpec(memory_space=pltpu.SMEM)] + [vmem] * 6
        + [pl.BlockSpec(memory_space=pl.ANY)],
        out_specs=(vmem, vmem, vmem),
        scratch_shapes=[
            pltpu.VMEM(out_weight.shape, out_weight.dtype),
            pltpu.VMEM((n_tp, rows, heads * width), jnp.bfloat16),
            pltpu.VMEM((n_sp - 1,) + kv.shape, kv.dtype),
            pltpu.VMEM((heads, tiles, 2 * tile, width), jnp.float32),
            pltpu.VMEM((heads, tiles, 2 * tile, 1), jnp.float32),
            pltpu.VMEM((heads, tiles, 2 * tile, 1), jnp.float32),
            pltpu.VMEM((tokens, heads * width), jnp.bfloat16),
            dma((n_sp - 1, heads)),
            dma((n_sp - 1, heads)),
            dma((n_tp,)),
            dma((n_tp,)),
            dma((n_z,)),
            dma((n_z,)),
            dma,
            dma,
        ],
        compiler_params=pltpu.CompilerParams(
            collective_id=0, has_side_effects=True, vmem_limit_bytes=48 * 1024 * 1024
        ),
        name="attend",
    )(lambdas, q, kv, head_gain.reshape(1, -1), meta, residual, norm_gain.reshape(1, -1), out_weight)


def experts_kernel(
    n_sp,
    n_z,
    x_ref,
    meta_ref,
    base_ref,
    gate_hbm,
    up_hbm,
    down_hbm,
    out_ref,
    gate,
    up,
    down,
    zrows,
    pack,
    arrived,
    psend,
    own,
    precv,
    ret,
    zsend,
    zret,
    mine,
    w_sem,
    zs_send,
    zs_recv,
    ps_send,
    ps_recv,
    fw_send,
    fw_recv,
    pp_send,
    pp_recv,
    rt_send,
    rt_recv,
    zr_send,
    zr_recv,
):
    rows, model = x_ref.shape
    local, cap = pack.shape[2], pack.shape[3]
    slots = n_sp * local * cap
    c = lax.axis_index("sp")
    t = lax.axis_index("tp")
    n_tp = n_z * CORES
    core = t % CORES
    partner = (c, t + 1 - 2 * core)
    loads = [
        pltpu.make_async_copy(a, b, w_sem.at[i])
        for i, (a, b) in enumerate(((gate_hbm, gate), (up_hbm, up), (down_hbm, down)))
    ]
    for load in loads:
        load.start()

    def column(d):
        return ((c + d) % n_sp, t)

    def layer(d):
        return (c, (t + CORES * d) % n_tp)

    barrier = pltpu.get_barrier_semaphore()
    for d in range(1, n_sp):
        pl.semaphore_signal(barrier, inc=1, device_id=column(d), device_id_type=MESH)
    for d in range(1, n_z):
        pl.semaphore_signal(barrier, inc=1, device_id=layer(d), device_id_type=MESH)
    pl.semaphore_signal(barrier, inc=1, device_id=partner, device_id_type=MESH)
    pl.semaphore_wait(barrier, n_sp + n_z - 1)

    def remote(src, dst, send, recv, target):
        return pltpu.make_async_remote_copy(
            src_ref=src,
            dst_ref=dst,
            send_sem=send,
            recv_sem=recv,
            device_id=target,
            device_id_type=MESH,
        )

    def z_copy(d):
        return remote(x_ref, zrows.at[d - 1], zs_send.at[d], zs_recv.at[d], layer(d))

    def pack_copy(d, s):
        return remote(
            pack.at[s, d - 1], arrived.at[0, s, d], ps_send.at[d, s], ps_recv.at[d, s], column(d)
        )

    def share_copy(d, s):
        return remote(
            arrived.at[0, s, d], arrived.at[1, s, d], fw_send.at[d, s], fw_recv.at[d, s], partner
        )

    def pair_copy(s):
        return remote(psend.at[s], precv.at[s], pp_send.at[s], pp_recv.at[s], partner)

    def back_copy(d, s):
        return remote(
            own.at[s, d], ret.at[s, d], rt_send.at[d, s], rt_recv.at[d, s], column(n_sp - d)
        )

    def z_back(d):
        return remote(
            zsend.at[d], zret.at[d], zr_send.at[d], zr_recv.at[d], layer(n_z - d)
        )

    for d in range(1, n_z):
        z_copy(d).start()

    def route_hits(s, r):
        target = lax.broadcasted_iota(jnp.int32, (slots, rows), 0).astype(jnp.float32)
        return target == meta_ref[s, r : r + 1, :rows]

    def pack_rows(s):
        if s:
            z_copy(s).wait_recv()
        hits = route_hits(s, 0) | route_hits(s, 1)
        pick = jnp.where(hits, 1.0, 0.0).astype(jnp.bfloat16)
        source = x_ref[...] if s == 0 else zrows[s - 1]
        packed = (
            jnp.dot(pick, source, preferred_element_type=jnp.float32)
            .astype(jnp.bfloat16)
            .reshape(n_sp, local, cap, model)
        )
        for d in range(1, n_sp):
            pack[s, d - 1] = packed[d]
            pack_copy(d, s).start()
        arrived[0, s, 0] = packed[0]
        share_copy(0, s).start()

    def run_experts(s):
        for d in range(1, n_sp):
            pack_copy(d, s).wait_recv()
            share_copy(d, s).start()
        for d in range(n_sp):
            share_copy(d, s).wait_recv()

        def expert_step(e, carry):
            x = arrived[:, s, :, e].reshape(2 * n_sp * cap, model)
            gated = jnp.dot(x, gate[e], preferred_element_type=jnp.float32)
            lifted = jnp.dot(x, up[e], preferred_element_type=jnp.float32)
            inner = (gated / (1.0 + jnp.exp(-gated)) * lifted).astype(jnp.bfloat16)
            y = jnp.dot(inner, down[e], preferred_element_type=jnp.float32)
            y = y.astype(jnp.bfloat16).reshape(2, n_sp, cap, model)
            own[s, :, e] = y[0]
            psend[s, :, e] = y[1]
            return carry

        lax.fori_loop(0, local, expert_step, 0)
        pair_copy(s).start()

    def reduce_pair(s):
        pair_copy(s).wait_recv()
        for d in list(range(1, n_sp)) + [0]:
            total = own[s, d].astype(jnp.float32) + precv[s, d].astype(jnp.float32)
            total = total.astype(jnp.bfloat16)
            if d == 0:
                ret[s, 0] = total
            else:
                own[s, d] = total
                back_copy(d, s).start()

    def mix_rows(s):
        for d in range(1, n_sp):
            back_copy(d, s).wait_recv()
        mixing = jnp.where(route_hits(s, 0), meta_ref[s, 2:3, :rows], 0.0) + jnp.where(
            route_hits(s, 1), meta_ref[s, 3:4, :rows], 0.0
        )
        high = mixing.astype(jnp.bfloat16)
        low = (mixing - high.astype(jnp.float32)).astype(jnp.bfloat16)
        back = ret[s].reshape(slots, model)
        numbers = (((0,), (0,)), ((), ()))
        merged = lax.dot_general(
            high, back, numbers, preferred_element_type=jnp.float32
        ) + lax.dot_general(low, back, numbers, preferred_element_type=jnp.float32)
        if s:
            zsend[s] = merged.astype(jnp.bfloat16)
            z_back(s).start()
        else:
            mine[...] = merged

    pack_rows(0)
    for load in loads:
        load.wait()
    if n_z > 1:
        pack_rows(1)
    for s in range(n_z):
        run_experts(s)
        if s + 2 < n_z:
            pack_rows(s + 2)
        elif s + 2 - n_z < n_z - 2:
            mix_rows(s + 2 - n_z)
        reduce_pair(s)
    for s in range(max(0, n_z - 2), n_z):
        mix_rows(s)
    merged = mine[...]
    for s in range(1, n_z):
        z_back(s).wait_recv()
        merged = merged + zret[s].astype(jnp.float32)
    out_ref[...] = (base_ref[...].astype(jnp.float32) + merged).astype(jnp.bfloat16)

    for d in range(1, n_z):
        z_copy(d).wait_send()
        z_back(d).wait_send()
    for s in range(n_z):
        for d in range(n_sp):
            if d:
                pack_copy(d, s).wait_send()
                back_copy(d, s).wait_send()
            share_copy(d, s).wait_send()
        pair_copy(s).wait_send()


def experts(normed, zmeta, updated, gate_weight, up_weight, down_weight, n_sp, n_z, cap):
    rows, model = normed.shape
    local = gate_weight.shape[0]
    dma = pltpu.SemaphoreType.DMA
    vmem = pl.BlockSpec(memory_space=pltpu.VMEM)
    hbm = pl.BlockSpec(memory_space=pl.ANY)
    block = (local, cap, model)

    def buffer(*shape):
        return pltpu.VMEM(shape, jnp.bfloat16)

    return pl.pallas_call(
        functools.partial(experts_kernel, n_sp, n_z),
        out_shape=jax.ShapeDtypeStruct((rows, model), jnp.bfloat16),
        in_specs=[vmem] * 3 + [hbm] * 3,
        out_specs=vmem,
        scratch_shapes=[
            buffer(*gate_weight.shape),
            buffer(*up_weight.shape),
            buffer(*down_weight.shape),
            buffer(n_z - 1, rows, model),
            buffer(n_z, n_sp - 1, *block),
            buffer(2, n_z, n_sp, *block),
            buffer(n_z, n_sp, *block),
            buffer(n_z, n_sp, *block),
            buffer(n_z, n_sp, *block),
            buffer(n_z, n_sp, *block),
            buffer(n_z, rows, model),
            buffer(n_z, rows, model),
            pltpu.VMEM((rows, model), jnp.float32),
            dma((3,)),
            dma((n_z,)),
            dma((n_z,)),
            dma((n_sp, n_z)),
            dma((n_sp, n_z)),
            dma((n_sp, n_z)),
            dma((n_sp, n_z)),
            dma((n_z,)),
            dma((n_z,)),
            dma((n_sp, n_z)),
            dma((n_sp, n_z)),
            dma((n_z,)),
            dma((n_z,)),
        ],
        compiler_params=pltpu.CompilerParams(
            collective_id=1, has_side_effects=True, vmem_limit_bytes=VMEM_BYTES
        ),
        name="experts",
    )(normed, zmeta, updated, gate_weight, up_weight, down_weight)


def layer_kernel(
    n_sp,
    n_tp,
    scale,
    lam_ref,
    q_ref,
    kv_ref,
    gain_ref,
    meta_ref,
    base_ref,
    norm_ref,
    w_hbm,
    gate_hbm,
    up_hbm,
    down_hbm,
    out_ref,
    gathered,
    kvbuf,
    acc,
    top,
    tot,
    att,
    updated,
    x_ref,
    zmeta,
    gate,
    up,
    down,
    zrows,
    pack,
    arrived,
    psend,
    own,
    precv,
    ret,
    zsend,
    zret,
    fold,
    mine,
    kv_send,
    kv_recv,
    at_send,
    at_recv,
    me_send,
    me_recv,
    w_sem,
    zs_send,
    zs_recv,
    ps_send,
    ps_recv,
    fw_send,
    fw_recv,
    pp_send,
    pp_recv,
    rt_send,
    rt_recv,
    zr_send,
    zr_recv,
    tw_send,
    tw_recv,
    fo_send,
    fo_recv,
    go,
):
    heads, tiles, wide, _ = q_ref.shape
    tile = wide // 2
    rows, model = base_ref.shape
    width = kv_ref.shape[3]
    n_z = n_tp // CORES
    local, cap = pack.shape[2], pack.shape[3]
    slots = n_sp * local * cap
    span = n_sp * local * cap
    c = lax.axis_index("sp")
    t = lax.axis_index("tp")
    core = t % CORES
    partner = (c, t + 1 - 2 * core)

    def column(d):
        return ((c + d) % n_sp, t)

    z = t // CORES
    twin_z = z + 1 - 2 * (z % 2)
    far_z = (z + n_z // 2) % n_z
    twin = (c, twin_z * CORES + core)
    far = [None, (c, far_z * CORES + core), (c, (far_z + 1 - 2 * (far_z % 2)) * CORES + core)]

    weight = (psend, precv)
    loads = [
        pltpu.make_async_copy(a, b, w_sem.at[i])
        for i, (a, b) in enumerate(
            [
                (w_hbm.at[source, h], weight[h].at[source * width : (source + 1) * width])
                for h in range(heads)
                for source in range(n_tp)
            ]
            + [(gate_hbm, gate), (up_hbm, up), (down_hbm, down)]
        )
    ]
    for load in loads:
        load.start()
    barrier = pltpu.get_barrier_semaphore()
    for d in range(1, n_sp):
        pl.semaphore_signal(barrier, inc=1, device_id=column(d), device_id_type=MESH)
    for d in range(1, n_tp):
        pl.semaphore_signal(barrier, inc=1, device_id=(c, (t + d) % n_tp), device_id_type=MESH)
    pl.semaphore_wait(barrier, n_sp + n_tp - 2)

    def remote(src, dst, send, recv, target):
        return pltpu.make_async_remote_copy(
            src_ref=src,
            dst_ref=dst,
            send_sem=send,
            recv_sem=recv,
            device_id=target,
            device_id_type=MESH,
        )

    def kv_copies(slot, source, h, to, mine_too, parts=(0, 1)):
        return [
            remote(
                kv_ref.at[h, part] if mine_too else kvbuf.at[source, h, part],
                kvbuf.at[source, h, part],
                kv_send.at[slot, part],
                kv_recv.at[source, h, part],
                (to, t),
            )
            for part in parts
        ]

    def kv_wait(source, h):
        for part in range(2):
            remote(
                kvbuf.at[source, h, part],
                kvbuf.at[source, h, part],
                kv_send.at[0, part],
                kv_recv.at[source, h, part],
                partner,
            ).wait_recv()

    first_sends = [
        kv_copies(0, 0, 0, 2, True)
        + kv_copies(1, 0, 1, 1, True)
        + kv_copies(2, 0, 1, 2, True)
        + kv_copies(3, 0, 0, 1, True),
        kv_copies(0, 1, 0, 3, True) + kv_copies(1, 1, 1, 0, True) + kv_copies(2, 1, 1, 3, True),
        kv_copies(0, 2, 0, 3, True) + kv_copies(1, 2, 1, 3, True, (0,)),
        [],
    ]
    relayed = [(1, 1), (0, 1), (0, 0), (1, 0)]
    late_sends = [
        kv_copies(4, 1, 1, 2, False),
        kv_copies(3, 0, 1, 3, False),
        kv_copies(2, 0, 0, 3, False) + kv_copies(1, 2, 1, 3, True, (1,)),
        kv_copies(0, 1, 0, 2, False),
    ]

    def meta_copy(d):
        return remote(meta_ref, zmeta.at[d], me_send.at[d], me_recv.at[d], far[d])

    for k in range(n_sp):
        @pl.when(c == k)
        def _():
            for copy in first_sends[k]:
                copy.start()

    for d in (1, 2):
        meta_copy(d).start()
    zmeta[0] = meta_ref[...]

    factor = scale * LOG2E

    def scores_of(h, i, keys):
        return (
            lax.dot_general(
                q_ref[h, i], keys, (((1,), (1,)), ((), ())), preferred_element_type=jnp.float32
            )
            * factor
        )

    for i in range(tiles):
        extent = (i + 1) * tile
        for h in range(heads):
            s = scores_of(h, i, kv_ref[h, 0, :extent])
            row = lax.rem(lax.broadcasted_iota(jnp.int32, (wide, extent), 0), tile) + i * tile
            col = lax.broadcasted_iota(jnp.int32, (wide, extent), 1)
            s = jnp.where(col <= row, s, -jnp.inf)
            high = jnp.max(s, axis=1, keepdims=True)
            p = jnp.exp2(s - high)
            top[h, i] = high
            tot[h, i] = jnp.sum(p, axis=1, keepdims=True)
            acc[h, i] = jnp.dot(
                p.astype(jnp.bfloat16), kv_ref[h, 1, :extent], preferred_element_type=jnp.float32
            )

    for k in range(n_sp):
        @pl.when(c == k)
        def _():
            kv_wait(*relayed[k])
            for copy in late_sends[k]:
                copy.start()

    def order_of(orders):
        codes = [sum((2 * s + h) * 8**j for j, (s, h) in enumerate(o)) for o in orders]
        code, count = jnp.int32(codes[0]), jnp.int32(len(orders[0]))
        for k in range(1, n_sp):
            code = jnp.where(c == k, codes[k], code)
            count = jnp.where(c == k, len(orders[k]), count)
        return code, count

    def absorb(orders, waited):
        code, count = order_of(orders)

        def piece_step(j, code):
            piece = code % 8
            source, h = piece // 2, piece % 2

            @pl.when(j >= waited)
            def _():
                kv_wait(source, h)

            keys, values = kvbuf[source, h, 0], kvbuf[source, h, 1]
            results = []
            for i in range(tiles):
                s = scores_of(h, i, keys)
                before = top[h, i]
                high = jnp.maximum(before, jnp.max(s, axis=1, keepdims=True))
                p = jnp.exp2(s - high)
                decay = jnp.exp2(before - high)
                total = tot[h, i] * decay + jnp.sum(p, axis=1, keepdims=True)
                summed = acc[h, i] * decay + jnp.dot(
                    p.astype(jnp.bfloat16), values, preferred_element_type=jnp.float32
                )
                results.append((high, total, summed))
            for i in range(tiles):
                top[h, i], tot[h, i], acc[h, i] = results[i]
            return code // 8

        lax.fori_loop(0, count, piece_step, code)

    def att_copy(h, d):
        to = (t + d) % n_tp
        return remote(
            att.at[h, pl.ds(pl.multiple_of(to * rows, rows), rows)],
            gathered.at[h, :, pl.ds(pl.multiple_of(t * width, width), width)],
            at_send.at[h, d],
            at_recv.at[h, d],
            (c, to),
        )

    def finish(h):
        for i in range(tiles):
            both = acc[h, i] / tot[h, i]
            mixed = both[:tile] - lam_ref[h] * both[tile:]
            mean = jnp.mean(mixed * mixed, axis=1, keepdims=True)
            normed = mixed * lax.rsqrt(mean + 1e-06) * gain_ref[...]
            att[h, i * tile : (i + 1) * tile] = normed.astype(att.dtype)
        for d in range(1, n_tp):
            att_copy(h, d).start()
        gathered[h, :, pl.ds(pl.multiple_of(t * width, width), width)] = att[
            h, pl.ds(pl.multiple_of(t * rows, rows), rows)
        ]

    def project(h):
        for load in loads[h * n_tp : (h + 1) * n_tp]:
            load.wait()
        for d in range(1, n_tp):
            att_copy(h, d).wait_recv()
        return jnp.dot(
            gathered[h],
            weight[h][: n_tp * width],
            preferred_element_type=jnp.float32,
        )

    absorb([[], [(0, 1), (0, 0)], [(0, 0), (0, 1), (1, 0)], [(1, 0), (2, 0), (1, 1), (0, 0)]], 1)
    finish(0)
    absorb([[], [], [(1, 1)], [(2, 1), (0, 1)]], 0)

    @pl.when(c == n_sp - 1)
    def _():
        for d in range(1, n_sp):
            pl.semaphore_signal(go, inc=1, device_id=column(d), device_id_type=MESH)

    finish(1)
    mine[...] = project(0)
    new = (base_ref[...].astype(jnp.float32) + mine[...] + project(1)).astype(jnp.bfloat16)
    updated[...] = new
    widened = new.astype(jnp.float32)
    mean = jnp.mean(widened * widened, axis=1, keepdims=True)
    x_ref[...] = (widened * lax.rsqrt(mean + 1e-06) * norm_ref[...]).astype(jnp.bfloat16)

    def z_copy(d):
        if d == 1:
            return remote(x_ref, zrows.at[0], zs_send.at[1], zs_recv.at[1], far[1])
        return remote(zrows.at[0], zrows.at[1], zs_send.at[2], zs_recv.at[2], twin)

    def pack_copy(d, s):
        return remote(
            pack.at[s, d - 1], arrived.at[0, s, d], ps_send.at[d, s], ps_recv.at[d, s], column(d)
        )

    def share_copy(d, s):
        return remote(
            arrived.at[0, s, d], arrived.at[1, s, d], fw_send.at[d, s], fw_recv.at[d, s], partner
        )

    def twin_copy(d):
        return remote(
            arrived.at[0, 0, d], arrived.at[0, TWIN, d], tw_send.at[d], tw_recv.at[d], twin
        )

    def pair_copy(s):
        block = pl.ds(s * span, span)
        return remote(psend.at[block], precv.at[block], pp_send.at[s], pp_recv.at[s], partner)

    def fold_copy(d):
        return remote(own.at[TWIN, d], fold.at[d], fo_send.at[d], fo_recv.at[d], twin)

    def back_copy(d, s):
        return remote(
            own.at[s, d], ret.at[s, d], rt_send.at[d, s], rt_recv.at[d, s], column(n_sp - d)
        )

    def z_back(d):
        return remote(zsend.at[d - 1], zret.at[d - 1], zr_send.at[d], zr_recv.at[d], far[d])

    outer = (z == 0) | (z == n_z - 1)

    @pl.when(jnp.logical_not(outer))
    def _():
        z_copy(1).start()

    for d in (1, 2):
        meta_copy(d).wait()

    def route_hits(s, r):
        target = lax.broadcasted_iota(jnp.int32, (slots, rows), 0).astype(jnp.float32)
        return target == zmeta[s, r : r + 1, :rows]

    def pack_rows(s):
        if s:
            z_copy(s).wait_recv()
        if s == 1:
            z_copy(2).start()
            for d in range(2, n_sp):
                twin_copy(d).start()
        hits = route_hits(s, 0) | route_hits(s, 1)
        pick = jnp.where(hits, 1.0, 0.0).astype(jnp.bfloat16)
        source = x_ref[...] if s == 0 else zrows[s - 1]
        packed = (
            jnp.dot(pick, source, preferred_element_type=jnp.float32)
            .astype(jnp.bfloat16)
            .reshape(n_sp, local, cap, model)
        )
        if s == 0:
            arrived[0, 0, 0] = packed[0]
            twin_copy(0).start()

            @pl.when(outer)
            def _():
                z_copy(1).start()

        for d in range(1, n_sp):
            pack[s, d - 1] = packed[d]
            pack_copy(d, s).start()
        if s:
            arrived[0, s, 0] = packed[0]
        share_copy(0, s).start()

    def rows_here(s):
        for d in range(n_sp):
            if s == TWIN:
                twin_copy(d).wait_recv()
            elif d:
                pack_copy(d, s).wait_recv()
            if s == 0 and d == 1:
                twin_copy(d).start()
            if s == TWIN or d:
                share_copy(d, s).start()
        for d in range(n_sp):
            share_copy(d, s).wait_recv()

    def run_experts(s):
        rows_here(s)

        def expert_step(e, carry):
            x = arrived[:, s, :, e].reshape(2 * n_sp * cap, model)
            gated = jnp.dot(x, gate[e], preferred_element_type=jnp.float32)
            lifted = jnp.dot(x, up[e], preferred_element_type=jnp.float32)
            inner = (gated / (1.0 + jnp.exp(-gated)) * lifted).astype(jnp.bfloat16)
            y = jnp.dot(inner, down[e], preferred_element_type=jnp.float32)
            y = y.astype(jnp.bfloat16).reshape(2, n_sp, cap, model)
            own[s, :, e] = y[0]
            for d in range(n_sp):
                place = pl.multiple_of(s * span + (d * local + e) * cap, cap)
                psend[pl.ds(place, cap)] = y[1, d]
            return carry

        lax.fori_loop(0, local, expert_step, 0)
        pair_copy(s).start()

    def reduce_pair(s):
        pair_copy(s).wait_recv()
        for d in list(range(1, n_sp)) + [0]:
            other = precv[s * span + d * local * cap : s * span + (d + 1) * local * cap]
            total = own[s, d].astype(jnp.float32) + other.reshape(local, cap, model).astype(
                jnp.float32
            )
            if s == 0:
                fold_copy(d).wait_recv()
                total = total + fold[d].astype(jnp.float32)
            total = total.astype(jnp.bfloat16)
            if s == TWIN:
                own[s, d] = total
                fold_copy(d).start()
            elif d == 0:
                ret[s, 0] = total
            else:
                own[s, d] = total
                back_copy(d, s).start()

    def mix_rows(s):
        for d in range(1, n_sp):
            back_copy(d, s).wait_recv()
        mixing = jnp.where(route_hits(s, 0), zmeta[s, 2:3, :rows], 0.0) + jnp.where(
            route_hits(s, 1), zmeta[s, 3:4, :rows], 0.0
        )
        high = mixing.astype(jnp.bfloat16)
        low = (mixing - high.astype(jnp.float32)).astype(jnp.bfloat16)
        back = ret[s].reshape(slots, model)
        numbers = (((0,), (0,)), ((), ()))
        merged = lax.dot_general(
            high, back, numbers, preferred_element_type=jnp.float32
        ) + lax.dot_general(low, back, numbers, preferred_element_type=jnp.float32)
        if s:
            zsend[s - 1] = merged.astype(jnp.bfloat16)
            z_back(s).start()
        return merged

    @pl.when(c != n_sp - 1)
    def _():
        pl.semaphore_wait(go, 1)

    pack_rows(0)
    for load in loads[heads * n_tp :]:
        load.wait()
    run_experts(0)
    pack_rows(1)
    pack_rows(2)
    run_experts(1)
    reduce_pair(1)
    run_experts(TWIN)
    reduce_pair(TWIN)
    run_experts(2)
    reduce_pair(2)
    mix_rows(1)
    mix_rows(2)
    reduce_pair(0)
    merged = updated[...].astype(jnp.float32)
    for s in (1, 2):
        z_back(s).wait_recv()
        merged = merged + zret[s - 1].astype(jnp.float32)
    mine[...] = merged
    out_ref[...] = (mine[...] + mix_rows(0)).astype(jnp.bfloat16)

    for k in range(n_sp):
        @pl.when(c == k)
        def _():
            for copy in first_sends[k] + late_sends[k]:
                copy.wait_send()

    for d in range(1, n_tp):
        for h in range(heads):
            att_copy(h, d).wait_send()
    for d in (1, 2):
        z_copy(d).wait_send()
        z_back(d).wait_send()
    for s in range(n_z):
        for d in range(n_sp):
            if d and s != TWIN:
                pack_copy(d, s).wait_send()
                back_copy(d, s).wait_send()
            share_copy(d, s).wait_send()
        pair_copy(s).wait_send()
    for d in range(n_sp):
        twin_copy(d).wait_send()
        fold_copy(d).wait_send()


def masked_queries(queries, tile):
    tokens, heads, pair = queries.shape
    tiles = tokens // tile
    first = (jnp.arange(pair) < pair // 2)[None, :]
    q = jnp.transpose(queries, (1, 0, 2)).reshape(heads, tiles, 1, tile, pair)
    sides = jnp.stack([first, ~first])
    return jnp.where(sides, q, jnp.zeros((), q.dtype)).reshape(heads, tiles, 2 * tile, pair)


def whole_layer(
    queries,
    key_pairs,
    head_values,
    lambdas,
    head_gain,
    meta,
    residual,
    norm_gain,
    out_weight,
    gate_weight,
    up_weight,
    down_weight,
    n_sp,
    n_tp,
    cap,
):
    tokens, heads, pair = queries.shape
    rows, model = residual.shape
    width = head_values.shape[2]
    local = gate_weight.shape[0]
    n_z = n_tp // CORES
    tile = math.gcd(tokens, 256)
    tiles = tokens // tile
    q = masked_queries(queries, tile)
    kv = jnp.transpose(jnp.stack([key_pairs, head_values]), (2, 0, 1, 3))
    dma = pltpu.SemaphoreType.DMA
    vmem = pl.BlockSpec(memory_space=pltpu.VMEM)
    hbm = pl.BlockSpec(memory_space=pl.ANY)
    block = (local, cap, model)
    flat = max(n_tp * width, n_z * n_sp * local * cap)

    def buffer(*shape):
        return pltpu.VMEM(shape, jnp.bfloat16)

    def single(*shape):
        return pltpu.VMEM(shape, jnp.float32)

    return pl.pallas_call(
        functools.partial(layer_kernel, n_sp, n_tp, (pair // 2) ** (-0.5)),
        out_shape=jax.ShapeDtypeStruct((rows, model), jnp.bfloat16),
        in_specs=[pl.BlockSpec(memory_space=pltpu.SMEM)] + [vmem] * 6 + [hbm] * 4,
        out_specs=vmem,
        scratch_shapes=[
            buffer(heads, rows, n_tp * width),
            buffer(n_sp - 1, *kv.shape),
            single(heads, tiles, 2 * tile, width),
            single(heads, tiles, 2 * tile, 1),
            single(heads, tiles, 2 * tile, 1),
            buffer(heads, tokens, width),
            buffer(rows, model),
            buffer(rows, model),
            single(3, *meta.shape),
            buffer(*gate_weight.shape),
            buffer(*up_weight.shape),
            buffer(*down_weight.shape),
            buffer(2, rows, model),
            buffer(3, n_sp - 1, *block),
            buffer(2, n_z, n_sp, *block),
            buffer(flat, model),
            buffer(n_z, n_sp, *block),
            buffer(flat, model),
            buffer(3, n_sp, *block),
            buffer(2, rows, model),
            buffer(2, rows, model),
            buffer(n_sp, *block),
            single(rows, model),
            dma((n_sp + 1, 2)),
            dma((n_sp - 1, heads, 2)),
            dma((heads, n_tp)),
            dma((heads, n_tp)),
            dma((n_z,)),
            dma((n_z,)),
            dma((heads * n_tp + 3,)),
            dma((n_z,)),
            dma((n_z,)),
            dma((n_sp, n_z)),
            dma((n_sp, n_z)),
            dma((n_sp, n_z)),
            dma((n_sp, n_z)),
            dma((n_z,)),
            dma((n_z,)),
            dma((n_sp, n_z)),
            dma((n_sp, n_z)),
            dma((n_z,)),
            dma((n_z,)),
            dma((n_sp,)),
            dma((n_sp,)),
            dma((n_sp,)),
            dma((n_sp,)),
            pltpu.SemaphoreType.REGULAR,
        ],
        compiler_params=pltpu.CompilerParams(
            collective_id=2, has_side_effects=True, vmem_limit_bytes=VMEM_BYTES
        ),
        name="layer",
    )(
        lambdas,
        q,
        kv,
        head_gain.reshape(1, -1),
        meta,
        residual,
        norm_gain.reshape(1, -1),
        out_weight.reshape(n_tp, heads, width, model),
        gate_weight,
        up_weight,
        down_weight,
    )


def shards(
    queries,
    key_pairs,
    head_values,
    lambdas,
    head_gain,
    out_weight,
    residual,
    norm_gain,
    expert_ids,
    route_weights,
    gate_weight,
    up_weight,
    down_weight,
):
    tokens_here, heads_here, pair_width = queries.shape
    value_width = head_values.shape[2]
    rows_here = residual.shape[0]
    sp_count = lax.axis_size("sp")
    tp_count = lax.axis_size("tp")
    z_count = tp_count // CORES
    route_count = expert_ids.shape[1]
    local_experts = gate_weight.shape[0]
    expert_count = local_experts * sp_count
    capacity = max(2, 4 * rows_here * route_count // (3 * expert_count))
    flat_ids = expert_ids.reshape(-1)
    indicator = (flat_ids[:, None] == jnp.arange(expert_count, dtype=jnp.int32)[None, :]).astype(
        jnp.int32
    )
    ranking = jnp.sum(jnp.cumsum(indicator, axis=0) * indicator, axis=1) - 1
    turned = (flat_ids - lax.axis_index("sp") * local_experts) % expert_count
    near_slots = (turned * capacity + ranking).reshape(rows_here, route_count)
    slots = flat_ids * capacity + ranking
    meta = jnp.concatenate([near_slots.astype(jnp.float32), route_weights], axis=1).T
    meta = jnp.pad(meta, ((0, 8 - 2 * route_count), (0, -rows_here % 128)), constant_values=-1.0)
    model_width = residual.shape[1]
    block_bytes = z_count * local_experts * capacity * model_width * 2
    if sp_count == PLANE and z_count == LAYERS and heads_here == HEADS_HERE and pair_width == value_width and (
        capacity % 16 == 0 and rows_here <= 128 and route_count == 2
        and (7 * sp_count - 1) * block_bytes <= 3 * VMEM_BYTES // 5
    ):
        return whole_layer(
            queries,
            key_pairs,
            head_values,
            lambdas,
            head_gain,
            meta,
            residual,
            norm_gain,
            out_weight,
            gate_weight,
            up_weight,
            down_weight,
            sp_count,
            tp_count,
            capacity,
        )
    updated, normed, zmeta = attend(
        queries,
        key_pairs,
        head_values,
        lambdas,
        head_gain,
        meta,
        residual,
        norm_gain,
        out_weight,
        sp_count,
        tp_count,
    )
    if capacity % 16 == 0 and rows_here <= 128 and route_count == 2 and (
        (7 * sp_count - 1) * block_bytes <= 3 * VMEM_BYTES // 5
    ):
        return experts(
            normed, zmeta, updated, gate_weight, up_weight, down_weight, sp_count, z_count, capacity
        )
    sources = jnp.arange(rows_here * route_count, dtype=jnp.int32) // route_count
    outgoing = (
        jnp.zeros((expert_count * capacity, model_width), jnp.bfloat16)
        .at[slots]
        .set(normed[sources])
    )
    arrived = lax.all_to_all(
        outgoing.reshape(sp_count, local_experts, capacity, model_width),
        "sp",
        split_axis=0,
        concat_axis=0,
        tiled=True,
    )
    piece_rows = lax.all_gather(arrived[None], "tp", axis=0, tiled=True)
    gate_part = jnp.einsum(
        "tsecd,edf->tsecf", piece_rows, gate_weight, preferred_element_type=jnp.float32
    )
    up_part = jnp.einsum(
        "tsecd,edf->tsecf", piece_rows, up_weight, preferred_element_type=jnp.float32
    )
    inner_rows = (jax.nn.silu(gate_part) * up_part).astype(jnp.bfloat16)
    partial_value = jnp.einsum(
        "tsecf,efd->tsecd", inner_rows, down_weight, preferred_element_type=jnp.float32
    )
    reduced = lax.psum_scatter(
        partial_value.astype(jnp.bfloat16), "tp", scatter_dimension=0, tiled=True
    )
    returned = lax.all_to_all(reduced[0], "sp", split_axis=0, concat_axis=0, tiled=True)
    picked = (
        returned.reshape(expert_count * capacity, model_width)[slots]
        .astype(jnp.float32)
        .reshape(rows_here, route_count, model_width)
    )
    moe_sum = jnp.sum(picked * route_weights[:, :, None], axis=1)
    return (updated.astype(jnp.float32) + moe_sum).astype(jnp.bfloat16)


def solution(mesh):
    placed = (
        P("sp", "tp", None),
        P("sp", "tp", None),
        P("sp", "tp", None),
        P("tp"),
        P(),
        P(),
        P(("sp", "tp"), None),
        P(),
        P(("sp", "tp"), None),
        P(("sp", "tp"), None),
        P("sp", None, "tp"),
        P("sp", None, "tp"),
        P("sp", "tp", None),
    )
    return jax.shard_map(
        shards, mesh=mesh, in_specs=placed, out_specs=P(("sp", "tp"), None), check_vma=False
    )
```

```python
import functools
import math

import jax
import jax.numpy as jnp
from jax import lax
from jax.experimental import pallas as pl
from jax.experimental.pallas import tpu as pltpu
from jax.sharding import PartitionSpec as P

MESH = pl.DeviceIdType.MESH
LOG2E = 1.4426950408889634
CORES = 2
PLANE = 4
HEADS_HERE = 2
LAYERS = 4
TWIN = 3
VMEM_BYTES = 67043328


def attend_kernel(
    n_sp,
    n_tp,
    scale,
    lam_ref,
    q_ref,
    kv_ref,
    gain_ref,
    meta_ref,
    base_ref,
    norm_ref,
    w_hbm,
    updated_ref,
    normed_ref,
    zmeta_ref,
    weight,
    gathered,
    kvbuf,
    acc,
    top,
    tot,
    att,
    kv_send,
    kv_recv,
    at_send,
    at_recv,
    me_send,
    me_recv,
    own_sem,
    w_sem,
):
    heads, tiles, wide, _ = q_ref.shape
    tile = wide // 2
    rows = base_ref.shape[0]
    n_z = n_tp // CORES
    c = lax.axis_index("sp")
    t = lax.axis_index("tp")
    load = pltpu.make_async_copy(w_hbm, weight, w_sem)
    load.start()
    barrier = pltpu.get_barrier_semaphore()
    for d in range(1, n_sp):
        pl.semaphore_signal(barrier, inc=1, device_id=((c + d) % n_sp, t), device_id_type=MESH)
    for d in range(1, n_tp):
        pl.semaphore_signal(barrier, inc=1, device_id=(c, (t + d) % n_tp), device_id_type=MESH)
    pl.semaphore_wait(barrier, n_sp + n_tp - 2)

    def kv_copy(d, h):
        return pltpu.make_async_remote_copy(
            src_ref=kv_ref.at[h],
            dst_ref=kvbuf.at[d - 1, h],
            send_sem=kv_send.at[d - 1, h],
            recv_sem=kv_recv.at[d - 1, h],
            device_id=((c + d) % n_sp, t),
            device_id_type=MESH,
        )

    def meta_copy(d):
        return pltpu.make_async_remote_copy(
            src_ref=meta_ref,
            dst_ref=zmeta_ref.at[d],
            send_sem=me_send.at[d],
            recv_sem=me_recv.at[d],
            device_id=(c, (t + CORES * d) % n_tp),
            device_id_type=MESH,
        )

    for d in range(1, n_sp):
        @pl.when(c + d < n_sp)
        def _():
            for h in range(heads):
                kv_copy(d, h).start()

    for d in range(1, n_z):
        meta_copy(d).start()
    zmeta_ref[0] = meta_ref[...]

    factor = scale * LOG2E

    def scores_of(h, i, keys):
        return (
            lax.dot_general(
                q_ref[h, i], keys, (((1,), (1,)), ((), ())), preferred_element_type=jnp.float32
            )
            * factor
        )

    for i in range(tiles):
        extent = (i + 1) * tile
        for h in range(heads):
            s = scores_of(h, i, kv_ref[h, 0, :extent])
            row = lax.rem(lax.broadcasted_iota(jnp.int32, (wide, extent), 0), tile) + i * tile
            col = lax.broadcasted_iota(jnp.int32, (wide, extent), 1)
            s = jnp.where(col <= row, s, -jnp.inf)
            high = jnp.max(s, axis=1, keepdims=True)
            p = jnp.exp2(s - high)
            top[h, i] = high
            tot[h, i] = jnp.sum(p, axis=1, keepdims=True)
            acc[h, i] = jnp.dot(
                p.astype(jnp.bfloat16), kv_ref[h, 1, :extent], preferred_element_type=jnp.float32
            )

    def span_step(step, carry):
        for h in range(heads):
            kv_copy(step, h).wait_recv()

        def tile_step(i, inner):
            for h in range(heads):
                s = scores_of(h, i, kvbuf[step - 1, h, 0])
                before = top[h, i]
                high = jnp.maximum(before, jnp.max(s, axis=1, keepdims=True))
                p = jnp.exp2(s - high)
                decay = jnp.exp2(before - high)
                top[h, i] = high
                tot[h, i] = tot[h, i] * decay + jnp.sum(p, axis=1, keepdims=True)
                acc[h, i] = acc[h, i] * decay + jnp.dot(
                    p.astype(jnp.bfloat16),
                    kvbuf[step - 1, h, 1],
                    preferred_element_type=jnp.float32,
                )
            return inner

        return lax.fori_loop(0, tiles, tile_step, carry)

    lax.fori_loop(1, c + 1, span_step, 0)

    for h in range(heads):
        width = acc.shape[3]
        for i in range(tiles):
            both = acc[h, i] / tot[h, i]
            mixed = both[:tile] - lam_ref[h] * both[tile:]
            mean = jnp.mean(mixed * mixed, axis=1, keepdims=True)
            normed = mixed * lax.rsqrt(mean + 1e-06) * gain_ref[...]
            att[i * tile : (i + 1) * tile, h * width : (h + 1) * width] = normed.astype(att.dtype)

    def att_copy(d):
        to = (t + d) % n_tp
        return pltpu.make_async_remote_copy(
            src_ref=att.at[pl.ds(pl.multiple_of(to * rows, rows), rows)],
            dst_ref=gathered.at[t],
            send_sem=at_send.at[d],
            recv_sem=at_recv.at[d],
            device_id=(c, to),
            device_id_type=MESH,
        )

    for d in range(1, n_tp):
        att_copy(d).start()
    own = pltpu.make_async_copy(
        att.at[pl.ds(pl.multiple_of(t * rows, rows), rows)], gathered.at[t], own_sem
    )
    own.start()
    own.wait()
    load.wait()
    span = att.shape[1]
    projected = jnp.zeros(base_ref.shape, jnp.float32)
    for d in range(n_tp):
        if d:
            att_copy(d).wait_recv()
        source = (t - d + n_tp) % n_tp
        projected = projected + jnp.dot(
            gathered[source],
            weight[pl.ds(pl.multiple_of(source * span, span), span), :],
            preferred_element_type=jnp.float32,
        )
    updated = (base_ref[...].astype(jnp.float32) + projected).astype(jnp.bfloat16)
    updated_ref[...] = updated
    widened = updated.astype(jnp.float32)
    mean = jnp.mean(widened * widened, axis=1, keepdims=True)
    normed_ref[...] = (widened * lax.rsqrt(mean + 1e-06) * norm_ref[...]).astype(jnp.bfloat16)
    for d in range(1, n_tp):
        att_copy(d).wait_send()
    for d in range(1, n_z):
        meta_copy(d).wait()
    for d in range(1, n_sp):
        @pl.when(c + d < n_sp)
        def _():
            for h in range(heads):
                kv_copy(d, h).wait_send()


def attend(queries, key_pairs, head_values, lambdas, head_gain, meta, residual, norm_gain, out_weight, n_sp, n_tp):
    tokens, heads, pair = queries.shape
    rows = residual.shape[0]
    width = head_values.shape[2]
    half = pair // 2
    tile = math.gcd(tokens, 256)
    tiles = tokens // tile
    first = (jnp.arange(pair) < half)[None, :]
    q = jnp.transpose(queries, (1, 0, 2)).reshape(heads, tiles, 1, tile, pair)
    sides = jnp.stack([first, ~first])
    q = jnp.where(sides, q, jnp.zeros((), q.dtype)).reshape(heads, tiles, 2 * tile, pair)
    kv = jnp.transpose(jnp.stack([key_pairs, head_values]), (2, 0, 1, 3))
    dma = pltpu.SemaphoreType.DMA
    vmem = pl.BlockSpec(memory_space=pltpu.VMEM)
    n_z = n_tp // CORES
    return pl.pallas_call(
        functools.partial(attend_kernel, n_sp, n_tp, half ** (-0.5)),
        out_shape=(
            jax.ShapeDtypeStruct(residual.shape, jnp.bfloat16),
            jax.ShapeDtypeStruct(residual.shape, jnp.bfloat16),
            jax.ShapeDtypeStruct((n_z,) + meta.shape, meta.dtype),
        ),
        in_specs=[pl.BlockSpec(memory_space=pltpu.SMEM)] + [vmem] * 6
        + [pl.BlockSpec(memory_space=pl.ANY)],
        out_specs=(vmem, vmem, vmem),
        scratch_shapes=[
            pltpu.VMEM(out_weight.shape, out_weight.dtype),
            pltpu.VMEM((n_tp, rows, heads * width), jnp.bfloat16),
            pltpu.VMEM((n_sp - 1,) + kv.shape, kv.dtype),
            pltpu.VMEM((heads, tiles, 2 * tile, width), jnp.float32),
            pltpu.VMEM((heads, tiles, 2 * tile, 1), jnp.float32),
            pltpu.VMEM((heads, tiles, 2 * tile, 1), jnp.float32),
            pltpu.VMEM((tokens, heads * width), jnp.bfloat16),
            dma((n_sp - 1, heads)),
            dma((n_sp - 1, heads)),
            dma((n_tp,)),
            dma((n_tp,)),
            dma((n_z,)),
            dma((n_z,)),
            dma,
            dma,
        ],
        compiler_params=pltpu.CompilerParams(
            collective_id=0, has_side_effects=True, vmem_limit_bytes=48 * 1024 * 1024
        ),
        name="attend",
    )(lambdas, q, kv, head_gain.reshape(1, -1), meta, residual, norm_gain.reshape(1, -1), out_weight)


def experts_kernel(
    n_sp,
    n_z,
    x_ref,
    meta_ref,
    base_ref,
    gate_hbm,
    up_hbm,
    down_hbm,
    out_ref,
    gate,
    up,
    down,
    zrows,
    pack,
    arrived,
    psend,
    own,
    precv,
    ret,
    zsend,
    zret,
    mine,
    w_sem,
    zs_send,
    zs_recv,
    ps_send,
    ps_recv,
    fw_send,
    fw_recv,
    pp_send,
    pp_recv,
    rt_send,
    rt_recv,
    zr_send,
    zr_recv,
):
    rows, model = x_ref.shape
    local, cap = pack.shape[2], pack.shape[3]
    slots = n_sp * local * cap
    c = lax.axis_index("sp")
    t = lax.axis_index("tp")
    n_tp = n_z * CORES
    core = t % CORES
    partner = (c, t + 1 - 2 * core)
    loads = [
        pltpu.make_async_copy(a, b, w_sem.at[i])
        for i, (a, b) in enumerate(((gate_hbm, gate), (up_hbm, up), (down_hbm, down)))
    ]
    for load in loads:
        load.start()

    def column(d):
        return ((c + d) % n_sp, t)

    def layer(d):
        return (c, (t + CORES * d) % n_tp)

    barrier = pltpu.get_barrier_semaphore()
    for d in range(1, n_sp):
        pl.semaphore_signal(barrier, inc=1, device_id=column(d), device_id_type=MESH)
    for d in range(1, n_z):
        pl.semaphore_signal(barrier, inc=1, device_id=layer(d), device_id_type=MESH)
    pl.semaphore_signal(barrier, inc=1, device_id=partner, device_id_type=MESH)
    pl.semaphore_wait(barrier, n_sp + n_z - 1)

    def remote(src, dst, send, recv, target):
        return pltpu.make_async_remote_copy(
            src_ref=src,
            dst_ref=dst,
            send_sem=send,
            recv_sem=recv,
            device_id=target,
            device_id_type=MESH,
        )

    def z_copy(d):
        return remote(x_ref, zrows.at[d - 1], zs_send.at[d], zs_recv.at[d], layer(d))

    def pack_copy(d, s):
        return remote(
            pack.at[s, d - 1], arrived.at[0, s, d], ps_send.at[d, s], ps_recv.at[d, s], column(d)
        )

    def share_copy(d, s):
        return remote(
            arrived.at[0, s, d], arrived.at[1, s, d], fw_send.at[d, s], fw_recv.at[d, s], partner
        )

    def pair_copy(s):
        return remote(psend.at[s], precv.at[s], pp_send.at[s], pp_recv.at[s], partner)

    def back_copy(d, s):
        return remote(
            own.at[s, d], ret.at[s, d], rt_send.at[d, s], rt_recv.at[d, s], column(n_sp - d)
        )

    def z_back(d):
        return remote(
            zsend.at[d], zret.at[d], zr_send.at[d], zr_recv.at[d], layer(n_z - d)
        )

    for d in range(1, n_z):
        z_copy(d).start()

    def route_hits(s, r):
        target = lax.broadcasted_iota(jnp.int32, (slots, rows), 0).astype(jnp.float32)
        return target == meta_ref[s, r : r + 1, :rows]

    def pack_rows(s):
        if s:
            z_copy(s).wait_recv()
        hits = route_hits(s, 0) | route_hits(s, 1)
        pick = jnp.where(hits, 1.0, 0.0).astype(jnp.bfloat16)
        source = x_ref[...] if s == 0 else zrows[s - 1]
        packed = (
            jnp.dot(pick, source, preferred_element_type=jnp.float32)
            .astype(jnp.bfloat16)
            .reshape(n_sp, local, cap, model)
        )
        for d in range(1, n_sp):
            pack[s, d - 1] = packed[d]
            pack_copy(d, s).start()
        arrived[0, s, 0] = packed[0]
        share_copy(0, s).start()

    def run_experts(s):
        for d in range(1, n_sp):
            pack_copy(d, s).wait_recv()
            share_copy(d, s).start()
        for d in range(n_sp):
            share_copy(d, s).wait_recv()

        def expert_step(e, carry):
            x = arrived[:, s, :, e].reshape(2 * n_sp * cap, model)
            gated = jnp.dot(x, gate[e], preferred_element_type=jnp.float32)
            lifted = jnp.dot(x, up[e], preferred_element_type=jnp.float32)
            inner = (gated / (1.0 + jnp.exp(-gated)) * lifted).astype(jnp.bfloat16)
            y = jnp.dot(inner, down[e], preferred_element_type=jnp.float32)
            y = y.astype(jnp.bfloat16).reshape(2, n_sp, cap, model)
            own[s, :, e] = y[0]
            psend[s, :, e] = y[1]
            return carry

        lax.fori_loop(0, local, expert_step, 0)
        pair_copy(s).start()

    def reduce_pair(s):
        pair_copy(s).wait_recv()
        for d in list(range(1, n_sp)) + [0]:
            total = own[s, d].astype(jnp.float32) + precv[s, d].astype(jnp.float32)
            total = total.astype(jnp.bfloat16)
            if d == 0:
                ret[s, 0] = total
            else:
                own[s, d] = total
                back_copy(d, s).start()

    def mix_rows(s):
        for d in range(1, n_sp):
            back_copy(d, s).wait_recv()
        mixing = jnp.where(route_hits(s, 0), meta_ref[s, 2:3, :rows], 0.0) + jnp.where(
            route_hits(s, 1), meta_ref[s, 3:4, :rows], 0.0
        )
        high = mixing.astype(jnp.bfloat16)
        low = (mixing - high.astype(jnp.float32)).astype(jnp.bfloat16)
        back = ret[s].reshape(slots, model)
        numbers = (((0,), (0,)), ((), ()))
        merged = lax.dot_general(
            high, back, numbers, preferred_element_type=jnp.float32
        ) + lax.dot_general(low, back, numbers, preferred_element_type=jnp.float32)
        if s:
            zsend[s] = merged.astype(jnp.bfloat16)
            z_back(s).start()
        else:
            mine[...] = merged

    pack_rows(0)
    for load in loads:
        load.wait()
    if n_z > 1:
        pack_rows(1)
    for s in range(n_z):
        run_experts(s)
        if s + 2 < n_z:
            pack_rows(s + 2)
        elif s + 2 - n_z < n_z - 2:
            mix_rows(s + 2 - n_z)
        reduce_pair(s)
    for s in range(max(0, n_z - 2), n_z):
        mix_rows(s)
    merged = mine[...]
    for s in range(1, n_z):
        z_back(s).wait_recv()
        merged = merged + zret[s].astype(jnp.float32)
    out_ref[...] = (base_ref[...].astype(jnp.float32) + merged).astype(jnp.bfloat16)

    for d in range(1, n_z):
        z_copy(d).wait_send()
        z_back(d).wait_send()
    for s in range(n_z):
        for d in range(n_sp):
            if d:
                pack_copy(d, s).wait_send()
                back_copy(d, s).wait_send()
            share_copy(d, s).wait_send()
        pair_copy(s).wait_send()


def experts(normed, zmeta, updated, gate_weight, up_weight, down_weight, n_sp, n_z, cap):
    rows, model = normed.shape
    local = gate_weight.shape[0]
    dma = pltpu.SemaphoreType.DMA
    vmem = pl.BlockSpec(memory_space=pltpu.VMEM)
    hbm = pl.BlockSpec(memory_space=pl.ANY)
    block = (local, cap, model)

    def buffer(*shape):
        return pltpu.VMEM(shape, jnp.bfloat16)

    return pl.pallas_call(
        functools.partial(experts_kernel, n_sp, n_z),
        out_shape=jax.ShapeDtypeStruct((rows, model), jnp.bfloat16),
        in_specs=[vmem] * 3 + [hbm] * 3,
        out_specs=vmem,
        scratch_shapes=[
            buffer(*gate_weight.shape),
            buffer(*up_weight.shape),
            buffer(*down_weight.shape),
            buffer(n_z - 1, rows, model),
            buffer(n_z, n_sp - 1, *block),
            buffer(2, n_z, n_sp, *block),
            buffer(n_z, n_sp, *block),
            buffer(n_z, n_sp, *block),
            buffer(n_z, n_sp, *block),
            buffer(n_z, n_sp, *block),
            buffer(n_z, rows, model),
            buffer(n_z, rows, model),
            pltpu.VMEM((rows, model), jnp.float32),
            dma((3,)),
            dma((n_z,)),
            dma((n_z,)),
            dma((n_sp, n_z)),
            dma((n_sp, n_z)),
            dma((n_sp, n_z)),
            dma((n_sp, n_z)),
            dma((n_z,)),
            dma((n_z,)),
            dma((n_sp, n_z)),
            dma((n_sp, n_z)),
            dma((n_z,)),
            dma((n_z,)),
        ],
        compiler_params=pltpu.CompilerParams(
            collective_id=1, has_side_effects=True, vmem_limit_bytes=VMEM_BYTES
        ),
        name="experts",
    )(normed, zmeta, updated, gate_weight, up_weight, down_weight)


def layer_kernel(
    n_sp,
    n_tp,
    scale,
    lam_ref,
    raw_ref,
    k_ref,
    v_ref,
    gain_ref,
    ids_ref,
    mix_ref,
    base_ref,
    norm_ref,
    w_hbm,
    gate_hbm,
    up_hbm,
    down_hbm,
    out_ref,
    q_ref,
    gathered,
    kvbuf,
    acc,
    top,
    tot,
    att,
    bases,
    updated,
    x_ref,
    zmeta,
    gate,
    up,
    down,
    zrows,
    pack,
    arrived,
    psend,
    own,
    precv,
    ret,
    zsend,
    zret,
    fold,
    parts,
    kv_send,
    kv_recv,
    at_send,
    at_recv,
    ar_send,
    ar_recv,
    ba_send,
    ba_recv,
    me_send,
    me_recv,
    w_sem,
    ps_send,
    ps_recv,
    fw_send,
    fw_recv,
    pp_send,
    pp_recv,
    rt_send,
    rt_recv,
    zr_send,
    zr_recv,
    tw_send,
    tw_recv,
    fo_send,
    fo_recv,
    go,
):
    heads, tiles, wide, _ = q_ref.shape
    tile = wide // 2
    rows, model = base_ref.shape
    width = v_ref.shape[2]
    n_z = n_tp // CORES
    local, cap = pack.shape[2], pack.shape[3]
    slots = n_sp * local * cap
    span = n_sp * local * cap
    c = lax.axis_index("sp")
    t = lax.axis_index("tp")
    core = t % CORES
    partner = (c, t + 1 - 2 * core)

    def column(d):
        return ((c + d) % n_sp, t)

    z = t // CORES
    twin_z = z + 1 - 2 * (z % 2)
    far_z = (z + n_z // 2) % n_z
    twin = (c, twin_z * CORES + core)
    far = [None, (c, far_z * CORES + core), (c, (far_z + 1 - 2 * (far_z % 2)) * CORES + core)]

    weight = (psend, precv)
    loads = [
        pltpu.make_async_copy(a, b, w_sem.at[i])
        for i, (a, b) in enumerate(
            [
                (w_hbm.at[source, h], weight[h].at[source * width : (source + 1) * width])
                for h in range(heads)
                for source in range(n_tp)
            ]
            + [(gate_hbm, gate), (up_hbm, up), (down_hbm, down)]
        )
    ]
    for load in loads:
        load.start()
    barrier = pltpu.get_barrier_semaphore()
    for d in range(1, n_sp):
        pl.semaphore_signal(barrier, inc=1, device_id=column(d), device_id_type=MESH)
    for d in range(1, n_tp):
        pl.semaphore_signal(barrier, inc=1, device_id=(c, (t + d) % n_tp), device_id_type=MESH)
    pl.semaphore_wait(barrier, n_sp + n_tp - 2)

    def remote(src, dst, send, recv, target):
        return pltpu.make_async_remote_copy(
            src_ref=src,
            dst_ref=dst,
            send_sem=send,
            recv_sem=recv,
            device_id=target,
            device_id_type=MESH,
        )

    def kv_copies(slot, source, h, to, mine_too, parts=(0, 1)):
        return [
            remote(
                (k_ref, v_ref)[part].at[h] if mine_too else kvbuf.at[source, h, part],
                kvbuf.at[source, h, part],
                kv_send.at[slot, part],
                kv_recv.at[source, h, part],
                (to, t),
            )
            for part in parts
        ]

    def kv_wait(source, h):
        for part in range(2):
            remote(
                kvbuf.at[source, h, part],
                kvbuf.at[source, h, part],
                kv_send.at[0, part],
                kv_recv.at[source, h, part],
                partner,
            ).wait_recv()

    first_sends = [
        kv_copies(0, 0, 0, 2, True)
        + kv_copies(1, 0, 1, 1, True)
        + kv_copies(2, 0, 1, 2, True)
        + kv_copies(3, 0, 0, 1, True),
        kv_copies(0, 1, 0, 3, True) + kv_copies(1, 1, 1, 0, True) + kv_copies(2, 1, 1, 3, True),
        kv_copies(0, 2, 0, 3, True) + kv_copies(1, 2, 1, 3, True, (0,)),
        [],
    ]
    relayed = [(1, 1), (0, 1), (0, 0), (1, 0)]
    late_sends = [
        kv_copies(4, 1, 1, 2, False),
        kv_copies(3, 0, 1, 3, False),
        kv_copies(2, 0, 0, 3, False) + kv_copies(1, 2, 1, 3, True, (1,)),
        kv_copies(0, 1, 0, 2, False),
    ]

    def meta_copy(d):
        return remote(zmeta.at[0], zmeta.at[d], me_send.at[d], me_recv.at[d], far[d])

    for k in range(n_sp):
        @pl.when(c == k)
        def _():
            for copy in first_sends[k]:
                copy.start()

    def base_copy(d, side):
        columns = slice(side * (model // 2), (side + 1) * (model // 2))
        return remote(
            base_ref.at[:, columns] if d == 1 else bases.at[0, :, columns],
            bases.at[d - 1, :, columns],
            ba_send.at[d - 1, side],
            ba_recv.at[d - 1, side],
            far[1] if d == 1 else twin,
        )

    def pass_base(side):
        base_copy(1, side).wait_recv()
        base_copy(2, side).start()

    for side in range(2):
        base_copy(1, side).start()

    experts = n_sp * local
    shape = (experts, rows)
    names = lax.broadcasted_iota(jnp.int32, shape, 0)
    named = [names == ids_ref[r : r + 1, :] for r in range(2)]
    chosen = jnp.where(named[0] | named[1], 1.0, 0.0).astype(jnp.bfloat16)
    earlier = lax.broadcasted_iota(jnp.int32, (rows, rows), 0) < lax.broadcasted_iota(
        jnp.int32, (rows, rows), 1
    )
    ranks = jnp.dot(
        chosen, jnp.where(earlier, 1.0, 0.0).astype(jnp.bfloat16), preferred_element_type=jnp.float32
    )
    zmeta[0] = jnp.full(zmeta.shape[1:], -1.0, jnp.float32)
    for r in range(2):
        turned = ids_ref[r : r + 1, :] - c * local
        turned = jnp.where(turned < 0, turned + experts, turned)
        rank = jnp.sum(jnp.where(named[r], ranks, 0.0), axis=0, keepdims=True)
        zmeta[0, r : r + 1, :rows] = (turned * cap).astype(jnp.float32) + rank
        zmeta[0, 2 + r : 3 + r, :rows] = mix_ref[r : r + 1, :]
    for d in (1, 2):
        meta_copy(d).start()

    side = lax.broadcasted_iota(jnp.int32, (tile, raw_ref.shape[2]), 1) < raw_ref.shape[2] // 2
    for h in range(heads):
        for i in range(tiles):
            part = raw_ref[h, i * tile : (i + 1) * tile]
            q_ref[h, i, :tile] = jnp.where(side, part, jnp.zeros_like(part))
            q_ref[h, i, tile:] = jnp.where(side, jnp.zeros_like(part), part)

    factor = scale * LOG2E

    def scores_of(h, i, keys):
        return (
            lax.dot_general(
                q_ref[h, i], keys, (((1,), (1,)), ((), ())), preferred_element_type=jnp.float32
            )
            * factor
        )

    for i in range(tiles):
        extent = (i + 1) * tile
        for h in range(heads):
            s = scores_of(h, i, k_ref[h, :extent])
            row = lax.rem(lax.broadcasted_iota(jnp.int32, (wide, extent), 0), tile) + i * tile
            col = lax.broadcasted_iota(jnp.int32, (wide, extent), 1)
            s = jnp.where(col <= row, s, -jnp.inf)
            high = jnp.max(s, axis=1, keepdims=True)
            p = jnp.exp2(s - high)
            top[h, i] = high
            tot[h, i] = jnp.sum(p, axis=1, keepdims=True)
            acc[h, i] = jnp.dot(
                p.astype(jnp.bfloat16), v_ref[h, :extent], preferred_element_type=jnp.float32
            )

    for k in range(n_sp):
        @pl.when(c == k)
        def _():
            kv_wait(*relayed[k])
            for copy in late_sends[k]:
                copy.start()

    pass_base(0)

    def order_of(orders):
        codes = [sum((2 * s + h) * 8**j for j, (s, h) in enumerate(o)) for o in orders]
        code, count = jnp.int32(codes[0]), jnp.int32(len(orders[0]))
        for k in range(1, n_sp):
            code = jnp.where(c == k, codes[k], code)
            count = jnp.where(c == k, len(orders[k]), count)
        return code, count

    def absorb(orders, waited, passing=False):
        code, count = order_of(orders)

        def piece_step(j, code):
            piece = code % 8
            source, h = piece // 2, piece % 2

            @pl.when(j >= waited)
            def _():
                kv_wait(source, h)

            if passing:

                @pl.when(j == count - 1)
                def _():
                    pass_base(1)

            keys, values = kvbuf[source, h, 0], kvbuf[source, h, 1]
            results = []
            for i in range(tiles):
                s = scores_of(h, i, keys)
                before = top[h, i]
                high = jnp.maximum(before, jnp.max(s, axis=1, keepdims=True))
                p = jnp.exp2(s - high)
                decay = jnp.exp2(before - high)
                total = tot[h, i] * decay + jnp.sum(p, axis=1, keepdims=True)
                summed = acc[h, i] * decay + jnp.dot(
                    p.astype(jnp.bfloat16), values, preferred_element_type=jnp.float32
                )
                results.append((high, total, summed))
            for i in range(tiles):
                top[h, i], tot[h, i], acc[h, i] = results[i]
            return code // 8

        lax.fori_loop(0, count, piece_step, code)

    half = n_z // 2

    def block_rows(b, to_z, to_core):
        layer = to_z if b == 0 else (to_z + half) % n_z
        if b == 2:
            layer = layer + 1 - 2 * (layer % 2)
        return pl.ds(pl.multiple_of((layer * CORES + to_core) * rows, rows), rows)

    here = pl.ds(pl.multiple_of(t * width, width), width)

    def att_copy(h, b, d):
        to = (t + d) % n_tp
        return remote(
            att.at[h, block_rows(b, to // CORES, to % CORES)],
            gathered.at[h, b, :, here],
            at_send.at[h, b, d],
            at_recv.at[h, b, d],
            (c, to),
        )

    def relay_copy(h):
        side = half * CORES * width
        across = pl.ds(pl.multiple_of((1 - z // half) * side, side), side)
        return remote(
            gathered.at[h, 1, :, across],
            gathered.at[h, 2, :, across],
            ar_send.at[h],
            ar_recv.at[h],
            twin,
        )

    def near(d):
        return ((t + d) % n_tp) // CORES // half == z // half

    def finish(h):
        for i in range(tiles):
            both = acc[h, i] / tot[h, i]
            mixed = both[:tile] - lam_ref[h] * both[tile:]
            mean = jnp.mean(mixed * mixed, axis=1, keepdims=True)
            normed = mixed * lax.rsqrt(mean + 1e-06) * gain_ref[...]
            att[h, i * tile : (i + 1) * tile] = normed.astype(att.dtype)
        for b in range(2):
            for d in range(1, n_tp):
                att_copy(h, b, d).start()
        for d in range(1, n_tp):

            @pl.when(near(d))
            def _():
                att_copy(h, 2, d).start()

        for b in range(3):
            gathered[h, b, :, here] = att[h, block_rows(b, z, core)]

    def await_rows(h, b):
        for d in range(1, n_tp):
            if b < 2:
                att_copy(h, b, d).wait_recv()
            else:

                @pl.when(near(n_tp - d))
                def _():
                    att_copy(h, b, d).wait_recv()

        if b == 1:
            relay_copy(h).start()
        if b == 2:
            relay_copy(h).wait_recv()

    def project(h, b):
        return jnp.dot(
            gathered[h, b], weight[h][: n_tp * width], preferred_element_type=jnp.float32
        )

    def normalize(base, projected):
        new = (base.astype(jnp.float32) + projected).astype(jnp.bfloat16)
        widened = new.astype(jnp.float32)
        mean = jnp.mean(widened * widened, axis=1, keepdims=True)
        return new, (widened * lax.rsqrt(mean + 1e-06) * norm_ref[...]).astype(jnp.bfloat16)

    def far_rows(b):
        await_rows(1, b)
        if b == 2:
            for part in range(2):
                base_copy(2, part).wait_recv()
        _, normed = normalize(bases[b - 1], parts[b] + project(1, b))
        zrows[b - 1] = normed

    absorb([[], [(0, 1), (0, 0)], [(0, 0), (0, 1), (1, 0)], [(1, 0), (2, 0), (1, 1), (0, 0)]], 1, True)

    @pl.when(c == 0)
    def _():
        pass_base(1)

    finish(0)
    absorb([[], [], [(1, 1)], [(2, 1), (0, 1)]], 0)

    @pl.when(c == n_sp - 1)
    def _():
        for d in range(1, n_sp):
            pl.semaphore_signal(go, inc=1, device_id=column(d), device_id_type=MESH)

    finish(1)
    for load in loads[: heads * n_tp]:
        load.wait()
    await_rows(0, 0)
    parts[0] = project(0, 0)
    await_rows(0, 1)
    parts[1] = project(0, 1)
    await_rows(1, 0)
    new, normed = normalize(base_ref[...], parts[0] + project(1, 0))
    updated[...] = new
    x_ref[...] = normed

    def pack_copy(d, s):
        return remote(
            pack.at[s, d - 1], arrived.at[0, s, d], ps_send.at[d, s], ps_recv.at[d, s], column(d)
        )

    def share_copy(d, s):
        return remote(
            arrived.at[0, s, d], arrived.at[1, s, d], fw_send.at[d, s], fw_recv.at[d, s], partner
        )

    def twin_copy(d):
        return remote(
            arrived.at[0, 0, d], arrived.at[0, TWIN, d], tw_send.at[d], tw_recv.at[d], twin
        )

    def pair_copy(s):
        block = pl.ds(s * span, span)
        return remote(psend.at[block], precv.at[block], pp_send.at[s], pp_recv.at[s], partner)

    def fold_copy(d):
        return remote(own.at[TWIN, d], fold.at[d], fo_send.at[d], fo_recv.at[d], twin)

    def back_copy(d, s):
        return remote(
            own.at[s, d], ret.at[s, d], rt_send.at[d, s], rt_recv.at[d, s], column(n_sp - d)
        )

    def z_back(d):
        return remote(zsend.at[d - 1], zret.at[d - 1], zr_send.at[d], zr_recv.at[d], far[d])

    outer = (z == 0) | (z == n_z - 1)
    for d in (1, 2):
        meta_copy(d).wait()

    def route_hits(s, r):
        target = lax.broadcasted_iota(jnp.int32, (slots, rows), 0).astype(jnp.float32)
        return target == zmeta[s, r : r + 1, :rows]

    def pack_rows(s):
        hits = route_hits(s, 0) | route_hits(s, 1)
        pick = jnp.where(hits, 1.0, 0.0).astype(jnp.bfloat16)
        source = x_ref[...] if s == 0 else zrows[s - 1]
        packed = (
            jnp.dot(pick, source, preferred_element_type=jnp.float32)
            .astype(jnp.bfloat16)
            .reshape(n_sp, local, cap, model)
        )
        if s == 0:
            arrived[0, 0, 0] = packed[0]
            twin_copy(0).start()
        for d in range(1, n_sp):
            pack[s, d - 1] = packed[d]
            pack_copy(d, s).start()
        if s:
            arrived[0, s, 0] = packed[0]
        share_copy(0, s).start()

    def rows_here(s):
        for d in range(n_sp):
            if s == TWIN:
                twin_copy(d).wait_recv()
            elif s and d:
                pack_copy(d, s).wait_recv()
            if s == TWIN or d:
                share_copy(d, s).start()
        for d in range(n_sp):
            share_copy(d, s).wait_recv()

    def run_experts(s):
        rows_here(s)

        def expert_step(e, carry):
            x = arrived[:, s, :, e].reshape(2 * n_sp * cap, model)
            gated = jnp.dot(x, gate[e], preferred_element_type=jnp.float32)
            lifted = jnp.dot(x, up[e], preferred_element_type=jnp.float32)
            inner = (gated / (1.0 + jnp.exp(-gated)) * lifted).astype(jnp.bfloat16)
            y = jnp.dot(inner, down[e], preferred_element_type=jnp.float32)
            y = y.astype(jnp.bfloat16).reshape(2, n_sp, cap, model)
            own[s, :, e] = y[0]
            for d in range(n_sp):
                place = pl.multiple_of(s * span + (d * local + e) * cap, cap)
                psend[pl.ds(place, cap)] = y[1, d]
            return carry

        lax.fori_loop(0, local, expert_step, 0)
        pair_copy(s).start()

    def reduce_pair(s):
        pair_copy(s).wait_recv()
        for d in list(range(1, n_sp)) + [0]:
            other = precv[s * span + d * local * cap : s * span + (d + 1) * local * cap]
            total = own[s, d].astype(jnp.float32) + other.reshape(local, cap, model).astype(
                jnp.float32
            )
            if s == 0:
                fold_copy(d).wait_recv()
                total = total + fold[d].astype(jnp.float32)
            total = total.astype(jnp.bfloat16)
            if s == TWIN:
                own[s, d] = total
                if d in (1, 2):
                    fold_copy(d).start()
                else:

                    @pl.when(jnp.logical_not(outer))
                    def _():
                        fold_copy(d).start()

            elif d == 0:
                ret[s, 0] = total
            else:
                own[s, d] = total
                back_copy(d, s).start()

    def mix_rows(s):
        for d in range(1, n_sp):
            back_copy(d, s).wait_recv()
        mixing = jnp.where(route_hits(s, 0), zmeta[s, 2:3, :rows], 0.0) + jnp.where(
            route_hits(s, 1), zmeta[s, 3:4, :rows], 0.0
        )
        high = mixing.astype(jnp.bfloat16)
        low = (mixing - high.astype(jnp.float32)).astype(jnp.bfloat16)
        back = ret[s].reshape(slots, model)
        numbers = (((0,), (0,)), ((), ()))
        merged = lax.dot_general(
            high, back, numbers, preferred_element_type=jnp.float32
        ) + lax.dot_general(low, back, numbers, preferred_element_type=jnp.float32)
        if s:
            zsend[s - 1] = merged.astype(jnp.bfloat16)
            z_back(s).start()
        return merged

    @pl.when(c != n_sp - 1)
    def _():
        pl.semaphore_wait(go, 1)

    pack_rows(0)
    for load in loads[heads * n_tp :]:
        load.wait()
    far_rows(1)
    pack_rows(1)
    await_rows(0, 2)
    parts[2] = project(0, 2)
    for d in range(1, n_sp):
        pack_copy(d, 0).wait_recv()
        twin_copy(d).start()
    far_rows(2)
    pack_rows(2)
    run_experts(0)
    run_experts(1)
    reduce_pair(1)
    run_experts(TWIN)
    reduce_pair(TWIN)
    run_experts(2)
    reduce_pair(2)
    mix_rows(1)

    @pl.when(outer)
    def _():
        for d in (n_sp - 1, 0):
            fold_copy(d).start()

    mix_rows(2)
    reduce_pair(0)
    merged = updated[...].astype(jnp.float32)
    for s in (1, 2):
        z_back(s).wait_recv()
        merged = merged + zret[s - 1].astype(jnp.float32)
    parts[0] = merged
    out_ref[...] = (parts[0] + mix_rows(0)).astype(jnp.bfloat16)

    for k in range(n_sp):
        @pl.when(c == k)
        def _():
            for copy in first_sends[k] + late_sends[k]:
                copy.wait_send()

    for h in range(heads):
        for d in range(1, n_tp):
            for b in range(2):
                att_copy(h, b, d).wait_send()

            @pl.when(near(d))
            def _():
                att_copy(h, 2, d).wait_send()

        relay_copy(h).wait_send()
    for d in (1, 2):
        for side in range(2):
            base_copy(d, side).wait_send()
    for d in (1, 2):
        z_back(d).wait_send()
    for s in range(n_z):
        for d in range(n_sp):
            if d and s != TWIN:
                pack_copy(d, s).wait_send()
                back_copy(d, s).wait_send()
            share_copy(d, s).wait_send()
        pair_copy(s).wait_send()
    for d in range(n_sp):
        twin_copy(d).wait_send()
        fold_copy(d).wait_send()


def whole_layer(
    queries,
    key_pairs,
    head_values,
    lambdas,
    head_gain,
    expert_ids,
    route_weights,
    residual,
    norm_gain,
    out_weight,
    gate_weight,
    up_weight,
    down_weight,
    n_sp,
    n_tp,
    cap,
):
    tokens, heads, pair = queries.shape
    rows, model = residual.shape
    width = head_values.shape[2]
    local = gate_weight.shape[0]
    n_z = n_tp // CORES
    tile = math.gcd(tokens, 256)
    tiles = tokens // tile
    q, k, v = (jnp.transpose(x, (1, 0, 2)) for x in (queries, key_pairs, head_values))
    dma = pltpu.SemaphoreType.DMA
    vmem = pl.BlockSpec(memory_space=pltpu.VMEM)
    hbm = pl.BlockSpec(memory_space=pl.ANY)
    block = (local, cap, model)
    flat = max(n_tp * width, n_z * n_sp * local * cap)

    def buffer(*shape):
        return pltpu.VMEM(shape, jnp.bfloat16)

    def single(*shape):
        return pltpu.VMEM(shape, jnp.float32)

    return pl.pallas_call(
        functools.partial(layer_kernel, n_sp, n_tp, (pair // 2) ** (-0.5)),
        out_shape=jax.ShapeDtypeStruct((rows, model), jnp.bfloat16),
        in_specs=[pl.BlockSpec(memory_space=pltpu.SMEM)] + [vmem] * 8 + [hbm] * 4,
        out_specs=vmem,
        scratch_shapes=[
            buffer(heads, tiles, 2 * tile, pair),
            buffer(heads, 3, rows, n_tp * width),
            buffer(n_sp - 1, heads, 2, tokens, width),
            single(heads, tiles, 2 * tile, width),
            single(heads, tiles, 2 * tile, 1),
            single(heads, tiles, 2 * tile, 1),
            buffer(heads, tokens, width),
            buffer(2, rows, model),
            buffer(rows, model),
            buffer(rows, model),
            single(3, 8, rows + -rows % 128),
            buffer(*gate_weight.shape),
            buffer(*up_weight.shape),
            buffer(*down_weight.shape),
            buffer(2, rows, model),
            buffer(3, n_sp - 1, *block),
            buffer(2, n_z, n_sp, *block),
            buffer(flat, model),
            buffer(n_z, n_sp, *block),
            buffer(flat, model),
            buffer(3, n_sp, *block),
            buffer(2, rows, model),
            buffer(2, rows, model),
            buffer(n_sp, *block),
            single(3, rows, model),
            dma((n_sp + 1, 2)),
            dma((n_sp - 1, heads, 2)),
            dma((heads, 3, n_tp)),
            dma((heads, 3, n_tp)),
            dma((heads,)),
            dma((heads,)),
            dma((2, 2)),
            dma((2, 2)),
            dma((n_z,)),
            dma((n_z,)),
            dma((heads * n_tp + 3,)),
            dma((n_sp, n_z)),
            dma((n_sp, n_z)),
            dma((n_sp, n_z)),
            dma((n_sp, n_z)),
            dma((n_z,)),
            dma((n_z,)),
            dma((n_sp, n_z)),
            dma((n_sp, n_z)),
            dma((n_z,)),
            dma((n_z,)),
            dma((n_sp,)),
            dma((n_sp,)),
            dma((n_sp,)),
            dma((n_sp,)),
            pltpu.SemaphoreType.REGULAR,
        ],
        compiler_params=pltpu.CompilerParams(
            collective_id=2, has_side_effects=True, vmem_limit_bytes=VMEM_BYTES
        ),
        name="layer",
    )(
        lambdas,
        q,
        k,
        v,
        head_gain.reshape(1, -1),
        expert_ids.T,
        route_weights.T,
        residual,
        norm_gain.reshape(1, -1),
        out_weight.reshape(n_tp, heads, width, model),
        gate_weight,
        up_weight,
        down_weight,
    )


def shards(
    queries,
    key_pairs,
    head_values,
    lambdas,
    head_gain,
    out_weight,
    residual,
    norm_gain,
    expert_ids,
    route_weights,
    gate_weight,
    up_weight,
    down_weight,
):
    tokens_here, heads_here, pair_width = queries.shape
    value_width = head_values.shape[2]
    rows_here = residual.shape[0]
    sp_count = lax.axis_size("sp")
    tp_count = lax.axis_size("tp")
    z_count = tp_count // CORES
    route_count = expert_ids.shape[1]
    local_experts = gate_weight.shape[0]
    expert_count = local_experts * sp_count
    capacity = max(2, 4 * rows_here * route_count // (3 * expert_count))
    model_width = residual.shape[1]
    block_bytes = z_count * local_experts * capacity * model_width * 2
    if sp_count == PLANE and z_count == LAYERS and heads_here == HEADS_HERE and pair_width == value_width and (
        capacity % 16 == 0 and rows_here <= 128 and route_count == 2
        and (7 * sp_count - 1) * block_bytes <= 3 * VMEM_BYTES // 5
    ):
        return whole_layer(
            queries,
            key_pairs,
            head_values,
            lambdas,
            head_gain,
            expert_ids,
            route_weights,
            residual,
            norm_gain,
            out_weight,
            gate_weight,
            up_weight,
            down_weight,
            sp_count,
            tp_count,
            capacity,
        )
    flat_ids = expert_ids.reshape(-1)
    indicator = (flat_ids[:, None] == jnp.arange(expert_count, dtype=jnp.int32)[None, :]).astype(
        jnp.int32
    )
    ranking = jnp.sum(jnp.cumsum(indicator, axis=0) * indicator, axis=1) - 1
    turned = (flat_ids - lax.axis_index("sp") * local_experts) % expert_count
    near_slots = (turned * capacity + ranking).reshape(rows_here, route_count)
    slots = flat_ids * capacity + ranking
    meta = jnp.concatenate([near_slots.astype(jnp.float32), route_weights], axis=1).T
    meta = jnp.pad(meta, ((0, 8 - 2 * route_count), (0, -rows_here % 128)), constant_values=-1.0)
    updated, normed, zmeta = attend(
        queries,
        key_pairs,
        head_values,
        lambdas,
        head_gain,
        meta,
        residual,
        norm_gain,
        out_weight,
        sp_count,
        tp_count,
    )
    if capacity % 16 == 0 and rows_here <= 128 and route_count == 2 and (
        (7 * sp_count - 1) * block_bytes <= 3 * VMEM_BYTES // 5
    ):
        return experts(
            normed, zmeta, updated, gate_weight, up_weight, down_weight, sp_count, z_count, capacity
        )
    sources = jnp.arange(rows_here * route_count, dtype=jnp.int32) // route_count
    outgoing = (
        jnp.zeros((expert_count * capacity, model_width), jnp.bfloat16)
        .at[slots]
        .set(normed[sources])
    )
    arrived = lax.all_to_all(
        outgoing.reshape(sp_count, local_experts, capacity, model_width),
        "sp",
        split_axis=0,
        concat_axis=0,
        tiled=True,
    )
    piece_rows = lax.all_gather(arrived[None], "tp", axis=0, tiled=True)
    gate_part = jnp.einsum(
        "tsecd,edf->tsecf", piece_rows, gate_weight, preferred_element_type=jnp.float32
    )
    up_part = jnp.einsum(
        "tsecd,edf->tsecf", piece_rows, up_weight, preferred_element_type=jnp.float32
    )
    inner_rows = (jax.nn.silu(gate_part) * up_part).astype(jnp.bfloat16)
    partial_value = jnp.einsum(
        "tsecf,efd->tsecd", inner_rows, down_weight, preferred_element_type=jnp.float32
    )
    reduced = lax.psum_scatter(
        partial_value.astype(jnp.bfloat16), "tp", scatter_dimension=0, tiled=True
    )
    returned = lax.all_to_all(reduced[0], "sp", split_axis=0, concat_axis=0, tiled=True)
    picked = (
        returned.reshape(expert_count * capacity, model_width)[slots]
        .astype(jnp.float32)
        .reshape(rows_here, route_count, model_width)
    )
    moe_sum = jnp.sum(picked * route_weights[:, :, None], axis=1)
    return (updated.astype(jnp.float32) + moe_sum).astype(jnp.bfloat16)


def solution(mesh):
    placed = (
        P("sp", "tp", None),
        P("sp", "tp", None),
        P("sp", "tp", None),
        P("tp"),
        P(),
        P(),
        P(("sp", "tp"), None),
        P(),
        P(("sp", "tp"), None),
        P(("sp", "tp"), None),
        P("sp", None, "tp"),
        P("sp", None, "tp"),
        P("sp", "tp", None),
    )
    return jax.shard_map(
        shards, mesh=mesh, in_specs=placed, out_specs=P(("sp", "tp"), None), check_vma=False
    )
```

```python
import functools
import math

import jax
import jax.numpy as jnp
from jax import lax
from jax.experimental import pallas as pl
from jax.experimental.pallas import tpu as pltpu
from jax.sharding import PartitionSpec as P

MESH = pl.DeviceIdType.MESH
LOG2E = 1.4426950408889634
CORES = 2
PLANE = 4
HEADS_HERE = 2
LAYERS = 4
TWIN = 3
VMEM_BYTES = 67043328


def attend_kernel(
    n_sp,
    n_tp,
    scale,
    lam_ref,
    q_ref,
    kv_ref,
    gain_ref,
    meta_ref,
    base_ref,
    norm_ref,
    w_hbm,
    updated_ref,
    normed_ref,
    zmeta_ref,
    weight,
    gathered,
    kvbuf,
    acc,
    top,
    tot,
    att,
    kv_send,
    kv_recv,
    at_send,
    at_recv,
    me_send,
    me_recv,
    own_sem,
    w_sem,
):
    heads, tiles, wide, _ = q_ref.shape
    tile = wide // 2
    rows = base_ref.shape[0]
    n_z = n_tp // CORES
    c = lax.axis_index("sp")
    t = lax.axis_index("tp")
    load = pltpu.make_async_copy(w_hbm, weight, w_sem)
    load.start()
    barrier = pltpu.get_barrier_semaphore()
    for d in range(1, n_sp):
        pl.semaphore_signal(barrier, inc=1, device_id=((c + d) % n_sp, t), device_id_type=MESH)
    for d in range(1, n_tp):
        pl.semaphore_signal(barrier, inc=1, device_id=(c, (t + d) % n_tp), device_id_type=MESH)
    pl.semaphore_wait(barrier, n_sp + n_tp - 2)

    def kv_copy(d, h):
        return pltpu.make_async_remote_copy(
            src_ref=kv_ref.at[h],
            dst_ref=kvbuf.at[d - 1, h],
            send_sem=kv_send.at[d - 1, h],
            recv_sem=kv_recv.at[d - 1, h],
            device_id=((c + d) % n_sp, t),
            device_id_type=MESH,
        )

    def meta_copy(d):
        return pltpu.make_async_remote_copy(
            src_ref=meta_ref,
            dst_ref=zmeta_ref.at[d],
            send_sem=me_send.at[d],
            recv_sem=me_recv.at[d],
            device_id=(c, (t + CORES * d) % n_tp),
            device_id_type=MESH,
        )

    for d in range(1, n_sp):
        @pl.when(c + d < n_sp)
        def _():
            for h in range(heads):
                kv_copy(d, h).start()

    for d in range(1, n_z):
        meta_copy(d).start()
    zmeta_ref[0] = meta_ref[...]

    factor = scale * LOG2E

    def scores_of(h, i, keys):
        return (
            lax.dot_general(
                q_ref[h, i], keys, (((1,), (1,)), ((), ())), preferred_element_type=jnp.float32
            )
            * factor
        )

    for i in range(tiles):
        extent = (i + 1) * tile
        for h in range(heads):
            s = scores_of(h, i, kv_ref[h, 0, :extent])
            row = lax.rem(lax.broadcasted_iota(jnp.int32, (wide, extent), 0), tile) + i * tile
            col = lax.broadcasted_iota(jnp.int32, (wide, extent), 1)
            s = jnp.where(col <= row, s, -jnp.inf)
            high = jnp.max(s, axis=1, keepdims=True)
            p = jnp.exp2(s - high)
            top[h, i] = high
            tot[h, i] = jnp.sum(p, axis=1, keepdims=True)
            acc[h, i] = jnp.dot(
                p.astype(jnp.bfloat16), kv_ref[h, 1, :extent], preferred_element_type=jnp.float32
            )

    def span_step(step, carry):
        for h in range(heads):
            kv_copy(step, h).wait_recv()

        def tile_step(i, inner):
            for h in range(heads):
                s = scores_of(h, i, kvbuf[step - 1, h, 0])
                before = top[h, i]
                high = jnp.maximum(before, jnp.max(s, axis=1, keepdims=True))
                p = jnp.exp2(s - high)
                decay = jnp.exp2(before - high)
                top[h, i] = high
                tot[h, i] = tot[h, i] * decay + jnp.sum(p, axis=1, keepdims=True)
                acc[h, i] = acc[h, i] * decay + jnp.dot(
                    p.astype(jnp.bfloat16),
                    kvbuf[step - 1, h, 1],
                    preferred_element_type=jnp.float32,
                )
            return inner

        return lax.fori_loop(0, tiles, tile_step, carry)

    lax.fori_loop(1, c + 1, span_step, 0)

    for h in range(heads):
        width = acc.shape[3]
        for i in range(tiles):
            both = acc[h, i] / tot[h, i]
            mixed = both[:tile] - lam_ref[h] * both[tile:]
            mean = jnp.mean(mixed * mixed, axis=1, keepdims=True)
            normed = mixed * lax.rsqrt(mean + 1e-06) * gain_ref[...]
            att[i * tile : (i + 1) * tile, h * width : (h + 1) * width] = normed.astype(att.dtype)

    def att_copy(d):
        to = (t + d) % n_tp
        return pltpu.make_async_remote_copy(
            src_ref=att.at[pl.ds(pl.multiple_of(to * rows, rows), rows)],
            dst_ref=gathered.at[t],
            send_sem=at_send.at[d],
            recv_sem=at_recv.at[d],
            device_id=(c, to),
            device_id_type=MESH,
        )

    for d in range(1, n_tp):
        att_copy(d).start()
    own = pltpu.make_async_copy(
        att.at[pl.ds(pl.multiple_of(t * rows, rows), rows)], gathered.at[t], own_sem
    )
    own.start()
    own.wait()
    load.wait()
    span = att.shape[1]
    projected = jnp.zeros(base_ref.shape, jnp.float32)
    for d in range(n_tp):
        if d:
            att_copy(d).wait_recv()
        source = (t - d + n_tp) % n_tp
        projected = projected + jnp.dot(
            gathered[source],
            weight[pl.ds(pl.multiple_of(source * span, span), span), :],
            preferred_element_type=jnp.float32,
        )
    updated = (base_ref[...].astype(jnp.float32) + projected).astype(jnp.bfloat16)
    updated_ref[...] = updated
    widened = updated.astype(jnp.float32)
    mean = jnp.mean(widened * widened, axis=1, keepdims=True)
    normed_ref[...] = (widened * lax.rsqrt(mean + 1e-06) * norm_ref[...]).astype(jnp.bfloat16)
    for d in range(1, n_tp):
        att_copy(d).wait_send()
    for d in range(1, n_z):
        meta_copy(d).wait()
    for d in range(1, n_sp):
        @pl.when(c + d < n_sp)
        def _():
            for h in range(heads):
                kv_copy(d, h).wait_send()


def attend(queries, key_pairs, head_values, lambdas, head_gain, meta, residual, norm_gain, out_weight, n_sp, n_tp):
    tokens, heads, pair = queries.shape
    rows = residual.shape[0]
    width = head_values.shape[2]
    half = pair // 2
    tile = math.gcd(tokens, 256)
    tiles = tokens // tile
    first = (jnp.arange(pair) < half)[None, :]
    q = jnp.transpose(queries, (1, 0, 2)).reshape(heads, tiles, 1, tile, pair)
    sides = jnp.stack([first, ~first])
    q = jnp.where(sides, q, jnp.zeros((), q.dtype)).reshape(heads, tiles, 2 * tile, pair)
    kv = jnp.transpose(jnp.stack([key_pairs, head_values]), (2, 0, 1, 3))
    dma = pltpu.SemaphoreType.DMA
    vmem = pl.BlockSpec(memory_space=pltpu.VMEM)
    n_z = n_tp // CORES
    return pl.pallas_call(
        functools.partial(attend_kernel, n_sp, n_tp, half ** (-0.5)),
        out_shape=(
            jax.ShapeDtypeStruct(residual.shape, jnp.bfloat16),
            jax.ShapeDtypeStruct(residual.shape, jnp.bfloat16),
            jax.ShapeDtypeStruct((n_z,) + meta.shape, meta.dtype),
        ),
        in_specs=[pl.BlockSpec(memory_space=pltpu.SMEM)] + [vmem] * 6
        + [pl.BlockSpec(memory_space=pl.ANY)],
        out_specs=(vmem, vmem, vmem),
        scratch_shapes=[
            pltpu.VMEM(out_weight.shape, out_weight.dtype),
            pltpu.VMEM((n_tp, rows, heads * width), jnp.bfloat16),
            pltpu.VMEM((n_sp - 1,) + kv.shape, kv.dtype),
            pltpu.VMEM((heads, tiles, 2 * tile, width), jnp.float32),
            pltpu.VMEM((heads, tiles, 2 * tile, 1), jnp.float32),
            pltpu.VMEM((heads, tiles, 2 * tile, 1), jnp.float32),
            pltpu.VMEM((tokens, heads * width), jnp.bfloat16),
            dma((n_sp - 1, heads)),
            dma((n_sp - 1, heads)),
            dma((n_tp,)),
            dma((n_tp,)),
            dma((n_z,)),
            dma((n_z,)),
            dma,
            dma,
        ],
        compiler_params=pltpu.CompilerParams(
            collective_id=0, has_side_effects=True, vmem_limit_bytes=48 * 1024 * 1024
        ),
        name="attend",
    )(lambdas, q, kv, head_gain.reshape(1, -1), meta, residual, norm_gain.reshape(1, -1), out_weight)


def experts_kernel(
    n_sp,
    n_z,
    x_ref,
    meta_ref,
    base_ref,
    gate_hbm,
    up_hbm,
    down_hbm,
    out_ref,
    gate,
    up,
    down,
    zrows,
    pack,
    arrived,
    psend,
    own,
    precv,
    ret,
    zsend,
    zret,
    mine,
    w_sem,
    zs_send,
    zs_recv,
    ps_send,
    ps_recv,
    fw_send,
    fw_recv,
    pp_send,
    pp_recv,
    rt_send,
    rt_recv,
    zr_send,
    zr_recv,
):
    rows, model = x_ref.shape
    local, cap = pack.shape[2], pack.shape[3]
    slots = n_sp * local * cap
    c = lax.axis_index("sp")
    t = lax.axis_index("tp")
    n_tp = n_z * CORES
    core = t % CORES
    partner = (c, t + 1 - 2 * core)
    loads = [
        pltpu.make_async_copy(a, b, w_sem.at[i])
        for i, (a, b) in enumerate(((gate_hbm, gate), (up_hbm, up), (down_hbm, down)))
    ]
    for load in loads:
        load.start()

    def column(d):
        return ((c + d) % n_sp, t)

    def layer(d):
        return (c, (t + CORES * d) % n_tp)

    barrier = pltpu.get_barrier_semaphore()
    for d in range(1, n_sp):
        pl.semaphore_signal(barrier, inc=1, device_id=column(d), device_id_type=MESH)
    for d in range(1, n_z):
        pl.semaphore_signal(barrier, inc=1, device_id=layer(d), device_id_type=MESH)
    pl.semaphore_signal(barrier, inc=1, device_id=partner, device_id_type=MESH)
    pl.semaphore_wait(barrier, n_sp + n_z - 1)

    def remote(src, dst, send, recv, target):
        return pltpu.make_async_remote_copy(
            src_ref=src,
            dst_ref=dst,
            send_sem=send,
            recv_sem=recv,
            device_id=target,
            device_id_type=MESH,
        )

    def z_copy(d):
        return remote(x_ref, zrows.at[d - 1], zs_send.at[d], zs_recv.at[d], layer(d))

    def pack_copy(d, s):
        return remote(
            pack.at[s, d - 1], arrived.at[0, s, d], ps_send.at[d, s], ps_recv.at[d, s], column(d)
        )

    def share_copy(d, s):
        return remote(
            arrived.at[0, s, d], arrived.at[1, s, d], fw_send.at[d, s], fw_recv.at[d, s], partner
        )

    def pair_copy(s):
        return remote(psend.at[s], precv.at[s], pp_send.at[s], pp_recv.at[s], partner)

    def back_copy(d, s):
        return remote(
            own.at[s, d], ret.at[s, d], rt_send.at[d, s], rt_recv.at[d, s], column(n_sp - d)
        )

    def z_back(d):
        return remote(
            zsend.at[d], zret.at[d], zr_send.at[d], zr_recv.at[d], layer(n_z - d)
        )

    for d in range(1, n_z):
        z_copy(d).start()

    def route_hits(s, r):
        target = lax.broadcasted_iota(jnp.int32, (slots, rows), 0).astype(jnp.float32)
        return target == meta_ref[s, r : r + 1, :rows]

    def pack_rows(s):
        if s:
            z_copy(s).wait_recv()
        hits = route_hits(s, 0) | route_hits(s, 1)
        pick = jnp.where(hits, 1.0, 0.0).astype(jnp.bfloat16)
        source = x_ref[...] if s == 0 else zrows[s - 1]
        packed = (
            jnp.dot(pick, source, preferred_element_type=jnp.float32)
            .astype(jnp.bfloat16)
            .reshape(n_sp, local, cap, model)
        )
        for d in range(1, n_sp):
            pack[s, d - 1] = packed[d]
            pack_copy(d, s).start()
        arrived[0, s, 0] = packed[0]
        share_copy(0, s).start()

    def run_experts(s):
        for d in range(1, n_sp):
            pack_copy(d, s).wait_recv()
            share_copy(d, s).start()
        for d in range(n_sp):
            share_copy(d, s).wait_recv()

        def expert_step(e, carry):
            x = arrived[:, s, :, e].reshape(2 * n_sp * cap, model)
            gated = jnp.dot(x, gate[e], preferred_element_type=jnp.float32)
            lifted = jnp.dot(x, up[e], preferred_element_type=jnp.float32)
            inner = (gated / (1.0 + jnp.exp(-gated)) * lifted).astype(jnp.bfloat16)
            y = jnp.dot(inner, down[e], preferred_element_type=jnp.float32)
            y = y.astype(jnp.bfloat16).reshape(2, n_sp, cap, model)
            own[s, :, e] = y[0]
            psend[s, :, e] = y[1]
            return carry

        lax.fori_loop(0, local, expert_step, 0)
        pair_copy(s).start()

    def reduce_pair(s):
        pair_copy(s).wait_recv()
        for d in list(range(1, n_sp)) + [0]:
            total = own[s, d].astype(jnp.float32) + precv[s, d].astype(jnp.float32)
            total = total.astype(jnp.bfloat16)
            if d == 0:
                ret[s, 0] = total
            else:
                own[s, d] = total
                back_copy(d, s).start()

    def mix_rows(s):
        for d in range(1, n_sp):
            back_copy(d, s).wait_recv()
        mixing = jnp.where(route_hits(s, 0), meta_ref[s, 2:3, :rows], 0.0) + jnp.where(
            route_hits(s, 1), meta_ref[s, 3:4, :rows], 0.0
        )
        high = mixing.astype(jnp.bfloat16)
        low = (mixing - high.astype(jnp.float32)).astype(jnp.bfloat16)
        back = ret[s].reshape(slots, model)
        numbers = (((0,), (0,)), ((), ()))
        merged = lax.dot_general(
            high, back, numbers, preferred_element_type=jnp.float32
        ) + lax.dot_general(low, back, numbers, preferred_element_type=jnp.float32)
        if s:
            zsend[s] = merged.astype(jnp.bfloat16)
            z_back(s).start()
        else:
            mine[...] = merged

    pack_rows(0)
    for load in loads:
        load.wait()
    if n_z > 1:
        pack_rows(1)
    for s in range(n_z):
        run_experts(s)
        if s + 2 < n_z:
            pack_rows(s + 2)
        elif s + 2 - n_z < n_z - 2:
            mix_rows(s + 2 - n_z)
        reduce_pair(s)
    for s in range(max(0, n_z - 2), n_z):
        mix_rows(s)
    merged = mine[...]
    for s in range(1, n_z):
        z_back(s).wait_recv()
        merged = merged + zret[s].astype(jnp.float32)
    out_ref[...] = (base_ref[...].astype(jnp.float32) + merged).astype(jnp.bfloat16)

    for d in range(1, n_z):
        z_copy(d).wait_send()
        z_back(d).wait_send()
    for s in range(n_z):
        for d in range(n_sp):
            if d:
                pack_copy(d, s).wait_send()
                back_copy(d, s).wait_send()
            share_copy(d, s).wait_send()
        pair_copy(s).wait_send()


def experts(normed, zmeta, updated, gate_weight, up_weight, down_weight, n_sp, n_z, cap):
    rows, model = normed.shape
    local = gate_weight.shape[0]
    dma = pltpu.SemaphoreType.DMA
    vmem = pl.BlockSpec(memory_space=pltpu.VMEM)
    hbm = pl.BlockSpec(memory_space=pl.ANY)
    block = (local, cap, model)

    def buffer(*shape):
        return pltpu.VMEM(shape, jnp.bfloat16)

    return pl.pallas_call(
        functools.partial(experts_kernel, n_sp, n_z),
        out_shape=jax.ShapeDtypeStruct((rows, model), jnp.bfloat16),
        in_specs=[vmem] * 3 + [hbm] * 3,
        out_specs=vmem,
        scratch_shapes=[
            buffer(*gate_weight.shape),
            buffer(*up_weight.shape),
            buffer(*down_weight.shape),
            buffer(n_z - 1, rows, model),
            buffer(n_z, n_sp - 1, *block),
            buffer(2, n_z, n_sp, *block),
            buffer(n_z, n_sp, *block),
            buffer(n_z, n_sp, *block),
            buffer(n_z, n_sp, *block),
            buffer(n_z, n_sp, *block),
            buffer(n_z, rows, model),
            buffer(n_z, rows, model),
            pltpu.VMEM((rows, model), jnp.float32),
            dma((3,)),
            dma((n_z,)),
            dma((n_z,)),
            dma((n_sp, n_z)),
            dma((n_sp, n_z)),
            dma((n_sp, n_z)),
            dma((n_sp, n_z)),
            dma((n_z,)),
            dma((n_z,)),
            dma((n_sp, n_z)),
            dma((n_sp, n_z)),
            dma((n_z,)),
            dma((n_z,)),
        ],
        compiler_params=pltpu.CompilerParams(
            collective_id=1, has_side_effects=True, vmem_limit_bytes=VMEM_BYTES
        ),
        name="experts",
    )(normed, zmeta, updated, gate_weight, up_weight, down_weight)


def layer_kernel(
    n_sp,
    n_tp,
    scale,
    lam_ref,
    raw_ref,
    k_ref,
    v_ref,
    gain_ref,
    ids_ref,
    mix_ref,
    base_ref,
    norm_ref,
    w_hbm,
    gate_hbm,
    up_hbm,
    down_hbm,
    out_ref,
    q_ref,
    gathered,
    kvbuf,
    acc,
    top,
    att,
    bases,
    updated,
    x_ref,
    zmeta,
    gate,
    up,
    down,
    zrows,
    pack,
    arrived,
    psend,
    own,
    precv,
    ret,
    zsend,
    zret,
    fold,
    parts,
    kv_send,
    kv_recv,
    at_send,
    at_recv,
    ar_send,
    ar_recv,
    ba_send,
    ba_recv,
    me_send,
    me_recv,
    w_sem,
    ps_send,
    ps_recv,
    fw_send,
    fw_recv,
    pp_send,
    pp_recv,
    rt_send,
    rt_recv,
    zr_send,
    zr_recv,
    tw_send,
    tw_recv,
    fo_send,
    fo_recv,
    go,
):
    heads, tiles, wide, _ = q_ref.shape
    tile = wide // 2
    rows, model = base_ref.shape
    width = v_ref.shape[2]
    n_z = n_tp // CORES
    local, cap = pack.shape[2], pack.shape[3]
    slots = n_sp * local * cap
    span = n_sp * local * cap
    c = lax.axis_index("sp")
    t = lax.axis_index("tp")
    core = t % CORES
    partner = (c, t + 1 - 2 * core)

    def column(d):
        return ((c + d) % n_sp, t)

    z = t // CORES
    twin_z = z + 1 - 2 * (z % 2)
    far_z = (z + n_z // 2) % n_z
    twin = (c, twin_z * CORES + core)
    far = [None, (c, far_z * CORES + core), (c, (far_z + 1 - 2 * (far_z % 2)) * CORES + core)]

    weight = (psend, precv)
    loads = [
        pltpu.make_async_copy(a, b, w_sem.at[i])
        for i, (a, b) in enumerate(
            [
                (w_hbm.at[source, h], weight[h].at[source * width : (source + 1) * width])
                for h in range(heads)
                for source in range(n_tp)
            ]
            + [(gate_hbm, gate), (up_hbm, up), (down_hbm, down)]
        )
    ]
    for load in loads:
        load.start()
    barrier = pltpu.get_barrier_semaphore()
    for d in range(1, n_sp):
        pl.semaphore_signal(barrier, inc=1, device_id=column(d), device_id_type=MESH)
    for d in range(1, n_tp):
        pl.semaphore_signal(barrier, inc=1, device_id=(c, (t + d) % n_tp), device_id_type=MESH)
    pl.semaphore_wait(barrier, n_sp + n_tp - 2)

    def remote(src, dst, send, recv, target):
        return pltpu.make_async_remote_copy(
            src_ref=src,
            dst_ref=dst,
            send_sem=send,
            recv_sem=recv,
            device_id=target,
            device_id_type=MESH,
        )

    def kv_copies(slot, source, h, to, mine_too, parts=(0, 1)):
        return [
            remote(
                (k_ref, v_ref)[part].at[h] if mine_too else kvbuf.at[source, h, part],
                kvbuf.at[source, h, part],
                kv_send.at[slot, part],
                kv_recv.at[source, h, part],
                (to, t),
            )
            for part in parts
        ]

    def kv_wait(source, h):
        for part in range(2):
            remote(
                kvbuf.at[source, h, part],
                kvbuf.at[source, h, part],
                kv_send.at[0, part],
                kv_recv.at[source, h, part],
                partner,
            ).wait_recv()

    first_sends = [
        kv_copies(0, 0, 0, 2, True)
        + kv_copies(1, 0, 1, 1, True)
        + kv_copies(2, 0, 1, 2, True)
        + kv_copies(3, 0, 0, 1, True),
        kv_copies(0, 1, 0, 3, True) + kv_copies(1, 1, 1, 0, True) + kv_copies(2, 1, 1, 3, True),
        kv_copies(0, 2, 0, 3, True) + kv_copies(1, 2, 1, 3, True, (0,)),
        [],
    ]
    relayed = [(1, 1), (0, 1), (0, 0), (1, 0)]
    late_sends = [
        kv_copies(4, 1, 1, 2, False),
        kv_copies(3, 0, 1, 3, False),
        kv_copies(2, 0, 0, 3, False) + kv_copies(1, 2, 1, 3, True, (1,)),
        kv_copies(0, 1, 0, 2, False),
    ]

    def meta_copy(d):
        return remote(zmeta.at[0], zmeta.at[d], me_send.at[d], me_recv.at[d], far[d])

    for k in range(n_sp):
        @pl.when(c == k)
        def _():
            for copy in first_sends[k]:
                copy.start()

    def base_copy(d, side):
        columns = slice(side * (model // 2), (side + 1) * (model // 2))
        return remote(
            base_ref.at[:, columns] if d == 1 else bases.at[0, :, columns],
            bases.at[d - 1, :, columns],
            ba_send.at[d - 1, side],
            ba_recv.at[d - 1, side],
            far[1] if d == 1 else twin,
        )

    def pass_base(side):
        base_copy(1, side).wait_recv()
        base_copy(2, side).start()

    for side in range(2):
        base_copy(1, side).start()

    experts = n_sp * local
    shape = (experts, rows)
    names = lax.broadcasted_iota(jnp.int32, shape, 0)
    named = [names == ids_ref[r : r + 1, :] for r in range(2)]
    chosen = jnp.where(named[0] | named[1], 1.0, 0.0).astype(jnp.bfloat16)
    earlier = lax.broadcasted_iota(jnp.int32, (rows, rows), 0) < lax.broadcasted_iota(
        jnp.int32, (rows, rows), 1
    )
    ranks = jnp.dot(
        chosen, jnp.where(earlier, 1.0, 0.0).astype(jnp.bfloat16), preferred_element_type=jnp.float32
    )
    zmeta[0] = jnp.full(zmeta.shape[1:], -1.0, jnp.float32)
    for r in range(2):
        turned = ids_ref[r : r + 1, :] - c * local
        turned = jnp.where(turned < 0, turned + experts, turned)
        rank = jnp.sum(jnp.where(named[r], ranks, 0.0), axis=0, keepdims=True)
        zmeta[0, r : r + 1, :rows] = (turned * cap).astype(jnp.float32) + rank
        zmeta[0, 2 + r : 3 + r, :rows] = mix_ref[r : r + 1, :]
    for d in (1, 2):
        meta_copy(d).start()

    side = lax.broadcasted_iota(jnp.int32, (tile, raw_ref.shape[2]), 1) < raw_ref.shape[2] // 2
    for h in range(heads):
        for i in range(tiles):
            part = raw_ref[h, i * tile : (i + 1) * tile]
            q_ref[h, i, :tile] = jnp.where(side, part, jnp.zeros_like(part))
            q_ref[h, i, tile:] = jnp.where(side, jnp.zeros_like(part), part)

    factor = scale * LOG2E

    def scores_of(h, i, keys):
        return (
            lax.dot_general(
                q_ref[h, i], keys, (((1,), (1,)), ((), ())), preferred_element_type=jnp.float32
            )
            * factor
        )

    def with_ones(values):
        return jnp.concatenate([values, jnp.ones_like(values)], axis=1)

    for i in range(tiles):
        extent = (i + 1) * tile
        for h in range(heads):
            s = scores_of(h, i, k_ref[h, :extent])
            row = lax.rem(lax.broadcasted_iota(jnp.int32, (wide, extent), 0), tile) + i * tile
            col = lax.broadcasted_iota(jnp.int32, (wide, extent), 1)
            s = jnp.where(col <= row, s, -jnp.inf)
            high = jnp.max(s, axis=1, keepdims=True)
            p = jnp.exp2(s - high)
            top[h, i] = high
            acc[h, i] = jnp.dot(
                p.astype(jnp.bfloat16),
                with_ones(v_ref[h, :extent]),
                preferred_element_type=jnp.float32,
            )

    for k in range(n_sp):
        @pl.when(c == k)
        def _():
            kv_wait(*relayed[k])
            for copy in late_sends[k]:
                copy.start()

    pass_base(0)

    def order_of(orders):
        codes = [sum((2 * s + h) * 8**j for j, (s, h) in enumerate(o)) for o in orders]
        code, count = jnp.int32(codes[0]), jnp.int32(len(orders[0]))
        for k in range(1, n_sp):
            code = jnp.where(c == k, codes[k], code)
            count = jnp.where(c == k, len(orders[k]), count)
        return code, count

    def absorb(orders, waited, passing=False):
        code, count = order_of(orders)

        def piece_step(j, code):
            piece = code % 8
            source, h = piece // 2, piece % 2

            @pl.when(j >= waited)
            def _():
                kv_wait(source, h)

            if passing:

                @pl.when(j == count - 1)
                def _():
                    pass_base(1)

            keys, values = kvbuf[source, h, 0], with_ones(kvbuf[source, h, 1])
            results = []
            for i in range(tiles):
                s = scores_of(h, i, keys)
                before = top[h, i]
                high = jnp.maximum(before, jnp.max(s, axis=1, keepdims=True))
                p = jnp.exp2(s - high)
                decay = jnp.exp2(before - high)
                summed = acc[h, i] * decay + jnp.dot(
                    p.astype(jnp.bfloat16), values, preferred_element_type=jnp.float32
                )
                results.append((high, summed))
            for i in range(tiles):
                top[h, i], acc[h, i] = results[i]
            return code // 8

        lax.fori_loop(0, count, piece_step, code)

    half = n_z // 2

    def block_rows(b, to_z, to_core):
        layer = to_z if b == 0 else (to_z + half) % n_z
        if b == 2:
            layer = layer + 1 - 2 * (layer % 2)
        return pl.ds(pl.multiple_of((layer * CORES + to_core) * rows, rows), rows)

    here = pl.ds(pl.multiple_of(t * width, width), width)

    def att_copy(h, b, d):
        to = (t + d) % n_tp
        return remote(
            att.at[h, block_rows(b, to // CORES, to % CORES)],
            gathered.at[h, b, :, here],
            at_send.at[h, b, d],
            at_recv.at[h, b, d],
            (c, to),
        )

    def relay_copy(h):
        side = half * CORES * width
        across = pl.ds(pl.multiple_of((1 - z // half) * side, side), side)
        return remote(
            gathered.at[h, 1, :, across],
            gathered.at[h, 2, :, across],
            ar_send.at[h],
            ar_recv.at[h],
            twin,
        )

    def near(d):
        return ((t + d) % n_tp) // CORES // half == z // half

    def finish(h):
        for i in range(tiles):
            both = acc[h, i, :, :width] / acc[h, i, :, width:]
            mixed = both[:tile] - lam_ref[h] * both[tile:]
            mean = jnp.mean(mixed * mixed, axis=1, keepdims=True)
            normed = mixed * lax.rsqrt(mean + 1e-06) * gain_ref[...]
            att[h, i * tile : (i + 1) * tile] = normed.astype(att.dtype)
        for d in range(1, n_tp):
            att_copy(h, 0, d).start()
        for b in range(3):
            gathered[h, b, :, here] = att[h, block_rows(b, z, core)]

    def finish_far():
        for h in range(heads):
            for d in range(1, n_tp):
                att_copy(h, 1, d).start()
        for h in range(heads):
            for d in range(1, n_tp):

                @pl.when(near(d))
                def _():
                    att_copy(h, 2, d).start()


    def await_rows(h, b):
        for d in range(1, n_tp):
            if b < 2:
                att_copy(h, b, d).wait_recv()
            else:

                @pl.when(near(n_tp - d))
                def _():
                    att_copy(h, b, d).wait_recv()

        if b == 1:
            relay_copy(h).start()
        if b == 2:
            relay_copy(h).wait_recv()

    def project(h, b):
        return jnp.dot(
            gathered[h, b], weight[h][: n_tp * width], preferred_element_type=jnp.float32
        )

    def normalize(base, projected):
        new = (base.astype(jnp.float32) + projected).astype(jnp.bfloat16)
        widened = new.astype(jnp.float32)
        mean = jnp.mean(widened * widened, axis=1, keepdims=True)
        return new, (widened * lax.rsqrt(mean + 1e-06) * norm_ref[...]).astype(jnp.bfloat16)

    def far_rows(b):
        await_rows(0, b)
        parts[b] = project(0, b)
        await_rows(1, b)
        if b == 2:
            for part in range(2):
                base_copy(2, part).wait_recv()
        _, normed = normalize(bases[b - 1], parts[b] + project(1, b))
        zrows[b - 1] = normed

    absorb([[], [(0, 1), (0, 0)], [(0, 0), (0, 1), (1, 0)], [(1, 0), (2, 0), (1, 1), (0, 0)]], 1, True)

    @pl.when(c == 0)
    def _():
        pass_base(1)

    finish(0)
    absorb([[], [], [(1, 1)], [(2, 1), (0, 1)]], 0)

    @pl.when(c == n_sp - 1)
    def _():
        for d in range(1, n_sp):
            pl.semaphore_signal(go, inc=1, device_id=column(d), device_id_type=MESH)

    finish(1)
    finish_far()
    for load in loads[: heads * n_tp]:
        load.wait()
    await_rows(0, 0)
    parts[0] = project(0, 0)
    await_rows(1, 0)
    new, normed = normalize(base_ref[...], parts[0] + project(1, 0))
    updated[...] = new
    x_ref[...] = normed

    def pack_copy(d, s):
        return remote(
            pack.at[s, d - 1], arrived.at[0, s, d], ps_send.at[d, s], ps_recv.at[d, s], column(d)
        )

    def share_copy(d, s):
        return remote(
            arrived.at[0, s, d], arrived.at[1, s, d], fw_send.at[d, s], fw_recv.at[d, s], partner
        )

    def twin_copy(d):
        return remote(
            arrived.at[0, 0, d], arrived.at[0, TWIN, d], tw_send.at[d], tw_recv.at[d], twin
        )

    def pair_copy(s):
        block = pl.ds(s * span, span)
        return remote(psend.at[block], precv.at[block], pp_send.at[s], pp_recv.at[s], partner)

    def fold_copy(d):
        return remote(own.at[TWIN, d], fold.at[d], fo_send.at[d], fo_recv.at[d], twin)

    def columns_of(part):
        return slice(part * (model // 2), (part + 1) * (model // 2))

    def back_copy(d, s, part):
        return remote(
            own.at[s, d, :, :, columns_of(part)],
            ret.at[s, d, :, :, columns_of(part)],
            rt_send.at[d, s, part],
            rt_recv.at[d, s, part],
            column(n_sp - d),
        )

    def z_part(d, part, target):
        return remote(
            zsend.at[d - 1, :, columns_of(part)],
            zret.at[d - 1, :, columns_of(part)],
            zr_send.at[d, part],
            zr_recv.at[d, part],
            target,
        )

    def z_back(d, part):
        return z_part(d, part, far[d])

    def z_join(part):
        return remote(
            zsend.at[0, :, columns_of(part)],
            zret.at[0, :, columns_of(part)],
            zr_send.at[0, part],
            zr_recv.at[0, part],
            twin,
        )

    outer = (z == 0) | (z == n_z - 1)
    for d in (1, 2):
        meta_copy(d).wait()

    def route_hits(s, r):
        target = lax.broadcasted_iota(jnp.int32, (slots, rows), 0).astype(jnp.float32)
        return target == zmeta[s, r : r + 1, :rows]

    def pack_rows(s):
        hits = route_hits(s, 0) | route_hits(s, 1)
        pick = jnp.where(hits, 1.0, 0.0).astype(jnp.bfloat16)
        source = x_ref[...] if s == 0 else zrows[s - 1]
        packed = (
            jnp.dot(pick, source, preferred_element_type=jnp.float32)
            .astype(jnp.bfloat16)
            .reshape(n_sp, local, cap, model)
        )
        if s == 0:
            arrived[0, 0, 0] = packed[0]
            twin_copy(0).start()
        for d in range(1, n_sp):
            pack[s, d - 1] = packed[d]
            pack_copy(d, s).start()
        if s:
            arrived[0, s, 0] = packed[0]
        share_copy(0, s).start()

    def rows_here(s):
        for d in range(n_sp):
            if s == TWIN:
                twin_copy(d).wait_recv()
            elif s and d:
                pack_copy(d, s).wait_recv()
            if s == TWIN or d:
                share_copy(d, s).start()
        for d in range(n_sp):
            share_copy(d, s).wait_recv()

    def run_experts(s):
        rows_here(s)

        def expert_step(e, carry):
            x = arrived[:, s, :, e].reshape(2 * n_sp * cap, model)
            gated = jnp.dot(x, gate[e], preferred_element_type=jnp.float32)
            lifted = jnp.dot(x, up[e], preferred_element_type=jnp.float32)
            inner = (gated / (1.0 + jnp.exp(-gated)) * lifted).astype(jnp.bfloat16)
            y = jnp.dot(inner, down[e], preferred_element_type=jnp.float32)
            y = y.astype(jnp.bfloat16).reshape(2, n_sp, cap, model)
            own[s, :, e] = y[0]
            for d in range(n_sp):
                place = pl.multiple_of(s * span + (d * local + e) * cap, cap)
                psend[pl.ds(place, cap)] = y[1, d]
            return carry

        lax.fori_loop(0, local, expert_step, 0)
        pair_copy(s).start()

    def reduce_pair(s):
        pair_copy(s).wait_recv()
        for d in list(range(1, n_sp)) + [0]:
            other = precv[s * span + d * local * cap : s * span + (d + 1) * local * cap]
            total = own[s, d].astype(jnp.float32) + other.reshape(local, cap, model).astype(
                jnp.float32
            )
            if s == 0:
                fold_copy(d).wait_recv()
                total = total + fold[d].astype(jnp.float32)
            total = total.astype(jnp.bfloat16)
            if s == TWIN:
                own[s, d] = total
                if d in (1, 2):
                    fold_copy(d).start()
                else:

                    @pl.when(jnp.logical_not(outer))
                    def _():
                        fold_copy(d).start()

            elif d == 0:
                ret[s, 0] = total
            else:
                own[s, d] = total
                back_copy(d, s, 0).start()
                if s == 0:
                    back_copy(d, s, 1).start()
        if s in (1, 2):
            for d in range(1, n_sp):
                back_copy(d, s, 1).start()

    def mix_rows(s, part):
        for d in range(1, n_sp):
            back_copy(d, s, part).wait_recv()
        columns = columns_of(part)
        mixing = jnp.where(route_hits(s, 0), zmeta[s, 2:3, :rows], 0.0) + jnp.where(
            route_hits(s, 1), zmeta[s, 3:4, :rows], 0.0
        )
        high = mixing.astype(jnp.bfloat16)
        low = (mixing - high.astype(jnp.float32)).astype(jnp.bfloat16)
        back = ret[s, :, :, :, columns].reshape(slots, model // 2)
        numbers = (((0,), (0,)), ((), ()))
        merged = lax.dot_general(
            high, back, numbers, preferred_element_type=jnp.float32
        ) + lax.dot_general(low, back, numbers, preferred_element_type=jnp.float32)
        if s == 1:
            zsend[0, :, columns] = merged.astype(jnp.bfloat16)

            @pl.when(outer)
            def _():
                z_join(part).start()

            @pl.when(jnp.logical_not(outer))
            def _():
                z_back(1, part).start()

        if s == 2:
            parts[0, :, columns] = merged

            @pl.when(jnp.logical_not(outer))
            def _():
                z_join(part).wait_recv()
                parts[0, :, columns] = parts[0, :, columns] + zret[0, :, columns].astype(jnp.float32)

            zsend[1, :, columns] = parts[0, :, columns].astype(jnp.bfloat16)
            z_back(2, part).start()
        return merged

    @pl.when(c != n_sp - 1)
    def _():
        pl.semaphore_wait(go, 1)

    pack_rows(0)
    for load in loads[heads * n_tp :]:
        load.wait()
    far_rows(1)
    pack_rows(1)
    for d in range(1, n_sp):
        pack_copy(d, 0).wait_recv()
        twin_copy(d).start()
    far_rows(2)
    pack_rows(2)
    run_experts(0)
    run_experts(1)
    reduce_pair(1)
    run_experts(TWIN)
    reduce_pair(TWIN)
    run_experts(2)
    reduce_pair(2)
    mix_rows(1, 0)
    mix_rows(1, 1)

    @pl.when(outer)
    def _():
        for d in (n_sp - 1, 0):
            fold_copy(d).start()

    mix_rows(2, 0)
    mix_rows(2, 1)
    reduce_pair(0)
    parts[0] = updated[...].astype(jnp.float32)
    for part in range(2):
        columns = columns_of(part)

        @pl.when(outer)
        def _():
            z_back(1, part).wait_recv()
            parts[0, :, columns] = parts[0, :, columns] + zret[0, :, columns].astype(jnp.float32)

        z_back(2, part).wait_recv()
        parts[0, :, columns] = parts[0, :, columns] + zret[1, :, columns].astype(jnp.float32)
    for part in range(2):
        columns = columns_of(part)
        out_ref[:, columns] = (parts[0, :, columns] + mix_rows(0, part)).astype(jnp.bfloat16)

    for k in range(n_sp):
        @pl.when(c == k)
        def _():
            for copy in first_sends[k] + late_sends[k]:
                copy.wait_send()

    for h in range(heads):
        for d in range(1, n_tp):
            for b in range(2):
                att_copy(h, b, d).wait_send()

            @pl.when(near(d))
            def _():
                att_copy(h, 2, d).wait_send()

        relay_copy(h).wait_send()
    for d in (1, 2):
        for side in range(2):
            base_copy(d, side).wait_send()
    for part in range(2):

        @pl.when(outer)
        def _():
            z_join(part).wait_send()

        @pl.when(jnp.logical_not(outer))
        def _():
            z_back(1, part).wait_send()

        z_back(2, part).wait_send()
    for s in range(n_z):
        for d in range(n_sp):
            if d and s != TWIN:
                pack_copy(d, s).wait_send()
                for part in range(2):
                    back_copy(d, s, part).wait_send()
            share_copy(d, s).wait_send()
        pair_copy(s).wait_send()
    for d in range(n_sp):
        twin_copy(d).wait_send()
        fold_copy(d).wait_send()


def whole_layer(
    queries,
    key_pairs,
    head_values,
    lambdas,
    head_gain,
    expert_ids,
    route_weights,
    residual,
    norm_gain,
    out_weight,
    gate_weight,
    up_weight,
    down_weight,
    n_sp,
    n_tp,
    cap,
):
    tokens, heads, pair = queries.shape
    rows, model = residual.shape
    width = head_values.shape[2]
    local = gate_weight.shape[0]
    n_z = n_tp // CORES
    tile = math.gcd(tokens, 256)
    tiles = tokens // tile
    q, k, v = (jnp.transpose(x, (1, 0, 2)) for x in (queries, key_pairs, head_values))
    dma = pltpu.SemaphoreType.DMA
    vmem = pl.BlockSpec(memory_space=pltpu.VMEM)
    hbm = pl.BlockSpec(memory_space=pl.ANY)
    block = (local, cap, model)
    flat = max(n_tp * width, n_z * n_sp * local * cap)

    def buffer(*shape):
        return pltpu.VMEM(shape, jnp.bfloat16)

    def single(*shape):
        return pltpu.VMEM(shape, jnp.float32)

    return pl.pallas_call(
        functools.partial(layer_kernel, n_sp, n_tp, (pair // 2) ** (-0.5)),
        out_shape=jax.ShapeDtypeStruct((rows, model), jnp.bfloat16),
        in_specs=[pl.BlockSpec(memory_space=pltpu.SMEM)] + [vmem] * 8 + [hbm] * 4,
        out_specs=vmem,
        scratch_shapes=[
            buffer(heads, tiles, 2 * tile, pair),
            buffer(heads, 3, rows, n_tp * width),
            buffer(n_sp - 1, heads, 2, tokens, width),
            single(heads, tiles, 2 * tile, 2 * width),
            single(heads, tiles, 2 * tile, 1),
            buffer(heads, tokens, width),
            buffer(2, rows, model),
            buffer(rows, model),
            buffer(rows, model),
            single(3, 8, rows + -rows % 128),
            buffer(*gate_weight.shape),
            buffer(*up_weight.shape),
            buffer(*down_weight.shape),
            buffer(2, rows, model),
            buffer(3, n_sp - 1, *block),
            buffer(2, n_z, n_sp, *block),
            buffer(flat, model),
            buffer(n_z, n_sp, *block),
            buffer(flat, model),
            buffer(3, n_sp, *block),
            buffer(2, rows, model),
            buffer(2, rows, model),
            buffer(n_sp, *block),
            single(3, rows, model),
            dma((n_sp + 1, 2)),
            dma((n_sp - 1, heads, 2)),
            dma((heads, 3, n_tp)),
            dma((heads, 3, n_tp)),
            dma((heads,)),
            dma((heads,)),
            dma((2, 2)),
            dma((2, 2)),
            dma((n_z,)),
            dma((n_z,)),
            dma((heads * n_tp + 3,)),
            dma((n_sp, n_z)),
            dma((n_sp, n_z)),
            dma((n_sp, n_z)),
            dma((n_sp, n_z)),
            dma((n_z,)),
            dma((n_z,)),
            dma((n_sp, n_z, 2)),
            dma((n_sp, n_z, 2)),
            dma((n_z, 2)),
            dma((n_z, 2)),
            dma((n_sp,)),
            dma((n_sp,)),
            dma((n_sp,)),
            dma((n_sp,)),
            pltpu.SemaphoreType.REGULAR,
        ],
        compiler_params=pltpu.CompilerParams(
            collective_id=2, has_side_effects=True, vmem_limit_bytes=VMEM_BYTES
        ),
        name="layer",
    )(
        lambdas,
        q,
        k,
        v,
        head_gain.reshape(1, -1),
        expert_ids.T,
        route_weights.T,
        residual,
        norm_gain.reshape(1, -1),
        out_weight.reshape(n_tp, heads, width, model),
        gate_weight,
        up_weight,
        down_weight,
    )


def shards(
    queries,
    key_pairs,
    head_values,
    lambdas,
    head_gain,
    out_weight,
    residual,
    norm_gain,
    expert_ids,
    route_weights,
    gate_weight,
    up_weight,
    down_weight,
):
    tokens_here, heads_here, pair_width = queries.shape
    value_width = head_values.shape[2]
    rows_here = residual.shape[0]
    sp_count = lax.axis_size("sp")
    tp_count = lax.axis_size("tp")
    z_count = tp_count // CORES
    route_count = expert_ids.shape[1]
    local_experts = gate_weight.shape[0]
    expert_count = local_experts * sp_count
    capacity = max(2, 4 * rows_here * route_count // (3 * expert_count))
    model_width = residual.shape[1]
    block_bytes = z_count * local_experts * capacity * model_width * 2
    if sp_count == PLANE and z_count == LAYERS and heads_here == HEADS_HERE and pair_width == value_width and (
        capacity % 16 == 0 and rows_here <= 128 and route_count == 2
        and (7 * sp_count - 1) * block_bytes <= 3 * VMEM_BYTES // 5
    ):
        return whole_layer(
            queries,
            key_pairs,
            head_values,
            lambdas,
            head_gain,
            expert_ids,
            route_weights,
            residual,
            norm_gain,
            out_weight,
            gate_weight,
            up_weight,
            down_weight,
            sp_count,
            tp_count,
            capacity,
        )
    flat_ids = expert_ids.reshape(-1)
    indicator = (flat_ids[:, None] == jnp.arange(expert_count, dtype=jnp.int32)[None, :]).astype(
        jnp.int32
    )
    ranking = jnp.sum(jnp.cumsum(indicator, axis=0) * indicator, axis=1) - 1
    turned = (flat_ids - lax.axis_index("sp") * local_experts) % expert_count
    near_slots = (turned * capacity + ranking).reshape(rows_here, route_count)
    slots = flat_ids * capacity + ranking
    meta = jnp.concatenate([near_slots.astype(jnp.float32), route_weights], axis=1).T
    meta = jnp.pad(meta, ((0, 8 - 2 * route_count), (0, -rows_here % 128)), constant_values=-1.0)
    updated, normed, zmeta = attend(
        queries,
        key_pairs,
        head_values,
        lambdas,
        head_gain,
        meta,
        residual,
        norm_gain,
        out_weight,
        sp_count,
        tp_count,
    )
    if capacity % 16 == 0 and rows_here <= 128 and route_count == 2 and (
        (7 * sp_count - 1) * block_bytes <= 3 * VMEM_BYTES // 5
    ):
        return experts(
            normed, zmeta, updated, gate_weight, up_weight, down_weight, sp_count, z_count, capacity
        )
    sources = jnp.arange(rows_here * route_count, dtype=jnp.int32) // route_count
    outgoing = (
        jnp.zeros((expert_count * capacity, model_width), jnp.bfloat16)
        .at[slots]
        .set(normed[sources])
    )
    arrived = lax.all_to_all(
        outgoing.reshape(sp_count, local_experts, capacity, model_width),
        "sp",
        split_axis=0,
        concat_axis=0,
        tiled=True,
    )
    piece_rows = lax.all_gather(arrived[None], "tp", axis=0, tiled=True)
    gate_part = jnp.einsum(
        "tsecd,edf->tsecf", piece_rows, gate_weight, preferred_element_type=jnp.float32
    )
    up_part = jnp.einsum(
        "tsecd,edf->tsecf", piece_rows, up_weight, preferred_element_type=jnp.float32
    )
    inner_rows = (jax.nn.silu(gate_part) * up_part).astype(jnp.bfloat16)
    partial_value = jnp.einsum(
        "tsecf,efd->tsecd", inner_rows, down_weight, preferred_element_type=jnp.float32
    )
    reduced = lax.psum_scatter(
        partial_value.astype(jnp.bfloat16), "tp", scatter_dimension=0, tiled=True
    )
    returned = lax.all_to_all(reduced[0], "sp", split_axis=0, concat_axis=0, tiled=True)
    picked = (
        returned.reshape(expert_count * capacity, model_width)[slots]
        .astype(jnp.float32)
        .reshape(rows_here, route_count, model_width)
    )
    moe_sum = jnp.sum(picked * route_weights[:, :, None], axis=1)
    return (updated.astype(jnp.float32) + moe_sum).astype(jnp.bfloat16)


def solution(mesh):
    placed = (
        P("sp", "tp", None),
        P("sp", "tp", None),
        P("sp", "tp", None),
        P("tp"),
        P(),
        P(),
        P(("sp", "tp"), None),
        P(),
        P(("sp", "tp"), None),
        P(("sp", "tp"), None),
        P("sp", None, "tp"),
        P("sp", None, "tp"),
        P("sp", "tp", None),
    )
    return jax.shard_map(
        shards, mesh=mesh, in_specs=placed, out_specs=P(("sp", "tp"), None), check_vma=False
    )
```

```python
import functools
import math

import jax
import jax.numpy as jnp
from jax import lax
from jax.experimental import pallas as pl
from jax.experimental.pallas import tpu as pltpu
from jax.sharding import PartitionSpec as P

MESH = pl.DeviceIdType.MESH
LOG2E = 1.4426950408889634
CORES = 2
PLANE = 4
HEADS_HERE = 2
LAYERS = 4
TWIN = 3
VMEM_BYTES = 67043328


def attend_kernel(
    n_sp,
    n_tp,
    scale,
    lam_ref,
    q_ref,
    kv_ref,
    gain_ref,
    meta_ref,
    base_ref,
    norm_ref,
    w_hbm,
    updated_ref,
    normed_ref,
    zmeta_ref,
    weight,
    gathered,
    kvbuf,
    acc,
    top,
    tot,
    att,
    kv_send,
    kv_recv,
    at_send,
    at_recv,
    me_send,
    me_recv,
    own_sem,
    w_sem,
):
    heads, tiles, wide, _ = q_ref.shape
    tile = wide // 2
    rows = base_ref.shape[0]
    n_z = n_tp // CORES
    c = lax.axis_index("sp")
    t = lax.axis_index("tp")
    load = pltpu.make_async_copy(w_hbm, weight, w_sem)
    load.start()
    barrier = pltpu.get_barrier_semaphore()
    for d in range(1, n_sp):
        pl.semaphore_signal(barrier, inc=1, device_id=((c + d) % n_sp, t), device_id_type=MESH)
    for d in range(1, n_tp):
        pl.semaphore_signal(barrier, inc=1, device_id=(c, (t + d) % n_tp), device_id_type=MESH)
    pl.semaphore_wait(barrier, n_sp + n_tp - 2)

    def kv_copy(d, h):
        return pltpu.make_async_remote_copy(
            src_ref=kv_ref.at[h],
            dst_ref=kvbuf.at[d - 1, h],
            send_sem=kv_send.at[d - 1, h],
            recv_sem=kv_recv.at[d - 1, h],
            device_id=((c + d) % n_sp, t),
            device_id_type=MESH,
        )

    def meta_copy(d):
        return pltpu.make_async_remote_copy(
            src_ref=meta_ref,
            dst_ref=zmeta_ref.at[d],
            send_sem=me_send.at[d],
            recv_sem=me_recv.at[d],
            device_id=(c, (t + CORES * d) % n_tp),
            device_id_type=MESH,
        )

    for d in range(1, n_sp):
        @pl.when(c + d < n_sp)
        def _():
            for h in range(heads):
                kv_copy(d, h).start()

    for d in range(1, n_z):
        meta_copy(d).start()
    zmeta_ref[0] = meta_ref[...]

    factor = scale * LOG2E

    def scores_of(h, i, keys):
        return (
            lax.dot_general(
                q_ref[h, i], keys, (((1,), (1,)), ((), ())), preferred_element_type=jnp.float32
            )
            * factor
        )

    for i in range(tiles):
        extent = (i + 1) * tile
        for h in range(heads):
            s = scores_of(h, i, kv_ref[h, 0, :extent])
            row = lax.rem(lax.broadcasted_iota(jnp.int32, (wide, extent), 0), tile) + i * tile
            col = lax.broadcasted_iota(jnp.int32, (wide, extent), 1)
            s = jnp.where(col <= row, s, -jnp.inf)
            high = jnp.max(s, axis=1, keepdims=True)
            p = jnp.exp2(s - high)
            top[h, i] = high
            tot[h, i] = jnp.sum(p, axis=1, keepdims=True)
            acc[h, i] = jnp.dot(
                p.astype(jnp.bfloat16), kv_ref[h, 1, :extent], preferred_element_type=jnp.float32
            )

    def span_step(step, carry):
        for h in range(heads):
            kv_copy(step, h).wait_recv()

        def tile_step(i, inner):
            for h in range(heads):
                s = scores_of(h, i, kvbuf[step - 1, h, 0])
                before = top[h, i]
                high = jnp.maximum(before, jnp.max(s, axis=1, keepdims=True))
                p = jnp.exp2(s - high)
                decay = jnp.exp2(before - high)
                top[h, i] = high
                tot[h, i] = tot[h, i] * decay + jnp.sum(p, axis=1, keepdims=True)
                acc[h, i] = acc[h, i] * decay + jnp.dot(
                    p.astype(jnp.bfloat16),
                    kvbuf[step - 1, h, 1],
                    preferred_element_type=jnp.float32,
                )
            return inner

        return lax.fori_loop(0, tiles, tile_step, carry)

    lax.fori_loop(1, c + 1, span_step, 0)

    for h in range(heads):
        width = acc.shape[3]
        for i in range(tiles):
            both = acc[h, i] / tot[h, i]
            mixed = both[:tile] - lam_ref[h] * both[tile:]
            mean = jnp.mean(mixed * mixed, axis=1, keepdims=True)
            normed = mixed * lax.rsqrt(mean + 1e-06) * gain_ref[...]
            att[i * tile : (i + 1) * tile, h * width : (h + 1) * width] = normed.astype(att.dtype)

    def att_copy(d):
        to = (t + d) % n_tp
        return pltpu.make_async_remote_copy(
            src_ref=att.at[pl.ds(pl.multiple_of(to * rows, rows), rows)],
            dst_ref=gathered.at[t],
            send_sem=at_send.at[d],
            recv_sem=at_recv.at[d],
            device_id=(c, to),
            device_id_type=MESH,
        )

    for d in range(1, n_tp):
        att_copy(d).start()
    own = pltpu.make_async_copy(
        att.at[pl.ds(pl.multiple_of(t * rows, rows), rows)], gathered.at[t], own_sem
    )
    own.start()
    own.wait()
    load.wait()
    span = att.shape[1]
    projected = jnp.zeros(base_ref.shape, jnp.float32)
    for d in range(n_tp):
        if d:
            att_copy(d).wait_recv()
        source = (t - d + n_tp) % n_tp
        projected = projected + jnp.dot(
            gathered[source],
            weight[pl.ds(pl.multiple_of(source * span, span), span), :],
            preferred_element_type=jnp.float32,
        )
    updated = (base_ref[...].astype(jnp.float32) + projected).astype(jnp.bfloat16)
    updated_ref[...] = updated
    widened = updated.astype(jnp.float32)
    mean = jnp.mean(widened * widened, axis=1, keepdims=True)
    normed_ref[...] = (widened * lax.rsqrt(mean + 1e-06) * norm_ref[...]).astype(jnp.bfloat16)
    for d in range(1, n_tp):
        att_copy(d).wait_send()
    for d in range(1, n_z):
        meta_copy(d).wait()
    for d in range(1, n_sp):
        @pl.when(c + d < n_sp)
        def _():
            for h in range(heads):
                kv_copy(d, h).wait_send()


def attend(queries, key_pairs, head_values, lambdas, head_gain, meta, residual, norm_gain, out_weight, n_sp, n_tp):
    tokens, heads, pair = queries.shape
    rows = residual.shape[0]
    width = head_values.shape[2]
    half = pair // 2
    tile = math.gcd(tokens, 256)
    tiles = tokens // tile
    first = (jnp.arange(pair) < half)[None, :]
    q = jnp.transpose(queries, (1, 0, 2)).reshape(heads, tiles, 1, tile, pair)
    sides = jnp.stack([first, ~first])
    q = jnp.where(sides, q, jnp.zeros((), q.dtype)).reshape(heads, tiles, 2 * tile, pair)
    kv = jnp.transpose(jnp.stack([key_pairs, head_values]), (2, 0, 1, 3))
    dma = pltpu.SemaphoreType.DMA
    vmem = pl.BlockSpec(memory_space=pltpu.VMEM)
    n_z = n_tp // CORES
    return pl.pallas_call(
        functools.partial(attend_kernel, n_sp, n_tp, half ** (-0.5)),
        out_shape=(
            jax.ShapeDtypeStruct(residual.shape, jnp.bfloat16),
            jax.ShapeDtypeStruct(residual.shape, jnp.bfloat16),
            jax.ShapeDtypeStruct((n_z,) + meta.shape, meta.dtype),
        ),
        in_specs=[pl.BlockSpec(memory_space=pltpu.SMEM)] + [vmem] * 6
        + [pl.BlockSpec(memory_space=pl.ANY)],
        out_specs=(vmem, vmem, vmem),
        scratch_shapes=[
            pltpu.VMEM(out_weight.shape, out_weight.dtype),
            pltpu.VMEM((n_tp, rows, heads * width), jnp.bfloat16),
            pltpu.VMEM((n_sp - 1,) + kv.shape, kv.dtype),
            pltpu.VMEM((heads, tiles, 2 * tile, width), jnp.float32),
            pltpu.VMEM((heads, tiles, 2 * tile, 1), jnp.float32),
            pltpu.VMEM((heads, tiles, 2 * tile, 1), jnp.float32),
            pltpu.VMEM((tokens, heads * width), jnp.bfloat16),
            dma((n_sp - 1, heads)),
            dma((n_sp - 1, heads)),
            dma((n_tp,)),
            dma((n_tp,)),
            dma((n_z,)),
            dma((n_z,)),
            dma,
            dma,
        ],
        compiler_params=pltpu.CompilerParams(
            collective_id=0, has_side_effects=True, vmem_limit_bytes=48 * 1024 * 1024
        ),
        name="attend",
    )(lambdas, q, kv, head_gain.reshape(1, -1), meta, residual, norm_gain.reshape(1, -1), out_weight)


def experts_kernel(
    n_sp,
    n_z,
    x_ref,
    meta_ref,
    base_ref,
    gate_hbm,
    up_hbm,
    down_hbm,
    out_ref,
    gate,
    up,
    down,
    zrows,
    pack,
    arrived,
    psend,
    own,
    precv,
    ret,
    zsend,
    zret,
    mine,
    w_sem,
    zs_send,
    zs_recv,
    ps_send,
    ps_recv,
    fw_send,
    fw_recv,
    pp_send,
    pp_recv,
    rt_send,
    rt_recv,
    zr_send,
    zr_recv,
):
    rows, model = x_ref.shape
    local, cap = pack.shape[2], pack.shape[3]
    slots = n_sp * local * cap
    c = lax.axis_index("sp")
    t = lax.axis_index("tp")
    n_tp = n_z * CORES
    core = t % CORES
    partner = (c, t + 1 - 2 * core)
    loads = [
        pltpu.make_async_copy(a, b, w_sem.at[i])
        for i, (a, b) in enumerate(((gate_hbm, gate), (up_hbm, up), (down_hbm, down)))
    ]
    for load in loads:
        load.start()

    def column(d):
        return ((c + d) % n_sp, t)

    def layer(d):
        return (c, (t + CORES * d) % n_tp)

    barrier = pltpu.get_barrier_semaphore()
    for d in range(1, n_sp):
        pl.semaphore_signal(barrier, inc=1, device_id=column(d), device_id_type=MESH)
    for d in range(1, n_z):
        pl.semaphore_signal(barrier, inc=1, device_id=layer(d), device_id_type=MESH)
    pl.semaphore_signal(barrier, inc=1, device_id=partner, device_id_type=MESH)
    pl.semaphore_wait(barrier, n_sp + n_z - 1)

    def remote(src, dst, send, recv, target):
        return pltpu.make_async_remote_copy(
            src_ref=src,
            dst_ref=dst,
            send_sem=send,
            recv_sem=recv,
            device_id=target,
            device_id_type=MESH,
        )

    def z_copy(d):
        return remote(x_ref, zrows.at[d - 1], zs_send.at[d], zs_recv.at[d], layer(d))

    def pack_copy(d, s):
        return remote(
            pack.at[s, d - 1], arrived.at[0, s, d], ps_send.at[d, s], ps_recv.at[d, s], column(d)
        )

    def share_copy(d, s):
        return remote(
            arrived.at[0, s, d], arrived.at[1, s, d], fw_send.at[d, s], fw_recv.at[d, s], partner
        )

    def pair_copy(s):
        return remote(psend.at[s], precv.at[s], pp_send.at[s], pp_recv.at[s], partner)

    def back_copy(d, s):
        return remote(
            own.at[s, d], ret.at[s, d], rt_send.at[d, s], rt_recv.at[d, s], column(n_sp - d)
        )

    def z_back(d):
        return remote(
            zsend.at[d], zret.at[d], zr_send.at[d], zr_recv.at[d], layer(n_z - d)
        )

    for d in range(1, n_z):
        z_copy(d).start()

    def route_hits(s, r):
        target = lax.broadcasted_iota(jnp.int32, (slots, rows), 0).astype(jnp.float32)
        return target == meta_ref[s, r : r + 1, :rows]

    def pack_rows(s):
        if s:
            z_copy(s).wait_recv()
        hits = route_hits(s, 0) | route_hits(s, 1)
        pick = jnp.where(hits, 1.0, 0.0).astype(jnp.bfloat16)
        source = x_ref[...] if s == 0 else zrows[s - 1]
        packed = (
            jnp.dot(pick, source, preferred_element_type=jnp.float32)
            .astype(jnp.bfloat16)
            .reshape(n_sp, local, cap, model)
        )
        for d in range(1, n_sp):
            pack[s, d - 1] = packed[d]
            pack_copy(d, s).start()
        arrived[0, s, 0] = packed[0]
        share_copy(0, s).start()

    def run_experts(s):
        for d in range(1, n_sp):
            pack_copy(d, s).wait_recv()
            share_copy(d, s).start()
        for d in range(n_sp):
            share_copy(d, s).wait_recv()

        def expert_step(e, carry):
            x = arrived[:, s, :, e].reshape(2 * n_sp * cap, model)
            gated = jnp.dot(x, gate[e], preferred_element_type=jnp.float32)
            lifted = jnp.dot(x, up[e], preferred_element_type=jnp.float32)
            inner = (gated / (1.0 + jnp.exp(-gated)) * lifted).astype(jnp.bfloat16)
            y = jnp.dot(inner, down[e], preferred_element_type=jnp.float32)
            y = y.astype(jnp.bfloat16).reshape(2, n_sp, cap, model)
            own[s, :, e] = y[0]
            psend[s, :, e] = y[1]
            return carry

        lax.fori_loop(0, local, expert_step, 0)
        pair_copy(s).start()

    def reduce_pair(s):
        pair_copy(s).wait_recv()
        for d in list(range(1, n_sp)) + [0]:
            total = own[s, d].astype(jnp.float32) + precv[s, d].astype(jnp.float32)
            total = total.astype(jnp.bfloat16)
            if d == 0:
                ret[s, 0] = total
            else:
                own[s, d] = total
                back_copy(d, s).start()

    def mix_rows(s):
        for d in range(1, n_sp):
            back_copy(d, s).wait_recv()
        mixing = jnp.where(route_hits(s, 0), meta_ref[s, 2:3, :rows], 0.0) + jnp.where(
            route_hits(s, 1), meta_ref[s, 3:4, :rows], 0.0
        )
        high = mixing.astype(jnp.bfloat16)
        low = (mixing - high.astype(jnp.float32)).astype(jnp.bfloat16)
        back = ret[s].reshape(slots, model)
        numbers = (((0,), (0,)), ((), ()))
        merged = lax.dot_general(
            high, back, numbers, preferred_element_type=jnp.float32
        ) + lax.dot_general(low, back, numbers, preferred_element_type=jnp.float32)
        if s:
            zsend[s] = merged.astype(jnp.bfloat16)
            z_back(s).start()
        else:
            mine[...] = merged

    pack_rows(0)
    for load in loads:
        load.wait()
    if n_z > 1:
        pack_rows(1)
    for s in range(n_z):
        run_experts(s)
        if s + 2 < n_z:
            pack_rows(s + 2)
        elif s + 2 - n_z < n_z - 2:
            mix_rows(s + 2 - n_z)
        reduce_pair(s)
    for s in range(max(0, n_z - 2), n_z):
        mix_rows(s)
    merged = mine[...]
    for s in range(1, n_z):
        z_back(s).wait_recv()
        merged = merged + zret[s].astype(jnp.float32)
    out_ref[...] = (base_ref[...].astype(jnp.float32) + merged).astype(jnp.bfloat16)

    for d in range(1, n_z):
        z_copy(d).wait_send()
        z_back(d).wait_send()
    for s in range(n_z):
        for d in range(n_sp):
            if d:
                pack_copy(d, s).wait_send()
                back_copy(d, s).wait_send()
            share_copy(d, s).wait_send()
        pair_copy(s).wait_send()


def experts(normed, zmeta, updated, gate_weight, up_weight, down_weight, n_sp, n_z, cap):
    rows, model = normed.shape
    local = gate_weight.shape[0]
    dma = pltpu.SemaphoreType.DMA
    vmem = pl.BlockSpec(memory_space=pltpu.VMEM)
    hbm = pl.BlockSpec(memory_space=pl.ANY)
    block = (local, cap, model)

    def buffer(*shape):
        return pltpu.VMEM(shape, jnp.bfloat16)

    return pl.pallas_call(
        functools.partial(experts_kernel, n_sp, n_z),
        out_shape=jax.ShapeDtypeStruct((rows, model), jnp.bfloat16),
        in_specs=[vmem] * 3 + [hbm] * 3,
        out_specs=vmem,
        scratch_shapes=[
            buffer(*gate_weight.shape),
            buffer(*up_weight.shape),
            buffer(*down_weight.shape),
            buffer(n_z - 1, rows, model),
            buffer(n_z, n_sp - 1, *block),
            buffer(2, n_z, n_sp, *block),
            buffer(n_z, n_sp, *block),
            buffer(n_z, n_sp, *block),
            buffer(n_z, n_sp, *block),
            buffer(n_z, n_sp, *block),
            buffer(n_z, rows, model),
            buffer(n_z, rows, model),
            pltpu.VMEM((rows, model), jnp.float32),
            dma((3,)),
            dma((n_z,)),
            dma((n_z,)),
            dma((n_sp, n_z)),
            dma((n_sp, n_z)),
            dma((n_sp, n_z)),
            dma((n_sp, n_z)),
            dma((n_z,)),
            dma((n_z,)),
            dma((n_sp, n_z)),
            dma((n_sp, n_z)),
            dma((n_z,)),
            dma((n_z,)),
        ],
        compiler_params=pltpu.CompilerParams(
            collective_id=1, has_side_effects=True, vmem_limit_bytes=VMEM_BYTES
        ),
        name="experts",
    )(normed, zmeta, updated, gate_weight, up_weight, down_weight)


def layer_kernel(
    n_sp,
    n_tp,
    scale,
    lam_ref,
    raw_q,
    raw_k,
    raw_v,
    gain_ref,
    ids_ref,
    mix_ref,
    base_ref,
    norm_ref,
    w_hbm,
    gate_hbm,
    up_hbm,
    down_hbm,
    out_ref,
    q_ref,
    k_ref,
    v_ref,
    gathered,
    kvbuf,
    acc,
    top,
    att,
    bases,
    updated,
    x_ref,
    zmeta,
    gate,
    up,
    down,
    zrows,
    pack,
    arrived,
    psend,
    own,
    precv,
    ret,
    zsend,
    zret,
    fold,
    parts,
    kv_send,
    kv_recv,
    at_send,
    at_recv,
    ar_send,
    ar_recv,
    ba_send,
    ba_recv,
    me_send,
    me_recv,
    w_sem,
    ps_send,
    ps_recv,
    fw_send,
    fw_recv,
    pp_send,
    pp_recv,
    rt_send,
    rt_recv,
    zr_send,
    zr_recv,
    tw_send,
    tw_recv,
    fo_send,
    fo_recv,
    go,
):
    heads, tiles, wide, _ = q_ref.shape
    tile = wide // 2
    rows, model = base_ref.shape
    width = v_ref.shape[2]
    n_z = n_tp // CORES
    local, cap = pack.shape[2], pack.shape[3]
    slots = n_sp * local * cap
    span = n_sp * local * cap
    c = lax.axis_index("sp")
    t = lax.axis_index("tp")
    core = t % CORES
    partner = (c, t + 1 - 2 * core)

    def column(d):
        return ((c + d) % n_sp, t)

    z = t // CORES
    twin_z = z + 1 - 2 * (z % 2)
    far_z = (z + n_z // 2) % n_z
    twin = (c, twin_z * CORES + core)
    far = [None, (c, far_z * CORES + core), (c, (far_z + 1 - 2 * (far_z % 2)) * CORES + core)]

    weight = (psend, precv)
    loads = [
        pltpu.make_async_copy(a, b, w_sem.at[i])
        for i, (a, b) in enumerate(
            [
                (w_hbm.at[source, h], weight[h].at[source * width : (source + 1) * width])
                for h in range(heads)
                for source in range(n_tp)
            ]
            + [(gate_hbm, gate), (up_hbm, up), (down_hbm, down)]
        )
    ]
    for load in loads:
        load.start()
    barrier = pltpu.get_barrier_semaphore()
    for d in range(1, n_sp):
        pl.semaphore_signal(barrier, inc=1, device_id=column(d), device_id_type=MESH)
    for d in range(1, n_tp):
        pl.semaphore_signal(barrier, inc=1, device_id=(c, (t + d) % n_tp), device_id_type=MESH)
    for h in range(heads):
        k_ref[h] = raw_k[:, h, :]
        v_ref[h] = raw_v[:, h, :]
    pl.semaphore_wait(barrier, n_sp + n_tp - 2)

    def remote(src, dst, send, recv, target):
        return pltpu.make_async_remote_copy(
            src_ref=src,
            dst_ref=dst,
            send_sem=send,
            recv_sem=recv,
            device_id=target,
            device_id_type=MESH,
        )

    def kv_copies(slot, source, h, to, mine_too, parts=(0, 1)):
        return [
            remote(
                (k_ref, v_ref)[part].at[h] if mine_too else kvbuf.at[source, h, part],
                kvbuf.at[source, h, part],
                kv_send.at[slot, part],
                kv_recv.at[source, h, part],
                (to, t),
            )
            for part in parts
        ]

    def kv_wait(source, h):
        for part in range(2):
            remote(
                kvbuf.at[source, h, part],
                kvbuf.at[source, h, part],
                kv_send.at[0, part],
                kv_recv.at[source, h, part],
                partner,
            ).wait_recv()

    first_sends = [
        kv_copies(0, 0, 0, 2, True)
        + kv_copies(1, 0, 1, 1, True)
        + kv_copies(2, 0, 1, 2, True)
        + kv_copies(3, 0, 0, 1, True),
        kv_copies(0, 1, 0, 3, True) + kv_copies(1, 1, 1, 0, True) + kv_copies(2, 1, 1, 3, True),
        kv_copies(0, 2, 0, 3, True) + kv_copies(1, 2, 1, 3, True, (0,)),
        [],
    ]
    relayed = [(1, 1), (0, 1), (0, 0), (1, 0)]
    late_sends = [
        kv_copies(4, 1, 1, 2, False),
        kv_copies(3, 0, 1, 3, False),
        kv_copies(2, 0, 0, 3, False) + kv_copies(1, 2, 1, 3, True, (1,)),
        kv_copies(0, 1, 0, 2, False),
    ]

    def meta_copy(d):
        return remote(zmeta.at[0], zmeta.at[d], me_send.at[d], me_recv.at[d], far[d])

    for k in range(n_sp):
        @pl.when(c == k)
        def _():
            for copy in first_sends[k]:
                copy.start()

    def base_copy(d, side):
        columns = slice(side * (model // 2), (side + 1) * (model // 2))
        return remote(
            base_ref.at[:, columns] if d == 1 else bases.at[0, :, columns],
            bases.at[d - 1, :, columns],
            ba_send.at[d - 1, side],
            ba_recv.at[d - 1, side],
            far[1] if d == 1 else twin,
        )

    def pass_base(side):
        base_copy(1, side).wait_recv()
        base_copy(2, side).start()

    for side in range(2):
        base_copy(1, side).start()

    experts = n_sp * local
    shape = (experts, rows)
    names = lax.broadcasted_iota(jnp.int32, shape, 0)
    named = [names == ids_ref[r : r + 1, :] for r in range(2)]
    chosen = jnp.where(named[0] | named[1], 1.0, 0.0).astype(jnp.bfloat16)
    earlier = lax.broadcasted_iota(jnp.int32, (rows, rows), 0) < lax.broadcasted_iota(
        jnp.int32, (rows, rows), 1
    )
    ranks = jnp.dot(
        chosen, jnp.where(earlier, 1.0, 0.0).astype(jnp.bfloat16), preferred_element_type=jnp.float32
    )
    zmeta[0] = jnp.full(zmeta.shape[1:], -1.0, jnp.float32)
    for r in range(2):
        turned = ids_ref[r : r + 1, :] - c * local
        turned = jnp.where(turned < 0, turned + experts, turned)
        rank = jnp.sum(jnp.where(named[r], ranks, 0.0), axis=0, keepdims=True)
        zmeta[0, r : r + 1, :rows] = (turned * cap).astype(jnp.float32) + rank
        zmeta[0, 2 + r : 3 + r, :rows] = mix_ref[r : r + 1, :]
    for d in (1, 2):
        meta_copy(d).start()

    side = lax.broadcasted_iota(jnp.int32, (tile, raw_q.shape[2]), 1) < raw_q.shape[2] // 2
    for h in range(heads):
        att[h] = raw_q[:, h, :]
        for i in range(tiles):
            part = att[h, i * tile : (i + 1) * tile]
            q_ref[h, i, :tile] = jnp.where(side, part, jnp.zeros_like(part))
            q_ref[h, i, tile:] = jnp.where(side, jnp.zeros_like(part), part)

    factor = scale * LOG2E

    def scores_of(h, i, keys):
        return (
            lax.dot_general(
                q_ref[h, i], keys, (((1,), (1,)), ((), ())), preferred_element_type=jnp.float32
            )
            * factor
        )

    def with_ones(values):
        return jnp.concatenate([values, jnp.ones_like(values)], axis=1)

    for i in range(tiles):
        extent = (i + 1) * tile
        for h in range(heads):
            s = scores_of(h, i, k_ref[h, :extent])
            row = lax.rem(lax.broadcasted_iota(jnp.int32, (wide, extent), 0), tile) + i * tile
            col = lax.broadcasted_iota(jnp.int32, (wide, extent), 1)
            s = jnp.where(col <= row, s, -jnp.inf)
            high = jnp.max(s, axis=1, keepdims=True)
            p = jnp.exp2(s - high)
            top[h, i] = high
            acc[h, i] = jnp.dot(
                p.astype(jnp.bfloat16),
                with_ones(v_ref[h, :extent]),
                preferred_element_type=jnp.float32,
            )

    for k in range(n_sp):
        @pl.when(c == k)
        def _():
            kv_wait(*relayed[k])
            for copy in late_sends[k]:
                copy.start()

    pass_base(0)

    def order_of(orders):
        codes = [sum((2 * s + h) * 8**j for j, (s, h) in enumerate(o)) for o in orders]
        code, count = jnp.int32(codes[0]), jnp.int32(len(orders[0]))
        for k in range(1, n_sp):
            code = jnp.where(c == k, codes[k], code)
            count = jnp.where(c == k, len(orders[k]), count)
        return code, count

    def absorb(orders, waited, passing=False):
        code, count = order_of(orders)

        def piece_step(j, code):
            piece = code % 8
            source, h = piece // 2, piece % 2

            @pl.when(j >= waited)
            def _():
                kv_wait(source, h)

            if passing:

                @pl.when(j == count - 1)
                def _():
                    pass_base(1)

            keys, values = kvbuf[source, h, 0], with_ones(kvbuf[source, h, 1])
            results = []
            for i in range(tiles):
                s = scores_of(h, i, keys)
                before = top[h, i]
                high = jnp.maximum(before, jnp.max(s, axis=1, keepdims=True))
                p = jnp.exp2(s - high)
                decay = jnp.exp2(before - high)
                summed = acc[h, i] * decay + jnp.dot(
                    p.astype(jnp.bfloat16), values, preferred_element_type=jnp.float32
                )
                results.append((high, summed))
            for i in range(tiles):
                top[h, i], acc[h, i] = results[i]
            return code // 8

        lax.fori_loop(0, count, piece_step, code)

    half = n_z // 2

    def block_rows(b, to_z, to_core):
        layer = to_z if b == 0 else (to_z + half) % n_z
        if b == 2:
            layer = layer + 1 - 2 * (layer % 2)
        return pl.ds(pl.multiple_of((layer * CORES + to_core) * rows, rows), rows)

    here = pl.ds(pl.multiple_of(t * width, width), width)

    def att_copy(h, b, d):
        to = (t + d) % n_tp
        return remote(
            att.at[h, block_rows(b, to // CORES, to % CORES)],
            gathered.at[h, b, :, here],
            at_send.at[h, b, d],
            at_recv.at[h, b, d],
            (c, to),
        )

    def relay_copy(h):
        side = half * CORES * width
        across = pl.ds(pl.multiple_of((1 - z // half) * side, side), side)
        return remote(
            gathered.at[h, 1, :, across],
            gathered.at[h, 2, :, across],
            ar_send.at[h],
            ar_recv.at[h],
            twin,
        )

    def near(d):
        return ((t + d) % n_tp) // CORES // half == z // half

    def finish(h):
        for i in range(tiles):
            both = acc[h, i, :, :width] / acc[h, i, :, width:]
            mixed = both[:tile] - lam_ref[h] * both[tile:]
            mean = jnp.mean(mixed * mixed, axis=1, keepdims=True)
            normed = mixed * lax.rsqrt(mean + 1e-06) * gain_ref[...]
            att[h, i * tile : (i + 1) * tile] = normed.astype(att.dtype)
        for d in range(1, n_tp):
            att_copy(h, 0, d).start()
        for b in range(3):
            gathered[h, b, :, here] = att[h, block_rows(b, z, core)]

    def finish_far():
        for h in range(heads):
            for d in range(1, n_tp):
                att_copy(h, 1, d).start()
        for h in range(heads):
            for d in range(1, n_tp):

                @pl.when(near(d))
                def _():
                    att_copy(h, 2, d).start()


    def await_rows(h, b):
        for d in range(1, n_tp):
            if b < 2:
                att_copy(h, b, d).wait_recv()
            else:

                @pl.when(near(n_tp - d))
                def _():
                    att_copy(h, b, d).wait_recv()

        if b == 1:
            relay_copy(h).start()
        if b == 2:
            relay_copy(h).wait_recv()

    def project(h, b):
        return jnp.dot(
            gathered[h, b], weight[h][: n_tp * width], preferred_element_type=jnp.float32
        )

    def normalize(base, projected):
        new = (base.astype(jnp.float32) + projected).astype(jnp.bfloat16)
        widened = new.astype(jnp.float32)
        mean = jnp.mean(widened * widened, axis=1, keepdims=True)
        return new, (widened * lax.rsqrt(mean + 1e-06) * norm_ref[...]).astype(jnp.bfloat16)

    def far_rows(b):
        await_rows(0, b)
        parts[b] = project(0, b)
        await_rows(1, b)
        if b == 2:
            for part in range(2):
                base_copy(2, part).wait_recv()
        _, normed = normalize(bases[b - 1], parts[b] + project(1, b))
        zrows[b - 1] = normed

    absorb([[], [(0, 1), (0, 0)], [(0, 0), (0, 1), (1, 0)], [(1, 0), (2, 0), (1, 1), (0, 0)]], 1, True)

    @pl.when(c == 0)
    def _():
        pass_base(1)

    finish(0)
    absorb([[], [], [(1, 1)], [(2, 1), (0, 1)]], 0)

    @pl.when(c == n_sp - 1)
    def _():
        for d in range(1, n_sp):
            pl.semaphore_signal(go, inc=1, device_id=column(d), device_id_type=MESH)

    finish(1)
    finish_far()
    for load in loads[: heads * n_tp]:
        load.wait()
    await_rows(0, 0)
    parts[0] = project(0, 0)
    await_rows(1, 0)
    new, normed = normalize(base_ref[...], parts[0] + project(1, 0))
    updated[...] = new
    x_ref[...] = normed

    def pack_copy(d, s):
        return remote(
            pack.at[s, d - 1], arrived.at[0, s, d], ps_send.at[d, s], ps_recv.at[d, s], column(d)
        )

    def share_copy(d, s):
        return remote(
            arrived.at[0, s, d], arrived.at[1, s, d], fw_send.at[d, s], fw_recv.at[d, s], partner
        )

    def twin_copy(d):
        return remote(
            arrived.at[0, 0, d], arrived.at[0, TWIN, d], tw_send.at[d], tw_recv.at[d], twin
        )

    def pair_copy(s):
        block = pl.ds(s * span, span)
        return remote(psend.at[block], precv.at[block], pp_send.at[s], pp_recv.at[s], partner)

    def fold_copy(d):
        return remote(own.at[TWIN, d], fold.at[d], fo_send.at[d], fo_recv.at[d], twin)

    def columns_of(part):
        return slice(part * (model // 2), (part + 1) * (model // 2))

    def back_copy(d, s, part):
        return remote(
            own.at[s, d, :, :, columns_of(part)],
            ret.at[s, d, :, :, columns_of(part)],
            rt_send.at[d, s, part],
            rt_recv.at[d, s, part],
            column(n_sp - d),
        )

    def z_part(d, part, target):
        return remote(
            zsend.at[d - 1, :, columns_of(part)],
            zret.at[d - 1, :, columns_of(part)],
            zr_send.at[d, part],
            zr_recv.at[d, part],
            target,
        )

    def z_back(d, part):
        return z_part(d, part, far[d])

    def z_join(part):
        return remote(
            zsend.at[0, :, columns_of(part)],
            zret.at[0, :, columns_of(part)],
            zr_send.at[0, part],
            zr_recv.at[0, part],
            twin,
        )

    outer = (z == 0) | (z == n_z - 1)
    for d in (1, 2):
        meta_copy(d).wait()

    def route_hits(s, r):
        target = lax.broadcasted_iota(jnp.int32, (slots, rows), 0).astype(jnp.float32)
        return target == zmeta[s, r : r + 1, :rows]

    def pack_rows(s):
        hits = route_hits(s, 0) | route_hits(s, 1)
        pick = jnp.where(hits, 1.0, 0.0).astype(jnp.bfloat16)
        source = x_ref[...] if s == 0 else zrows[s - 1]
        packed = (
            jnp.dot(pick, source, preferred_element_type=jnp.float32)
            .astype(jnp.bfloat16)
            .reshape(n_sp, local, cap, model)
        )
        if s == 0:
            arrived[0, 0, 0] = packed[0]
            twin_copy(0).start()
        for d in range(1, n_sp):
            pack[s, d - 1] = packed[d]
            pack_copy(d, s).start()
        if s:
            arrived[0, s, 0] = packed[0]
        share_copy(0, s).start()

    def rows_here(s):
        for d in range(n_sp):
            if s == TWIN:
                twin_copy(d).wait_recv()
            elif s and d:
                pack_copy(d, s).wait_recv()
            if s == TWIN or d:
                share_copy(d, s).start()
        for d in range(n_sp):
            share_copy(d, s).wait_recv()

    def run_experts(s):
        rows_here(s)

        def expert_step(e, carry):
            x = arrived[:, s, :, e].reshape(2 * n_sp * cap, model)
            gated = jnp.dot(x, gate[e], preferred_element_type=jnp.float32)
            lifted = jnp.dot(x, up[e], preferred_element_type=jnp.float32)
            inner = (gated / (1.0 + jnp.exp(-gated)) * lifted).astype(jnp.bfloat16)
            y = jnp.dot(inner, down[e], preferred_element_type=jnp.float32)
            y = y.astype(jnp.bfloat16).reshape(2, n_sp, cap, model)
            own[s, :, e] = y[0]
            for d in range(n_sp):
                place = pl.multiple_of(s * span + (d * local + e) * cap, cap)
                psend[pl.ds(place, cap)] = y[1, d]
            return carry

        lax.fori_loop(0, local, expert_step, 0)
        pair_copy(s).start()

    def reduce_pair(s):
        pair_copy(s).wait_recv()
        for d in list(range(1, n_sp)) + [0]:
            other = precv[s * span + d * local * cap : s * span + (d + 1) * local * cap]
            total = own[s, d].astype(jnp.float32) + other.reshape(local, cap, model).astype(
                jnp.float32
            )
            if s == 0:
                fold_copy(d).wait_recv()
                total = total + fold[d].astype(jnp.float32)
            total = total.astype(jnp.bfloat16)
            if s == TWIN:
                own[s, d] = total
                if d in (1, 2):
                    fold_copy(d).start()
                else:

                    @pl.when(jnp.logical_not(outer))
                    def _():
                        fold_copy(d).start()

            elif d == 0:
                ret[s, 0] = total
            else:
                own[s, d] = total
                back_copy(d, s, 0).start()
                if s == 0:
                    back_copy(d, s, 1).start()
        if s in (1, 2):
            for d in range(1, n_sp):
                back_copy(d, s, 1).start()

    def mix_rows(s, part):
        for d in range(1, n_sp):
            back_copy(d, s, part).wait_recv()
        columns = columns_of(part)
        mixing = jnp.where(route_hits(s, 0), zmeta[s, 2:3, :rows], 0.0) + jnp.where(
            route_hits(s, 1), zmeta[s, 3:4, :rows], 0.0
        )
        high = mixing.astype(jnp.bfloat16)
        low = (mixing - high.astype(jnp.float32)).astype(jnp.bfloat16)
        back = ret[s, :, :, :, columns].reshape(slots, model // 2)
        numbers = (((0,), (0,)), ((), ()))
        merged = lax.dot_general(
            high, back, numbers, preferred_element_type=jnp.float32
        ) + lax.dot_general(low, back, numbers, preferred_element_type=jnp.float32)
        if s == 1:
            zsend[0, :, columns] = merged.astype(jnp.bfloat16)

            @pl.when(outer)
            def _():
                z_join(part).start()

            @pl.when(jnp.logical_not(outer))
            def _():
                z_back(1, part).start()

        if s == 2:
            parts[0, :, columns] = merged

            @pl.when(jnp.logical_not(outer))
            def _():
                z_join(part).wait_recv()
                parts[0, :, columns] = parts[0, :, columns] + zret[0, :, columns].astype(jnp.float32)

            zsend[1, :, columns] = parts[0, :, columns].astype(jnp.bfloat16)
            z_back(2, part).start()
        return merged

    def sent_early():
        for k in range(n_sp):
            @pl.when(c == k)
            def _():
                for copy in first_sends[k] + late_sends[k]:
                    copy.wait_send()

        for h in range(heads):
            for d in range(1, n_tp):
                for b in range(2):
                    att_copy(h, b, d).wait_send()

                @pl.when(near(d))
                def _():
                    att_copy(h, 2, d).wait_send()

            relay_copy(h).wait_send()
        for d in (1, 2):
            for side in range(2):
                base_copy(d, side).wait_send()

    def sent_later():
        for s in range(n_z):
            for d in range(n_sp):
                if d and s != TWIN:
                    pack_copy(d, s).wait_send()
                if d and s in (1, 2):
                    for part in range(2):
                        back_copy(d, s, part).wait_send()
                share_copy(d, s).wait_send()
            pair_copy(s).wait_send()
        for d in range(n_sp):
            twin_copy(d).wait_send()

    @pl.when(c != n_sp - 1)
    def _():
        pl.semaphore_wait(go, 1)

    pack_rows(0)
    for load in loads[heads * n_tp :]:
        load.wait()
    far_rows(1)
    pack_rows(1)
    for d in range(1, n_sp):
        pack_copy(d, 0).wait_recv()
        twin_copy(d).start()
    far_rows(2)
    pack_rows(2)
    run_experts(0)
    sent_early()
    run_experts(1)
    reduce_pair(1)
    run_experts(TWIN)
    reduce_pair(TWIN)
    run_experts(2)
    reduce_pair(2)
    mix_rows(1, 0)
    mix_rows(1, 1)

    @pl.when(outer)
    def _():
        for d in (n_sp - 1, 0):
            fold_copy(d).start()

    mix_rows(2, 0)
    mix_rows(2, 1)
    sent_later()
    reduce_pair(0)
    parts[0] = updated[...].astype(jnp.float32)
    for part in range(2):
        columns = columns_of(part)

        @pl.when(outer)
        def _():
            z_back(1, part).wait_recv()
            parts[0, :, columns] = parts[0, :, columns] + zret[0, :, columns].astype(jnp.float32)

        z_back(2, part).wait_recv()
        parts[0, :, columns] = parts[0, :, columns] + zret[1, :, columns].astype(jnp.float32)
    for part in range(2):
        columns = columns_of(part)
        out_ref[:, columns] = (parts[0, :, columns] + mix_rows(0, part)).astype(jnp.bfloat16)

    for part in range(2):

        @pl.when(outer)
        def _():
            z_join(part).wait_send()

        @pl.when(jnp.logical_not(outer))
        def _():
            z_back(1, part).wait_send()

        z_back(2, part).wait_send()
    for d in range(n_sp):
        fold_copy(d).wait_send()
        if d:
            for part in range(2):
                back_copy(d, 0, part).wait_send()


def whole_layer(
    queries,
    key_pairs,
    head_values,
    lambdas,
    head_gain,
    expert_ids,
    route_weights,
    residual,
    norm_gain,
    out_weight,
    gate_weight,
    up_weight,
    down_weight,
    n_sp,
    n_tp,
    cap,
):
    tokens, heads, pair = queries.shape
    rows, model = residual.shape
    width = head_values.shape[2]
    local = gate_weight.shape[0]
    n_z = n_tp // CORES
    tile = math.gcd(tokens, 256)
    tiles = tokens // tile
    dma = pltpu.SemaphoreType.DMA
    vmem = pl.BlockSpec(memory_space=pltpu.VMEM)
    hbm = pl.BlockSpec(memory_space=pl.ANY)
    block = (local, cap, model)
    flat = max(n_tp * width, n_z * n_sp * local * cap)

    def buffer(*shape):
        return pltpu.VMEM(shape, jnp.bfloat16)

    def single(*shape):
        return pltpu.VMEM(shape, jnp.float32)

    return pl.pallas_call(
        functools.partial(layer_kernel, n_sp, n_tp, (pair // 2) ** (-0.5)),
        out_shape=jax.ShapeDtypeStruct((rows, model), jnp.bfloat16),
        in_specs=[pl.BlockSpec(memory_space=pltpu.SMEM)] + [vmem] * 8 + [hbm] * 4,
        out_specs=vmem,
        scratch_shapes=[
            buffer(heads, tiles, 2 * tile, pair),
            buffer(heads, tokens, pair),
            buffer(heads, tokens, width),
            buffer(heads, 3, rows, n_tp * width),
            buffer(n_sp - 1, heads, 2, tokens, width),
            single(heads, tiles, 2 * tile, 2 * width),
            single(heads, tiles, 2 * tile, 1),
            buffer(heads, tokens, width),
            buffer(2, rows, model),
            buffer(rows, model),
            buffer(rows, model),
            single(3, 8, rows + -rows % 128),
            buffer(*gate_weight.shape),
            buffer(*up_weight.shape),
            buffer(*down_weight.shape),
            buffer(2, rows, model),
            buffer(3, n_sp - 1, *block),
            buffer(2, n_z, n_sp, *block),
            buffer(flat, model),
            buffer(n_z, n_sp, *block),
            buffer(flat, model),
            buffer(3, n_sp, *block),
            buffer(2, rows, model),
            buffer(2, rows, model),
            buffer(n_sp, *block),
            single(3, rows, model),
            dma((n_sp + 1, 2)),
            dma((n_sp - 1, heads, 2)),
            dma((heads, 3, n_tp)),
            dma((heads, 3, n_tp)),
            dma((heads,)),
            dma((heads,)),
            dma((2, 2)),
            dma((2, 2)),
            dma((n_z,)),
            dma((n_z,)),
            dma((heads * n_tp + 3,)),
            dma((n_sp, n_z)),
            dma((n_sp, n_z)),
            dma((n_sp, n_z)),
            dma((n_sp, n_z)),
            dma((n_z,)),
            dma((n_z,)),
            dma((n_sp, n_z, 2)),
            dma((n_sp, n_z, 2)),
            dma((n_z, 2)),
            dma((n_z, 2)),
            dma((n_sp,)),
            dma((n_sp,)),
            dma((n_sp,)),
            dma((n_sp,)),
            pltpu.SemaphoreType.REGULAR,
        ],
        compiler_params=pltpu.CompilerParams(
            collective_id=2, has_side_effects=True, vmem_limit_bytes=VMEM_BYTES
        ),
        name="layer",
    )(
        lambdas,
        queries,
        key_pairs,
        head_values,
        head_gain.reshape(1, -1),
        expert_ids.T,
        route_weights.T,
        residual,
        norm_gain.reshape(1, -1),
        out_weight.reshape(n_tp, heads, width, model),
        gate_weight,
        up_weight,
        down_weight,
    )


def shards(
    queries,
    key_pairs,
    head_values,
    lambdas,
    head_gain,
    out_weight,
    residual,
    norm_gain,
    expert_ids,
    route_weights,
    gate_weight,
    up_weight,
    down_weight,
):
    tokens_here, heads_here, pair_width = queries.shape
    value_width = head_values.shape[2]
    rows_here = residual.shape[0]
    sp_count = lax.axis_size("sp")
    tp_count = lax.axis_size("tp")
    z_count = tp_count // CORES
    route_count = expert_ids.shape[1]
    local_experts = gate_weight.shape[0]
    expert_count = local_experts * sp_count
    capacity = max(2, 4 * rows_here * route_count // (3 * expert_count))
    model_width = residual.shape[1]
    block_bytes = z_count * local_experts * capacity * model_width * 2
    if sp_count == PLANE and z_count == LAYERS and heads_here == HEADS_HERE and pair_width == value_width and (
        capacity % 16 == 0 and rows_here <= 128 and route_count == 2
        and (7 * sp_count - 1) * block_bytes <= 3 * VMEM_BYTES // 5
    ):
        return whole_layer(
            queries,
            key_pairs,
            head_values,
            lambdas,
            head_gain,
            expert_ids,
            route_weights,
            residual,
            norm_gain,
            out_weight,
            gate_weight,
            up_weight,
            down_weight,
            sp_count,
            tp_count,
            capacity,
        )
    flat_ids = expert_ids.reshape(-1)
    indicator = (flat_ids[:, None] == jnp.arange(expert_count, dtype=jnp.int32)[None, :]).astype(
        jnp.int32
    )
    ranking = jnp.sum(jnp.cumsum(indicator, axis=0) * indicator, axis=1) - 1
    turned = (flat_ids - lax.axis_index("sp") * local_experts) % expert_count
    near_slots = (turned * capacity + ranking).reshape(rows_here, route_count)
    slots = flat_ids * capacity + ranking
    meta = jnp.concatenate([near_slots.astype(jnp.float32), route_weights], axis=1).T
    meta = jnp.pad(meta, ((0, 8 - 2 * route_count), (0, -rows_here % 128)), constant_values=-1.0)
    updated, normed, zmeta = attend(
        queries,
        key_pairs,
        head_values,
        lambdas,
        head_gain,
        meta,
        residual,
        norm_gain,
        out_weight,
        sp_count,
        tp_count,
    )
    if capacity % 16 == 0 and rows_here <= 128 and route_count == 2 and (
        (7 * sp_count - 1) * block_bytes <= 3 * VMEM_BYTES // 5
    ):
        return experts(
            normed, zmeta, updated, gate_weight, up_weight, down_weight, sp_count, z_count, capacity
        )
    sources = jnp.arange(rows_here * route_count, dtype=jnp.int32) // route_count
    outgoing = (
        jnp.zeros((expert_count * capacity, model_width), jnp.bfloat16)
        .at[slots]
        .set(normed[sources])
    )
    arrived = lax.all_to_all(
        outgoing.reshape(sp_count, local_experts, capacity, model_width),
        "sp",
        split_axis=0,
        concat_axis=0,
        tiled=True,
    )
    piece_rows = lax.all_gather(arrived[None], "tp", axis=0, tiled=True)
    gate_part = jnp.einsum(
        "tsecd,edf->tsecf", piece_rows, gate_weight, preferred_element_type=jnp.float32
    )
    up_part = jnp.einsum(
        "tsecd,edf->tsecf", piece_rows, up_weight, preferred_element_type=jnp.float32
    )
    inner_rows = (jax.nn.silu(gate_part) * up_part).astype(jnp.bfloat16)
    partial_value = jnp.einsum(
        "tsecf,efd->tsecd", inner_rows, down_weight, preferred_element_type=jnp.float32
    )
    reduced = lax.psum_scatter(
        partial_value.astype(jnp.bfloat16), "tp", scatter_dimension=0, tiled=True
    )
    returned = lax.all_to_all(reduced[0], "sp", split_axis=0, concat_axis=0, tiled=True)
    picked = (
        returned.reshape(expert_count * capacity, model_width)[slots]
        .astype(jnp.float32)
        .reshape(rows_here, route_count, model_width)
    )
    moe_sum = jnp.sum(picked * route_weights[:, :, None], axis=1)
    return (updated.astype(jnp.float32) + moe_sum).astype(jnp.bfloat16)


def solution(mesh):
    placed = (
        P("sp", "tp", None),
        P("sp", "tp", None),
        P("sp", "tp", None),
        P("tp"),
        P(),
        P(),
        P(("sp", "tp"), None),
        P(),
        P(("sp", "tp"), None),
        P(("sp", "tp"), None),
        P("sp", None, "tp"),
        P("sp", None, "tp"),
        P("sp", "tp", None),
    )
    return jax.shard_map(
        shards, mesh=mesh, in_specs=placed, out_specs=P(("sp", "tp"), None), check_vma=False
    )
```

```python
import functools
import math

import jax
import jax.numpy as jnp
from jax import lax
from jax.experimental import pallas as pl
from jax.experimental.pallas import tpu as pltpu
from jax.sharding import PartitionSpec as P

MESH = pl.DeviceIdType.MESH
LOG2E = 1.4426950408889634
CORES = 2
PLANE = 4
HEADS_HERE = 2
LAYERS = 4
TWIN = 3
VMEM_BYTES = 67043328


def attend_kernel(
    n_sp,
    n_tp,
    scale,
    lam_ref,
    q_ref,
    kv_ref,
    gain_ref,
    meta_ref,
    base_ref,
    norm_ref,
    w_hbm,
    updated_ref,
    normed_ref,
    zmeta_ref,
    weight,
    gathered,
    kvbuf,
    acc,
    top,
    tot,
    att,
    kv_send,
    kv_recv,
    at_send,
    at_recv,
    me_send,
    me_recv,
    own_sem,
    w_sem,
):
    heads, tiles, wide, _ = q_ref.shape
    tile = wide // 2
    rows = base_ref.shape[0]
    n_z = n_tp // CORES
    c = lax.axis_index("sp")
    t = lax.axis_index("tp")
    load = pltpu.make_async_copy(w_hbm, weight, w_sem)
    load.start()
    barrier = pltpu.get_barrier_semaphore()
    for d in range(1, n_sp):
        pl.semaphore_signal(barrier, inc=1, device_id=((c + d) % n_sp, t), device_id_type=MESH)
    for d in range(1, n_tp):
        pl.semaphore_signal(barrier, inc=1, device_id=(c, (t + d) % n_tp), device_id_type=MESH)
    pl.semaphore_wait(barrier, n_sp + n_tp - 2)

    def kv_copy(d, h):
        return pltpu.make_async_remote_copy(
            src_ref=kv_ref.at[h],
            dst_ref=kvbuf.at[d - 1, h],
            send_sem=kv_send.at[d - 1, h],
            recv_sem=kv_recv.at[d - 1, h],
            device_id=((c + d) % n_sp, t),
            device_id_type=MESH,
        )

    def meta_copy(d):
        return pltpu.make_async_remote_copy(
            src_ref=meta_ref,
            dst_ref=zmeta_ref.at[d],
            send_sem=me_send.at[d],
            recv_sem=me_recv.at[d],
            device_id=(c, (t + CORES * d) % n_tp),
            device_id_type=MESH,
        )

    for d in range(1, n_sp):
        @pl.when(c + d < n_sp)
        def _():
            for h in range(heads):
                kv_copy(d, h).start()

    for d in range(1, n_z):
        meta_copy(d).start()
    zmeta_ref[0] = meta_ref[...]

    factor = scale * LOG2E

    def scores_of(h, i, keys):
        return (
            lax.dot_general(
                q_ref[h, i], keys, (((1,), (1,)), ((), ())), preferred_element_type=jnp.float32
            )
            * factor
        )

    for i in range(tiles):
        extent = (i + 1) * tile
        for h in range(heads):
            s = scores_of(h, i, kv_ref[h, 0, :extent])
            row = lax.rem(lax.broadcasted_iota(jnp.int32, (wide, extent), 0), tile) + i * tile
            col = lax.broadcasted_iota(jnp.int32, (wide, extent), 1)
            s = jnp.where(col <= row, s, -jnp.inf)
            high = jnp.max(s, axis=1, keepdims=True)
            p = jnp.exp2(s - high)
            top[h, i] = high
            tot[h, i] = jnp.sum(p, axis=1, keepdims=True)
            acc[h, i] = jnp.dot(
                p.astype(jnp.bfloat16), kv_ref[h, 1, :extent], preferred_element_type=jnp.float32
            )

    def span_step(step, carry):
        for h in range(heads):
            kv_copy(step, h).wait_recv()

        def tile_step(i, inner):
            for h in range(heads):
                s = scores_of(h, i, kvbuf[step - 1, h, 0])
                before = top[h, i]
                high = jnp.maximum(before, jnp.max(s, axis=1, keepdims=True))
                p = jnp.exp2(s - high)
                decay = jnp.exp2(before - high)
                top[h, i] = high
                tot[h, i] = tot[h, i] * decay + jnp.sum(p, axis=1, keepdims=True)
                acc[h, i] = acc[h, i] * decay + jnp.dot(
                    p.astype(jnp.bfloat16),
                    kvbuf[step - 1, h, 1],
                    preferred_element_type=jnp.float32,
                )
            return inner

        return lax.fori_loop(0, tiles, tile_step, carry)

    lax.fori_loop(1, c + 1, span_step, 0)

    for h in range(heads):
        width = acc.shape[3]
        for i in range(tiles):
            both = acc[h, i] / tot[h, i]
            mixed = both[:tile] - lam_ref[h] * both[tile:]
            mean = jnp.mean(mixed * mixed, axis=1, keepdims=True)
            normed = mixed * lax.rsqrt(mean + 1e-06) * gain_ref[...]
            att[i * tile : (i + 1) * tile, h * width : (h + 1) * width] = normed.astype(att.dtype)

    def att_copy(d):
        to = (t + d) % n_tp
        return pltpu.make_async_remote_copy(
            src_ref=att.at[pl.ds(pl.multiple_of(to * rows, rows), rows)],
            dst_ref=gathered.at[t],
            send_sem=at_send.at[d],
            recv_sem=at_recv.at[d],
            device_id=(c, to),
            device_id_type=MESH,
        )

    for d in range(1, n_tp):
        att_copy(d).start()
    own = pltpu.make_async_copy(
        att.at[pl.ds(pl.multiple_of(t * rows, rows), rows)], gathered.at[t], own_sem
    )
    own.start()
    own.wait()
    load.wait()
    span = att.shape[1]
    projected = jnp.zeros(base_ref.shape, jnp.float32)
    for d in range(n_tp):
        if d:
            att_copy(d).wait_recv()
        source = (t - d + n_tp) % n_tp
        projected = projected + jnp.dot(
            gathered[source],
            weight[pl.ds(pl.multiple_of(source * span, span), span), :],
            preferred_element_type=jnp.float32,
        )
    updated = (base_ref[...].astype(jnp.float32) + projected).astype(jnp.bfloat16)
    updated_ref[...] = updated
    widened = updated.astype(jnp.float32)
    mean = jnp.mean(widened * widened, axis=1, keepdims=True)
    normed_ref[...] = (widened * lax.rsqrt(mean + 1e-06) * norm_ref[...]).astype(jnp.bfloat16)
    for d in range(1, n_tp):
        att_copy(d).wait_send()
    for d in range(1, n_z):
        meta_copy(d).wait()
    for d in range(1, n_sp):
        @pl.when(c + d < n_sp)
        def _():
            for h in range(heads):
                kv_copy(d, h).wait_send()


def attend(queries, key_pairs, head_values, lambdas, head_gain, meta, residual, norm_gain, out_weight, n_sp, n_tp):
    tokens, heads, pair = queries.shape
    rows = residual.shape[0]
    width = head_values.shape[2]
    half = pair // 2
    tile = math.gcd(tokens, 256)
    tiles = tokens // tile
    first = (jnp.arange(pair) < half)[None, :]
    q = jnp.transpose(queries, (1, 0, 2)).reshape(heads, tiles, 1, tile, pair)
    sides = jnp.stack([first, ~first])
    q = jnp.where(sides, q, jnp.zeros((), q.dtype)).reshape(heads, tiles, 2 * tile, pair)
    kv = jnp.transpose(jnp.stack([key_pairs, head_values]), (2, 0, 1, 3))
    dma = pltpu.SemaphoreType.DMA
    vmem = pl.BlockSpec(memory_space=pltpu.VMEM)
    n_z = n_tp // CORES
    return pl.pallas_call(
        functools.partial(attend_kernel, n_sp, n_tp, half ** (-0.5)),
        out_shape=(
            jax.ShapeDtypeStruct(residual.shape, jnp.bfloat16),
            jax.ShapeDtypeStruct(residual.shape, jnp.bfloat16),
            jax.ShapeDtypeStruct((n_z,) + meta.shape, meta.dtype),
        ),
        in_specs=[pl.BlockSpec(memory_space=pltpu.SMEM)] + [vmem] * 6
        + [pl.BlockSpec(memory_space=pl.ANY)],
        out_specs=(vmem, vmem, vmem),
        scratch_shapes=[
            pltpu.VMEM(out_weight.shape, out_weight.dtype),
            pltpu.VMEM((n_tp, rows, heads * width), jnp.bfloat16),
            pltpu.VMEM((n_sp - 1,) + kv.shape, kv.dtype),
            pltpu.VMEM((heads, tiles, 2 * tile, width), jnp.float32),
            pltpu.VMEM((heads, tiles, 2 * tile, 1), jnp.float32),
            pltpu.VMEM((heads, tiles, 2 * tile, 1), jnp.float32),
            pltpu.VMEM((tokens, heads * width), jnp.bfloat16),
            dma((n_sp - 1, heads)),
            dma((n_sp - 1, heads)),
            dma((n_tp,)),
            dma((n_tp,)),
            dma((n_z,)),
            dma((n_z,)),
            dma,
            dma,
        ],
        compiler_params=pltpu.CompilerParams(
            collective_id=0, has_side_effects=True, vmem_limit_bytes=48 * 1024 * 1024
        ),
        name="attend",
    )(lambdas, q, kv, head_gain.reshape(1, -1), meta, residual, norm_gain.reshape(1, -1), out_weight)


def experts_kernel(
    n_sp,
    n_z,
    x_ref,
    meta_ref,
    base_ref,
    gate_hbm,
    up_hbm,
    down_hbm,
    out_ref,
    gate,
    up,
    down,
    zrows,
    pack,
    arrived,
    psend,
    own,
    precv,
    ret,
    zsend,
    zret,
    mine,
    w_sem,
    zs_send,
    zs_recv,
    ps_send,
    ps_recv,
    fw_send,
    fw_recv,
    pp_send,
    pp_recv,
    rt_send,
    rt_recv,
    zr_send,
    zr_recv,
):
    rows, model = x_ref.shape
    local, cap = pack.shape[2], pack.shape[3]
    slots = n_sp * local * cap
    c = lax.axis_index("sp")
    t = lax.axis_index("tp")
    n_tp = n_z * CORES
    core = t % CORES
    partner = (c, t + 1 - 2 * core)
    loads = [
        pltpu.make_async_copy(a, b, w_sem.at[i])
        for i, (a, b) in enumerate(((gate_hbm, gate), (up_hbm, up), (down_hbm, down)))
    ]
    for load in loads:
        load.start()

    def column(d):
        return ((c + d) % n_sp, t)

    def layer(d):
        return (c, (t + CORES * d) % n_tp)

    barrier = pltpu.get_barrier_semaphore()
    for d in range(1, n_sp):
        pl.semaphore_signal(barrier, inc=1, device_id=column(d), device_id_type=MESH)
    for d in range(1, n_z):
        pl.semaphore_signal(barrier, inc=1, device_id=layer(d), device_id_type=MESH)
    pl.semaphore_signal(barrier, inc=1, device_id=partner, device_id_type=MESH)
    pl.semaphore_wait(barrier, n_sp + n_z - 1)

    def remote(src, dst, send, recv, target):
        return pltpu.make_async_remote_copy(
            src_ref=src,
            dst_ref=dst,
            send_sem=send,
            recv_sem=recv,
            device_id=target,
            device_id_type=MESH,
        )

    def z_copy(d):
        return remote(x_ref, zrows.at[d - 1], zs_send.at[d], zs_recv.at[d], layer(d))

    def pack_copy(d, s):
        return remote(
            pack.at[s, d - 1], arrived.at[0, s, d], ps_send.at[d, s], ps_recv.at[d, s], column(d)
        )

    def share_copy(d, s):
        return remote(
            arrived.at[0, s, d], arrived.at[1, s, d], fw_send.at[d, s], fw_recv.at[d, s], partner
        )

    def pair_copy(s):
        return remote(psend.at[s], precv.at[s], pp_send.at[s], pp_recv.at[s], partner)

    def back_copy(d, s):
        return remote(
            own.at[s, d], ret.at[s, d], rt_send.at[d, s], rt_recv.at[d, s], column(n_sp - d)
        )

    def z_back(d):
        return remote(
            zsend.at[d], zret.at[d], zr_send.at[d], zr_recv.at[d], layer(n_z - d)
        )

    for d in range(1, n_z):
        z_copy(d).start()

    def route_hits(s, r):
        target = lax.broadcasted_iota(jnp.int32, (slots, rows), 0).astype(jnp.float32)
        return target == meta_ref[s, r : r + 1, :rows]

    def pack_rows(s):
        if s:
            z_copy(s).wait_recv()
        hits = route_hits(s, 0) | route_hits(s, 1)
        pick = jnp.where(hits, 1.0, 0.0).astype(jnp.bfloat16)
        source = x_ref[...] if s == 0 else zrows[s - 1]
        packed = (
            jnp.dot(pick, source, preferred_element_type=jnp.float32)
            .astype(jnp.bfloat16)
            .reshape(n_sp, local, cap, model)
        )
        for d in range(1, n_sp):
            pack[s, d - 1] = packed[d]
            pack_copy(d, s).start()
        arrived[0, s, 0] = packed[0]
        share_copy(0, s).start()

    def run_experts(s):
        for d in range(1, n_sp):
            pack_copy(d, s).wait_recv()
            share_copy(d, s).start()
        for d in range(n_sp):
            share_copy(d, s).wait_recv()

        def expert_step(e, carry):
            x = arrived[:, s, :, e].reshape(2 * n_sp * cap, model)
            gated = jnp.dot(x, gate[e], preferred_element_type=jnp.float32)
            lifted = jnp.dot(x, up[e], preferred_element_type=jnp.float32)
            inner = (gated / (1.0 + jnp.exp(-gated)) * lifted).astype(jnp.bfloat16)
            y = jnp.dot(inner, down[e], preferred_element_type=jnp.float32)
            y = y.astype(jnp.bfloat16).reshape(2, n_sp, cap, model)
            own[s, :, e] = y[0]
            psend[s, :, e] = y[1]
            return carry

        lax.fori_loop(0, local, expert_step, 0)
        pair_copy(s).start()

    def reduce_pair(s):
        pair_copy(s).wait_recv()
        for d in list(range(1, n_sp)) + [0]:
            total = own[s, d].astype(jnp.float32) + precv[s, d].astype(jnp.float32)
            total = total.astype(jnp.bfloat16)
            if d == 0:
                ret[s, 0] = total
            else:
                own[s, d] = total
                back_copy(d, s).start()

    def mix_rows(s):
        for d in range(1, n_sp):
            back_copy(d, s).wait_recv()
        mixing = jnp.where(route_hits(s, 0), meta_ref[s, 2:3, :rows], 0.0) + jnp.where(
            route_hits(s, 1), meta_ref[s, 3:4, :rows], 0.0
        )
        high = mixing.astype(jnp.bfloat16)
        low = (mixing - high.astype(jnp.float32)).astype(jnp.bfloat16)
        back = ret[s].reshape(slots, model)
        numbers = (((0,), (0,)), ((), ()))
        merged = lax.dot_general(
            high, back, numbers, preferred_element_type=jnp.float32
        ) + lax.dot_general(low, back, numbers, preferred_element_type=jnp.float32)
        if s:
            zsend[s] = merged.astype(jnp.bfloat16)
            z_back(s).start()
        else:
            mine[...] = merged

    pack_rows(0)
    for load in loads:
        load.wait()
    if n_z > 1:
        pack_rows(1)
    for s in range(n_z):
        run_experts(s)
        if s + 2 < n_z:
            pack_rows(s + 2)
        elif s + 2 - n_z < n_z - 2:
            mix_rows(s + 2 - n_z)
        reduce_pair(s)
    for s in range(max(0, n_z - 2), n_z):
        mix_rows(s)
    merged = mine[...]
    for s in range(1, n_z):
        z_back(s).wait_recv()
        merged = merged + zret[s].astype(jnp.float32)
    out_ref[...] = (base_ref[...].astype(jnp.float32) + merged).astype(jnp.bfloat16)

    for d in range(1, n_z):
        z_copy(d).wait_send()
        z_back(d).wait_send()
    for s in range(n_z):
        for d in range(n_sp):
            if d:
                pack_copy(d, s).wait_send()
                back_copy(d, s).wait_send()
            share_copy(d, s).wait_send()
        pair_copy(s).wait_send()


def experts(normed, zmeta, updated, gate_weight, up_weight, down_weight, n_sp, n_z, cap):
    rows, model = normed.shape
    local = gate_weight.shape[0]
    dma = pltpu.SemaphoreType.DMA
    vmem = pl.BlockSpec(memory_space=pltpu.VMEM)
    hbm = pl.BlockSpec(memory_space=pl.ANY)
    block = (local, cap, model)

    def buffer(*shape):
        return pltpu.VMEM(shape, jnp.bfloat16)

    return pl.pallas_call(
        functools.partial(experts_kernel, n_sp, n_z),
        out_shape=jax.ShapeDtypeStruct((rows, model), jnp.bfloat16),
        in_specs=[vmem] * 3 + [hbm] * 3,
        out_specs=vmem,
        scratch_shapes=[
            buffer(*gate_weight.shape),
            buffer(*up_weight.shape),
            buffer(*down_weight.shape),
            buffer(n_z - 1, rows, model),
            buffer(n_z, n_sp - 1, *block),
            buffer(2, n_z, n_sp, *block),
            buffer(n_z, n_sp, *block),
            buffer(n_z, n_sp, *block),
            buffer(n_z, n_sp, *block),
            buffer(n_z, n_sp, *block),
            buffer(n_z, rows, model),
            buffer(n_z, rows, model),
            pltpu.VMEM((rows, model), jnp.float32),
            dma((3,)),
            dma((n_z,)),
            dma((n_z,)),
            dma((n_sp, n_z)),
            dma((n_sp, n_z)),
            dma((n_sp, n_z)),
            dma((n_sp, n_z)),
            dma((n_z,)),
            dma((n_z,)),
            dma((n_sp, n_z)),
            dma((n_sp, n_z)),
            dma((n_z,)),
            dma((n_z,)),
        ],
        compiler_params=pltpu.CompilerParams(
            collective_id=1, has_side_effects=True, vmem_limit_bytes=VMEM_BYTES
        ),
        name="experts",
    )(normed, zmeta, updated, gate_weight, up_weight, down_weight)


def layer_kernel(
    n_sp,
    n_tp,
    scale,
    lam_ref,
    raw_q,
    raw_k,
    raw_v,
    gain_ref,
    ids_ref,
    mix_ref,
    base_ref,
    norm_ref,
    w_hbm,
    gate_hbm,
    up_hbm,
    down_hbm,
    out_ref,
    q_ref,
    k_ref,
    v_ref,
    gathered,
    kvbuf,
    acc,
    top,
    att,
    bases,
    updated,
    x_ref,
    zmeta,
    gate,
    up,
    down,
    zrows,
    pack,
    arrived,
    psend,
    own,
    precv,
    ret,
    zsend,
    zret,
    fold,
    parts,
    kv_send,
    kv_recv,
    at_send,
    at_recv,
    ar_send,
    ar_recv,
    ba_send,
    ba_recv,
    me_send,
    me_recv,
    w_sem,
    ps_send,
    ps_recv,
    fw_send,
    fw_recv,
    pp_send,
    pp_recv,
    rt_send,
    rt_recv,
    zr_send,
    zr_recv,
    tw_send,
    tw_recv,
    fo_send,
    fo_recv,
    go,
):
    heads, tiles, wide, _ = q_ref.shape
    tile = wide // 2
    rows, model = base_ref.shape
    width = v_ref.shape[2]
    n_z = n_tp // CORES
    local, cap = pack.shape[2], pack.shape[3]
    slots = n_sp * local * cap
    span = n_sp * local * cap
    c = lax.axis_index("sp")
    t = lax.axis_index("tp")
    core = t % CORES
    partner = (c, t + 1 - 2 * core)

    def column(d):
        return ((c + d) % n_sp, t)

    z = t // CORES
    twin_z = z + 1 - 2 * (z % 2)
    far_z = (z + n_z // 2) % n_z
    twin = (c, twin_z * CORES + core)
    far = [
        None,
        (c, far_z * CORES + core),
        (c, (far_z + 1 - 2 * (far_z % 2)) * CORES + core),
        twin,
    ]
    split = fold.shape[3]

    weight = (psend, precv)
    loads = [
        pltpu.make_async_copy(a, b, w_sem.at[i])
        for i, (a, b) in enumerate(
            [
                (w_hbm.at[source, h], weight[h].at[source * width : (source + 1) * width])
                for h in range(heads)
                for source in range(n_tp)
            ]
            + [(gate_hbm, gate), (up_hbm, up), (down_hbm, down)]
        )
    ]
    for load in loads:
        load.start()
    barrier = pltpu.get_barrier_semaphore()
    for d in range(1, n_sp):
        pl.semaphore_signal(barrier, inc=1, device_id=column(d), device_id_type=MESH)
    for d in range(1, n_tp):
        pl.semaphore_signal(barrier, inc=1, device_id=(c, (t + d) % n_tp), device_id_type=MESH)
    for h in range(heads):
        k_ref[h] = raw_k[:, h, :]
        v_ref[h] = raw_v[:, h, :]
    pl.semaphore_wait(barrier, n_sp + n_tp - 2)

    def remote(src, dst, send, recv, target):
        return pltpu.make_async_remote_copy(
            src_ref=src,
            dst_ref=dst,
            send_sem=send,
            recv_sem=recv,
            device_id=target,
            device_id_type=MESH,
        )

    def kv_copies(slot, source, h, to, mine_too, parts=(0, 1)):
        return [
            remote(
                (k_ref, v_ref)[part].at[h] if mine_too else kvbuf.at[source, h, part],
                kvbuf.at[source, h, part],
                kv_send.at[slot, part],
                kv_recv.at[source, h, part],
                (to, t),
            )
            for part in parts
        ]

    def kv_wait(source, h):
        for part in range(2):
            remote(
                kvbuf.at[source, h, part],
                kvbuf.at[source, h, part],
                kv_send.at[0, part],
                kv_recv.at[source, h, part],
                partner,
            ).wait_recv()

    first_sends = [
        kv_copies(0, 0, 0, 2, True)
        + kv_copies(1, 0, 1, 1, True)
        + kv_copies(2, 0, 1, 2, True)
        + kv_copies(3, 0, 0, 1, True),
        kv_copies(0, 1, 0, 3, True) + kv_copies(1, 1, 1, 0, True) + kv_copies(2, 1, 1, 3, True),
        kv_copies(0, 2, 0, 3, True) + kv_copies(1, 2, 1, 3, True, (0,)),
        [],
    ]
    relayed = [(1, 1), (0, 1), (0, 0), (1, 0)]
    late_sends = [
        kv_copies(4, 1, 1, 2, False),
        kv_copies(3, 0, 1, 3, False),
        kv_copies(2, 0, 0, 3, False) + kv_copies(1, 2, 1, 3, True, (1,)),
        kv_copies(0, 1, 0, 2, False),
    ]

    def meta_copy(d):
        return remote(zmeta.at[0], zmeta.at[d], me_send.at[d], me_recv.at[d], far[d])

    for k in range(n_sp):
        @pl.when(c == k)
        def _():
            for copy in first_sends[k]:
                copy.start()

    def base_copy(d, side):
        columns = slice(side * (model // 2), (side + 1) * (model // 2))
        return remote(
            base_ref.at[:, columns] if d == 1 else bases.at[0, :, columns],
            bases.at[d - 1, :, columns],
            ba_send.at[d - 1, side],
            ba_recv.at[d - 1, side],
            far[1] if d == 1 else twin,
        )

    def pass_base(side):
        base_copy(1, side).wait_recv()
        base_copy(2, side).start()

    for side in range(2):
        base_copy(1, side).start()

    experts = n_sp * local
    shape = (experts, rows)
    names = lax.broadcasted_iota(jnp.int32, shape, 0)
    named = [names == ids_ref[r : r + 1, :] for r in range(2)]
    chosen = jnp.where(named[0] | named[1], 1.0, 0.0).astype(jnp.bfloat16)
    earlier = lax.broadcasted_iota(jnp.int32, (rows, rows), 0) < lax.broadcasted_iota(
        jnp.int32, (rows, rows), 1
    )
    ranks = jnp.dot(
        chosen, jnp.where(earlier, 1.0, 0.0).astype(jnp.bfloat16), preferred_element_type=jnp.float32
    )
    zmeta[0] = jnp.full(zmeta.shape[1:], -1.0, jnp.float32)
    for r in range(2):
        turned = ids_ref[r : r + 1, :] - c * local
        turned = jnp.where(turned < 0, turned + experts, turned)
        rank = jnp.sum(jnp.where(named[r], ranks, 0.0), axis=0, keepdims=True)
        zmeta[0, r : r + 1, :rows] = (turned * cap).astype(jnp.float32) + rank
        zmeta[0, 2 + r : 3 + r, :rows] = mix_ref[r : r + 1, :]
    for d in (1, 2, TWIN):
        meta_copy(d).start()

    side = lax.broadcasted_iota(jnp.int32, (tile, raw_q.shape[2]), 1) < raw_q.shape[2] // 2
    for h in range(heads):
        att[h] = raw_q[:, h, :]
        for i in range(tiles):
            part = att[h, i * tile : (i + 1) * tile]
            q_ref[h, i, :tile] = jnp.where(side, part, jnp.zeros_like(part))
            q_ref[h, i, tile:] = jnp.where(side, jnp.zeros_like(part), part)

    factor = scale * LOG2E

    def scores_of(h, i, keys):
        return (
            lax.dot_general(
                q_ref[h, i], keys, (((1,), (1,)), ((), ())), preferred_element_type=jnp.float32
            )
            * factor
        )

    def with_ones(values):
        return jnp.concatenate([values, jnp.ones_like(values)], axis=1)

    for i in range(tiles):
        extent = (i + 1) * tile
        for h in range(heads):
            s = scores_of(h, i, k_ref[h, :extent])
            row = lax.rem(lax.broadcasted_iota(jnp.int32, (wide, extent), 0), tile) + i * tile
            col = lax.broadcasted_iota(jnp.int32, (wide, extent), 1)
            s = jnp.where(col <= row, s, -jnp.inf)
            high = jnp.max(s, axis=1, keepdims=True)
            p = jnp.exp2(s - high)
            top[h, i] = high
            acc[h, i] = jnp.dot(
                p.astype(jnp.bfloat16),
                with_ones(v_ref[h, :extent]),
                preferred_element_type=jnp.float32,
            )

    for k in range(n_sp):
        @pl.when(c == k)
        def _():
            kv_wait(*relayed[k])
            for copy in late_sends[k]:
                copy.start()

    pass_base(0)

    def order_of(orders):
        codes = [sum((2 * s + h) * 8**j for j, (s, h) in enumerate(o)) for o in orders]
        code, count = jnp.int32(codes[0]), jnp.int32(len(orders[0]))
        for k in range(1, n_sp):
            code = jnp.where(c == k, codes[k], code)
            count = jnp.where(c == k, len(orders[k]), count)
        return code, count

    def absorb(orders, waited, passing=False):
        code, count = order_of(orders)

        def piece_step(j, code):
            piece = code % 8
            source, h = piece // 2, piece % 2

            @pl.when(j >= waited)
            def _():
                kv_wait(source, h)

            if passing:

                @pl.when(j == count - 1)
                def _():
                    pass_base(1)

            keys, values = kvbuf[source, h, 0], with_ones(kvbuf[source, h, 1])
            results = []
            for i in range(tiles):
                s = scores_of(h, i, keys)
                before = top[h, i]
                high = jnp.maximum(before, jnp.max(s, axis=1, keepdims=True))
                p = jnp.exp2(s - high)
                decay = jnp.exp2(before - high)
                summed = acc[h, i] * decay + jnp.dot(
                    p.astype(jnp.bfloat16), values, preferred_element_type=jnp.float32
                )
                results.append((high, summed))
            for i in range(tiles):
                top[h, i], acc[h, i] = results[i]
            return code // 8

        lax.fori_loop(0, count, piece_step, code)

    half = n_z // 2

    def block_rows(b, to_z, to_core):
        layer = to_z if b == 0 else (to_z + half) % n_z
        if b == 2:
            layer = layer + 1 - 2 * (layer % 2)
        return pl.ds(pl.multiple_of((layer * CORES + to_core) * rows, rows), rows)

    here = pl.ds(pl.multiple_of(t * width, width), width)

    def att_copy(h, b, d):
        to = (t + d) % n_tp
        return remote(
            att.at[h, block_rows(b, to // CORES, to % CORES)],
            gathered.at[h, b, :, here],
            at_send.at[h, b, d],
            at_recv.at[h, b, d],
            (c, to),
        )

    def relay_copy(h):
        side = half * CORES * width
        across = pl.ds(pl.multiple_of((1 - z // half) * side, side), side)
        return remote(
            gathered.at[h, 1, :, across],
            gathered.at[h, 2, :, across],
            ar_send.at[h],
            ar_recv.at[h],
            twin,
        )

    def near(d):
        return ((t + d) % n_tp) // CORES // half == z // half

    def finish(h):
        for i in range(tiles):
            both = acc[h, i, :, :width] / acc[h, i, :, width:]
            mixed = both[:tile] - lam_ref[h] * both[tile:]
            mean = jnp.mean(mixed * mixed, axis=1, keepdims=True)
            normed = mixed * lax.rsqrt(mean + 1e-06) * gain_ref[...]
            att[h, i * tile : (i + 1) * tile] = normed.astype(att.dtype)
        for d in range(1, n_tp):
            att_copy(h, 0, d).start()
        for b in range(3):
            gathered[h, b, :, here] = att[h, block_rows(b, z, core)]

    def finish_far():
        for h in range(heads):
            for d in range(1, n_tp):
                att_copy(h, 1, d).start()
        for h in range(heads):
            for d in range(1, n_tp):

                @pl.when(near(d))
                def _():
                    att_copy(h, 2, d).start()


    def await_rows(h, b):
        for d in range(1, n_tp):
            if b < 2:
                att_copy(h, b, d).wait_recv()
            else:

                @pl.when(near(n_tp - d))
                def _():
                    att_copy(h, b, d).wait_recv()

        if b == 1:
            relay_copy(h).start()
        if b == 2:
            relay_copy(h).wait_recv()

    def project(h, b):
        return jnp.dot(
            gathered[h, b], weight[h][: n_tp * width], preferred_element_type=jnp.float32
        )

    def normalize(base, projected):
        new = (base.astype(jnp.float32) + projected).astype(jnp.bfloat16)
        widened = new.astype(jnp.float32)
        mean = jnp.mean(widened * widened, axis=1, keepdims=True)
        return new, (widened * lax.rsqrt(mean + 1e-06) * norm_ref[...]).astype(jnp.bfloat16)

    def far_rows(b):
        await_rows(0, b)
        parts[b] = project(0, b)
        await_rows(1, b)
        if b == 2:
            for part in range(2):
                base_copy(2, part).wait_recv()
        _, normed = normalize(bases[b - 1], parts[b] + project(1, b))
        zrows[b - 1] = normed

    absorb([[], [(0, 1), (0, 0)], [(0, 0), (0, 1), (1, 0)], [(1, 0), (2, 0), (1, 1), (0, 0)]], 1, True)

    @pl.when(c == 0)
    def _():
        pass_base(1)

    finish(0)
    absorb([[], [], [(1, 1)], [(2, 1), (0, 1)]], 0)

    @pl.when(c == n_sp - 1)
    def _():
        for d in range(1, n_sp):
            pl.semaphore_signal(go, inc=1, device_id=column(d), device_id_type=MESH)

    finish(1)
    finish_far()
    for load in loads[: heads * n_tp]:
        load.wait()
    await_rows(0, 0)
    parts[0] = project(0, 0)
    await_rows(1, 0)
    new, normed = normalize(base_ref[...], parts[0] + project(1, 0))
    updated[...] = new
    x_ref[...] = normed

    def pack_copy(d, s):
        return remote(
            pack.at[s, d - 1], arrived.at[0, s, d], ps_send.at[d, s], ps_recv.at[d, s], column(d)
        )

    def share_copy(d, s):
        return remote(
            arrived.at[0, s, d], arrived.at[1, s, d], fw_send.at[d, s], fw_recv.at[d, s], partner
        )

    def twin_copy(d):
        return remote(
            arrived.at[0, 0, d], arrived.at[0, TWIN, d], tw_send.at[d], tw_recv.at[d], twin
        )

    def pair_copy(s):
        block = pl.ds(s * span, span)
        return remote(psend.at[block], precv.at[block], pp_send.at[s], pp_recv.at[s], partner)

    def fold_copy(d):
        return remote(
            own.at[TWIN, d, :, :, :split], fold.at[d], fo_send.at[d], fo_recv.at[d], twin
        )

    def columns_of(part):
        if part == 2:
            return slice(split, model)
        return slice(part * (model // 2), (part + 1) * (model // 2))

    def back_copy(d, s, part):
        return remote(
            own.at[s, d, :, :, columns_of(part)],
            ret.at[s, d, :, :, columns_of(part)],
            rt_send.at[d, s, part],
            rt_recv.at[d, s, part],
            column(n_sp - d),
        )

    def z_part(d, part, target):
        return remote(
            zsend.at[d - 1, :, columns_of(part)],
            zret.at[d - 1, :, columns_of(part)],
            zr_send.at[d, part],
            zr_recv.at[d, part],
            target,
        )

    def z_back(d, part):
        return z_part(d, part, far[d])

    def z_join(part):
        return remote(
            zsend.at[0, :, columns_of(part)],
            zret.at[0, :, columns_of(part)],
            zr_send.at[0, part],
            zr_recv.at[0, part],
            twin,
        )

    outer = (z == 0) | (z == n_z - 1)
    for d in (1, 2, TWIN):
        meta_copy(d).wait()

    def route_hits(s, r):
        target = lax.broadcasted_iota(jnp.int32, (slots, rows), 0).astype(jnp.float32)
        return target == zmeta[s, r : r + 1, :rows]

    def pack_rows(s):
        hits = route_hits(s, 0) | route_hits(s, 1)
        pick = jnp.where(hits, 1.0, 0.0).astype(jnp.bfloat16)
        source = x_ref[...] if s == 0 else zrows[s - 1]
        packed = (
            jnp.dot(pick, source, preferred_element_type=jnp.float32)
            .astype(jnp.bfloat16)
            .reshape(n_sp, local, cap, model)
        )
        if s == 0:
            arrived[0, 0, 0] = packed[0]
            twin_copy(0).start()
        for d in range(1, n_sp):
            pack[s, d - 1] = packed[d]
            pack_copy(d, s).start()
        if s:
            arrived[0, s, 0] = packed[0]
        share_copy(0, s).start()

    def rows_here(s):
        for d in range(n_sp):
            if s == TWIN:
                twin_copy(d).wait_recv()
            elif s and d:
                pack_copy(d, s).wait_recv()
            if s == TWIN or d:
                share_copy(d, s).start()
        for d in range(n_sp):
            share_copy(d, s).wait_recv()

    def run_experts(s):
        rows_here(s)

        def expert_step(e, carry):
            x = arrived[:, s, :, e].reshape(2 * n_sp * cap, model)
            gated = jnp.dot(x, gate[e], preferred_element_type=jnp.float32)
            lifted = jnp.dot(x, up[e], preferred_element_type=jnp.float32)
            inner = (gated / (1.0 + jnp.exp(-gated)) * lifted).astype(jnp.bfloat16)
            y = jnp.dot(inner, down[e], preferred_element_type=jnp.float32)
            y = y.astype(jnp.bfloat16).reshape(2, n_sp, cap, model)
            own[s, :, e] = y[0]
            for d in range(n_sp):
                place = pl.multiple_of(s * span + (d * local + e) * cap, cap)
                psend[pl.ds(place, cap)] = y[1, d]
            return carry

        lax.fori_loop(0, local, expert_step, 0)
        pair_copy(s).start()

    def reduce_pair(s):
        pair_copy(s).wait_recv()
        for d in list(range(1, n_sp)) + [0]:
            other = precv[s * span + d * local * cap : s * span + (d + 1) * local * cap]
            total = own[s, d].astype(jnp.float32) + other.reshape(local, cap, model).astype(
                jnp.float32
            )
            if s == 0:
                fold_copy(d).wait_recv()
                total = jnp.concatenate(
                    [total[:, :, :split] + fold[d].astype(jnp.float32), total[:, :, split:]], axis=2
                )
            total = total.astype(jnp.bfloat16)
            if s == TWIN:
                own[s, d] = total
                if d in (1, 2):
                    fold_copy(d).start()
                else:

                    @pl.when(jnp.logical_not(outer))
                    def _():
                        fold_copy(d).start()

                if d:
                    back_copy(d, TWIN, 2).start()
                else:
                    ret[TWIN, 0, :, :, split:] = total[:, :, split:]
            elif d == 0:
                ret[s, 0] = total
            else:
                own[s, d] = total
                back_copy(d, s, 0).start()
                if s == 0:
                    back_copy(d, s, 1).start()
        if s in (1, 2):
            for d in range(1, n_sp):
                back_copy(d, s, 1).start()

    def mix_rows(s, part):
        for d in range(1, n_sp):
            back_copy(d, s, part).wait_recv()
        columns = columns_of(part)
        mixing = jnp.where(route_hits(s, 0), zmeta[s, 2:3, :rows], 0.0) + jnp.where(
            route_hits(s, 1), zmeta[s, 3:4, :rows], 0.0
        )
        high = mixing.astype(jnp.bfloat16)
        low = (mixing - high.astype(jnp.float32)).astype(jnp.bfloat16)
        back = ret[s, :, :, :, columns].reshape(slots, -1)
        numbers = (((0,), (0,)), ((), ()))
        merged = lax.dot_general(
            high, back, numbers, preferred_element_type=jnp.float32
        ) + lax.dot_general(low, back, numbers, preferred_element_type=jnp.float32)
        if s == 1:
            zsend[0, :, columns] = merged.astype(jnp.bfloat16)

            @pl.when(outer)
            def _():
                z_join(part).start()

            @pl.when(jnp.logical_not(outer))
            def _():
                z_back(1, part).start()

        if s == TWIN:
            zsend[TWIN - 1, :, columns] = merged.astype(jnp.bfloat16)
            z_back(TWIN, 2).start()
        if s == 2:
            parts[0, :, columns] = merged

            @pl.when(jnp.logical_not(outer))
            def _():
                z_join(part).wait_recv()
                parts[0, :, columns] = parts[0, :, columns] + zret[0, :, columns].astype(jnp.float32)

            zsend[1, :, columns] = parts[0, :, columns].astype(jnp.bfloat16)
            z_back(2, part).start()
        return merged

    def sent_early():
        for k in range(n_sp):
            @pl.when(c == k)
            def _():
                for copy in first_sends[k] + late_sends[k]:
                    copy.wait_send()

        for h in range(heads):
            for d in range(1, n_tp):
                for b in range(2):
                    att_copy(h, b, d).wait_send()

                @pl.when(near(d))
                def _():
                    att_copy(h, 2, d).wait_send()

            relay_copy(h).wait_send()
        for d in (1, 2):
            for side in range(2):
                base_copy(d, side).wait_send()

    def sent_later():
        for s in range(n_z):
            for d in range(n_sp):
                if d and s != TWIN:
                    pack_copy(d, s).wait_send()
                if d and s in (1, 2):
                    for part in range(2):
                        back_copy(d, s, part).wait_send()
                if d and s == TWIN:
                    back_copy(d, s, 2).wait_send()
                share_copy(d, s).wait_send()
            pair_copy(s).wait_send()
        for d in range(n_sp):
            twin_copy(d).wait_send()

    @pl.when(c != n_sp - 1)
    def _():
        pl.semaphore_wait(go, 1)

    pack_rows(0)
    for load in loads[heads * n_tp :]:
        load.wait()
    far_rows(1)
    pack_rows(1)
    for d in range(1, n_sp):
        pack_copy(d, 0).wait_recv()
        twin_copy(d).start()
    far_rows(2)
    pack_rows(2)
    run_experts(0)
    sent_early()
    run_experts(1)
    reduce_pair(1)
    run_experts(TWIN)
    reduce_pair(TWIN)
    run_experts(2)
    reduce_pair(2)
    mix_rows(1, 0)
    mix_rows(1, 1)

    @pl.when(outer)
    def _():
        for d in (n_sp - 1, 0):
            fold_copy(d).start()

    mix_rows(TWIN, 2)
    mix_rows(2, 0)
    mix_rows(2, 1)
    sent_later()
    reduce_pair(0)
    parts[0] = updated[...].astype(jnp.float32)
    for part in range(2):
        columns = columns_of(part)

        @pl.when(outer)
        def _():
            z_back(1, part).wait_recv()
            parts[0, :, columns] = parts[0, :, columns] + zret[0, :, columns].astype(jnp.float32)

        z_back(2, part).wait_recv()
        parts[0, :, columns] = parts[0, :, columns] + zret[1, :, columns].astype(jnp.float32)
    z_back(TWIN, 2).wait_recv()
    parts[0, :, split:] = parts[0, :, split:] + zret[TWIN - 1, :, split:].astype(jnp.float32)
    for part in range(2):
        columns = columns_of(part)
        out_ref[:, columns] = (parts[0, :, columns] + mix_rows(0, part)).astype(jnp.bfloat16)

    for part in range(2):

        @pl.when(outer)
        def _():
            z_join(part).wait_send()

        @pl.when(jnp.logical_not(outer))
        def _():
            z_back(1, part).wait_send()

        z_back(2, part).wait_send()
    z_back(TWIN, 2).wait_send()
    for d in range(n_sp):
        fold_copy(d).wait_send()
        if d:
            for part in range(2):
                back_copy(d, 0, part).wait_send()


def whole_layer(
    queries,
    key_pairs,
    head_values,
    lambdas,
    head_gain,
    expert_ids,
    route_weights,
    residual,
    norm_gain,
    out_weight,
    gate_weight,
    up_weight,
    down_weight,
    n_sp,
    n_tp,
    cap,
):
    tokens, heads, pair = queries.shape
    rows, model = residual.shape
    width = head_values.shape[2]
    local = gate_weight.shape[0]
    n_z = n_tp // CORES
    tile = math.gcd(tokens, 256)
    tiles = tokens // tile
    dma = pltpu.SemaphoreType.DMA
    vmem = pl.BlockSpec(memory_space=pltpu.VMEM)
    hbm = pl.BlockSpec(memory_space=pl.ANY)
    block = (local, cap, model)
    flat = max(n_tp * width, n_z * n_sp * local * cap)

    def buffer(*shape):
        return pltpu.VMEM(shape, jnp.bfloat16)

    def single(*shape):
        return pltpu.VMEM(shape, jnp.float32)

    return pl.pallas_call(
        functools.partial(layer_kernel, n_sp, n_tp, (pair // 2) ** (-0.5)),
        out_shape=jax.ShapeDtypeStruct((rows, model), jnp.bfloat16),
        in_specs=[pl.BlockSpec(memory_space=pltpu.SMEM)] + [vmem] * 8 + [hbm] * 4,
        out_specs=vmem,
        scratch_shapes=[
            buffer(heads, tiles, 2 * tile, pair),
            buffer(heads, tokens, pair),
            buffer(heads, tokens, width),
            buffer(heads, 3, rows, n_tp * width),
            buffer(n_sp - 1, heads, 2, tokens, width),
            single(heads, tiles, 2 * tile, 2 * width),
            single(heads, tiles, 2 * tile, 1),
            buffer(heads, tokens, width),
            buffer(2, rows, model),
            buffer(rows, model),
            buffer(rows, model),
            single(4, 8, rows + -rows % 128),
            buffer(*gate_weight.shape),
            buffer(*up_weight.shape),
            buffer(*down_weight.shape),
            buffer(2, rows, model),
            buffer(3, n_sp - 1, *block),
            buffer(2, n_z, n_sp, *block),
            buffer(flat, model),
            buffer(n_z, n_sp, *block),
            buffer(flat, model),
            buffer(n_z, n_sp, *block),
            buffer(3, rows, model),
            buffer(3, rows, model),
            buffer(n_sp, local, cap, model - model // 4),
            single(3, rows, model),
            dma((n_sp + 1, 2)),
            dma((n_sp - 1, heads, 2)),
            dma((heads, 3, n_tp)),
            dma((heads, 3, n_tp)),
            dma((heads,)),
            dma((heads,)),
            dma((2, 2)),
            dma((2, 2)),
            dma((n_z,)),
            dma((n_z,)),
            dma((heads * n_tp + 3,)),
            dma((n_sp, n_z)),
            dma((n_sp, n_z)),
            dma((n_sp, n_z)),
            dma((n_sp, n_z)),
            dma((n_z,)),
            dma((n_z,)),
            dma((n_sp, n_z, 3)),
            dma((n_sp, n_z, 3)),
            dma((n_z, 3)),
            dma((n_z, 3)),
            dma((n_sp,)),
            dma((n_sp,)),
            dma((n_sp,)),
            dma((n_sp,)),
            pltpu.SemaphoreType.REGULAR,
        ],
        compiler_params=pltpu.CompilerParams(
            collective_id=2, has_side_effects=True, vmem_limit_bytes=VMEM_BYTES
        ),
        name="layer",
    )(
        lambdas,
        queries,
        key_pairs,
        head_values,
        head_gain.reshape(1, -1),
        expert_ids.T,
        route_weights.T,
        residual,
        norm_gain.reshape(1, -1),
        out_weight.reshape(n_tp, heads, width, model),
        gate_weight,
        up_weight,
        down_weight,
    )


def shards(
    queries,
    key_pairs,
    head_values,
    lambdas,
    head_gain,
    out_weight,
    residual,
    norm_gain,
    expert_ids,
    route_weights,
    gate_weight,
    up_weight,
    down_weight,
):
    tokens_here, heads_here, pair_width = queries.shape
    value_width = head_values.shape[2]
    rows_here = residual.shape[0]
    sp_count = lax.axis_size("sp")
    tp_count = lax.axis_size("tp")
    z_count = tp_count // CORES
    route_count = expert_ids.shape[1]
    local_experts = gate_weight.shape[0]
    expert_count = local_experts * sp_count
    capacity = max(2, 4 * rows_here * route_count // (3 * expert_count))
    model_width = residual.shape[1]
    block_bytes = z_count * local_experts * capacity * model_width * 2
    if sp_count == PLANE and z_count == LAYERS and heads_here == HEADS_HERE and pair_width == value_width and (
        capacity % 16 == 0 and rows_here <= 128 and route_count == 2
        and (7 * sp_count - 1) * block_bytes <= 3 * VMEM_BYTES // 5
    ):
        return whole_layer(
            queries,
            key_pairs,
            head_values,
            lambdas,
            head_gain,
            expert_ids,
            route_weights,
            residual,
            norm_gain,
            out_weight,
            gate_weight,
            up_weight,
            down_weight,
            sp_count,
            tp_count,
            capacity,
        )
    flat_ids = expert_ids.reshape(-1)
    indicator = (flat_ids[:, None] == jnp.arange(expert_count, dtype=jnp.int32)[None, :]).astype(
        jnp.int32
    )
    ranking = jnp.sum(jnp.cumsum(indicator, axis=0) * indicator, axis=1) - 1
    turned = (flat_ids - lax.axis_index("sp") * local_experts) % expert_count
    near_slots = (turned * capacity + ranking).reshape(rows_here, route_count)
    slots = flat_ids * capacity + ranking
    meta = jnp.concatenate([near_slots.astype(jnp.float32), route_weights], axis=1).T
    meta = jnp.pad(meta, ((0, 8 - 2 * route_count), (0, -rows_here % 128)), constant_values=-1.0)
    updated, normed, zmeta = attend(
        queries,
        key_pairs,
        head_values,
        lambdas,
        head_gain,
        meta,
        residual,
        norm_gain,
        out_weight,
        sp_count,
        tp_count,
    )
    if capacity % 16 == 0 and rows_here <= 128 and route_count == 2 and (
        (7 * sp_count - 1) * block_bytes <= 3 * VMEM_BYTES // 5
    ):
        return experts(
            normed, zmeta, updated, gate_weight, up_weight, down_weight, sp_count, z_count, capacity
        )
    sources = jnp.arange(rows_here * route_count, dtype=jnp.int32) // route_count
    outgoing = (
        jnp.zeros((expert_count * capacity, model_width), jnp.bfloat16)
        .at[slots]
        .set(normed[sources])
    )
    arrived = lax.all_to_all(
        outgoing.reshape(sp_count, local_experts, capacity, model_width),
        "sp",
        split_axis=0,
        concat_axis=0,
        tiled=True,
    )
    piece_rows = lax.all_gather(arrived[None], "tp", axis=0, tiled=True)
    gate_part = jnp.einsum(
        "tsecd,edf->tsecf", piece_rows, gate_weight, preferred_element_type=jnp.float32
    )
    up_part = jnp.einsum(
        "tsecd,edf->tsecf", piece_rows, up_weight, preferred_element_type=jnp.float32
    )
    inner_rows = (jax.nn.silu(gate_part) * up_part).astype(jnp.bfloat16)
    partial_value = jnp.einsum(
        "tsecf,efd->tsecd", inner_rows, down_weight, preferred_element_type=jnp.float32
    )
    reduced = lax.psum_scatter(
        partial_value.astype(jnp.bfloat16), "tp", scatter_dimension=0, tiled=True
    )
    returned = lax.all_to_all(reduced[0], "sp", split_axis=0, concat_axis=0, tiled=True)
    picked = (
        returned.reshape(expert_count * capacity, model_width)[slots]
        .astype(jnp.float32)
        .reshape(rows_here, route_count, model_width)
    )
    moe_sum = jnp.sum(picked * route_weights[:, :, None], axis=1)
    return (updated.astype(jnp.float32) + moe_sum).astype(jnp.bfloat16)


def solution(mesh):
    placed = (
        P("sp", "tp", None),
        P("sp", "tp", None),
        P("sp", "tp", None),
        P("tp"),
        P(),
        P(),
        P(("sp", "tp"), None),
        P(),
        P(("sp", "tp"), None),
        P(("sp", "tp"), None),
        P("sp", None, "tp"),
        P("sp", None, "tp"),
        P("sp", "tp", None),
    )
    return jax.shard_map(
        shards, mesh=mesh, in_specs=placed, out_specs=P(("sp", "tp"), None), check_vma=False
    )
```

```python
import functools
import math

import jax
import jax.numpy as jnp
from jax import lax
from jax.experimental import pallas as pl
from jax.experimental.pallas import tpu as pltpu
from jax.sharding import PartitionSpec as P

MESH = pl.DeviceIdType.MESH
LOG2E = 1.4426950408889634
CORES = 2
PLANE = 4
HEADS_HERE = 2
LAYERS = 4
TWIN = 3
VMEM_BYTES = 67043328


def attend_kernel(
    n_sp,
    n_tp,
    scale,
    lam_ref,
    q_ref,
    kv_ref,
    gain_ref,
    meta_ref,
    base_ref,
    norm_ref,
    w_hbm,
    updated_ref,
    normed_ref,
    zmeta_ref,
    weight,
    gathered,
    kvbuf,
    acc,
    top,
    tot,
    att,
    kv_send,
    kv_recv,
    at_send,
    at_recv,
    me_send,
    me_recv,
    own_sem,
    w_sem,
):
    heads, tiles, wide, _ = q_ref.shape
    tile = wide // 2
    rows = base_ref.shape[0]
    n_z = n_tp // CORES
    c = lax.axis_index("sp")
    t = lax.axis_index("tp")
    load = pltpu.make_async_copy(w_hbm, weight, w_sem)
    load.start()
    barrier = pltpu.get_barrier_semaphore()
    for d in range(1, n_sp):
        pl.semaphore_signal(barrier, inc=1, device_id=((c + d) % n_sp, t), device_id_type=MESH)
    for d in range(1, n_tp):
        pl.semaphore_signal(barrier, inc=1, device_id=(c, (t + d) % n_tp), device_id_type=MESH)
    pl.semaphore_wait(barrier, n_sp + n_tp - 2)

    def kv_copy(d, h):
        return pltpu.make_async_remote_copy(
            src_ref=kv_ref.at[h],
            dst_ref=kvbuf.at[d - 1, h],
            send_sem=kv_send.at[d - 1, h],
            recv_sem=kv_recv.at[d - 1, h],
            device_id=((c + d) % n_sp, t),
            device_id_type=MESH,
        )

    def meta_copy(d):
        return pltpu.make_async_remote_copy(
            src_ref=meta_ref,
            dst_ref=zmeta_ref.at[d],
            send_sem=me_send.at[d],
            recv_sem=me_recv.at[d],
            device_id=(c, (t + CORES * d) % n_tp),
            device_id_type=MESH,
        )

    for d in range(1, n_sp):
        @pl.when(c + d < n_sp)
        def _():
            for h in range(heads):
                kv_copy(d, h).start()

    for d in range(1, n_z):
        meta_copy(d).start()
    zmeta_ref[0] = meta_ref[...]

    factor = scale * LOG2E

    def scores_of(h, i, keys):
        return (
            lax.dot_general(
                q_ref[h, i], keys, (((1,), (1,)), ((), ())), preferred_element_type=jnp.float32
            )
            * factor
        )

    for i in range(tiles):
        extent = (i + 1) * tile
        for h in range(heads):
            s = scores_of(h, i, kv_ref[h, 0, :extent])
            row = lax.rem(lax.broadcasted_iota(jnp.int32, (wide, extent), 0), tile) + i * tile
            col = lax.broadcasted_iota(jnp.int32, (wide, extent), 1)
            s = jnp.where(col <= row, s, -jnp.inf)
            high = jnp.max(s, axis=1, keepdims=True)
            p = jnp.exp2(s - high)
            top[h, i] = high
            tot[h, i] = jnp.sum(p, axis=1, keepdims=True)
            acc[h, i] = jnp.dot(
                p.astype(jnp.bfloat16), kv_ref[h, 1, :extent], preferred_element_type=jnp.float32
            )

    def span_step(step, carry):
        for h in range(heads):
            kv_copy(step, h).wait_recv()

        def tile_step(i, inner):
            for h in range(heads):
                s = scores_of(h, i, kvbuf[step - 1, h, 0])
                before = top[h, i]
                high = jnp.maximum(before, jnp.max(s, axis=1, keepdims=True))
                p = jnp.exp2(s - high)
                decay = jnp.exp2(before - high)
                top[h, i] = high
                tot[h, i] = tot[h, i] * decay + jnp.sum(p, axis=1, keepdims=True)
                acc[h, i] = acc[h, i] * decay + jnp.dot(
                    p.astype(jnp.bfloat16),
                    kvbuf[step - 1, h, 1],
                    preferred_element_type=jnp.float32,
                )
            return inner

        return lax.fori_loop(0, tiles, tile_step, carry)

    lax.fori_loop(1, c + 1, span_step, 0)

    for h in range(heads):
        width = acc.shape[3]
        for i in range(tiles):
            both = acc[h, i] / tot[h, i]
            mixed = both[:tile] - lam_ref[h] * both[tile:]
            mean = jnp.mean(mixed * mixed, axis=1, keepdims=True)
            normed = mixed * lax.rsqrt(mean + 1e-06) * gain_ref[...]
            att[i * tile : (i + 1) * tile, h * width : (h + 1) * width] = normed.astype(att.dtype)

    def att_copy(d):
        to = (t + d) % n_tp
        return pltpu.make_async_remote_copy(
            src_ref=att.at[pl.ds(pl.multiple_of(to * rows, rows), rows)],
            dst_ref=gathered.at[t],
            send_sem=at_send.at[d],
            recv_sem=at_recv.at[d],
            device_id=(c, to),
            device_id_type=MESH,
        )

    for d in range(1, n_tp):
        att_copy(d).start()
    own = pltpu.make_async_copy(
        att.at[pl.ds(pl.multiple_of(t * rows, rows), rows)], gathered.at[t], own_sem
    )
    own.start()
    own.wait()
    load.wait()
    span = att.shape[1]
    projected = jnp.zeros(base_ref.shape, jnp.float32)
    for d in range(n_tp):
        if d:
            att_copy(d).wait_recv()
        source = (t - d + n_tp) % n_tp
        projected = projected + jnp.dot(
            gathered[source],
            weight[pl.ds(pl.multiple_of(source * span, span), span), :],
            preferred_element_type=jnp.float32,
        )
    updated = (base_ref[...].astype(jnp.float32) + projected).astype(jnp.bfloat16)
    updated_ref[...] = updated
    widened = updated.astype(jnp.float32)
    mean = jnp.mean(widened * widened, axis=1, keepdims=True)
    normed_ref[...] = (widened * lax.rsqrt(mean + 1e-06) * norm_ref[...]).astype(jnp.bfloat16)
    for d in range(1, n_tp):
        att_copy(d).wait_send()
    for d in range(1, n_z):
        meta_copy(d).wait()
    for d in range(1, n_sp):
        @pl.when(c + d < n_sp)
        def _():
            for h in range(heads):
                kv_copy(d, h).wait_send()


def attend(queries, key_pairs, head_values, lambdas, head_gain, meta, residual, norm_gain, out_weight, n_sp, n_tp):
    tokens, heads, pair = queries.shape
    rows = residual.shape[0]
    width = head_values.shape[2]
    half = pair // 2
    tile = math.gcd(tokens, 256)
    tiles = tokens // tile
    first = (jnp.arange(pair) < half)[None, :]
    q = jnp.transpose(queries, (1, 0, 2)).reshape(heads, tiles, 1, tile, pair)
    sides = jnp.stack([first, ~first])
    q = jnp.where(sides, q, jnp.zeros((), q.dtype)).reshape(heads, tiles, 2 * tile, pair)
    kv = jnp.transpose(jnp.stack([key_pairs, head_values]), (2, 0, 1, 3))
    dma = pltpu.SemaphoreType.DMA
    vmem = pl.BlockSpec(memory_space=pltpu.VMEM)
    n_z = n_tp // CORES
    return pl.pallas_call(
        functools.partial(attend_kernel, n_sp, n_tp, half ** (-0.5)),
        out_shape=(
            jax.ShapeDtypeStruct(residual.shape, jnp.bfloat16),
            jax.ShapeDtypeStruct(residual.shape, jnp.bfloat16),
            jax.ShapeDtypeStruct((n_z,) + meta.shape, meta.dtype),
        ),
        in_specs=[pl.BlockSpec(memory_space=pltpu.SMEM)] + [vmem] * 6
        + [pl.BlockSpec(memory_space=pl.ANY)],
        out_specs=(vmem, vmem, vmem),
        scratch_shapes=[
            pltpu.VMEM(out_weight.shape, out_weight.dtype),
            pltpu.VMEM((n_tp, rows, heads * width), jnp.bfloat16),
            pltpu.VMEM((n_sp - 1,) + kv.shape, kv.dtype),
            pltpu.VMEM((heads, tiles, 2 * tile, width), jnp.float32),
            pltpu.VMEM((heads, tiles, 2 * tile, 1), jnp.float32),
            pltpu.VMEM((heads, tiles, 2 * tile, 1), jnp.float32),
            pltpu.VMEM((tokens, heads * width), jnp.bfloat16),
            dma((n_sp - 1, heads)),
            dma((n_sp - 1, heads)),
            dma((n_tp,)),
            dma((n_tp,)),
            dma((n_z,)),
            dma((n_z,)),
            dma,
            dma,
        ],
        compiler_params=pltpu.CompilerParams(
            collective_id=0, has_side_effects=True, vmem_limit_bytes=48 * 1024 * 1024
        ),
        name="attend",
    )(lambdas, q, kv, head_gain.reshape(1, -1), meta, residual, norm_gain.reshape(1, -1), out_weight)


def experts_kernel(
    n_sp,
    n_z,
    x_ref,
    meta_ref,
    base_ref,
    gate_hbm,
    up_hbm,
    down_hbm,
    out_ref,
    gate,
    up,
    down,
    zrows,
    pack,
    arrived,
    psend,
    own,
    precv,
    ret,
    zsend,
    zret,
    mine,
    w_sem,
    zs_send,
    zs_recv,
    ps_send,
    ps_recv,
    fw_send,
    fw_recv,
    pp_send,
    pp_recv,
    rt_send,
    rt_recv,
    zr_send,
    zr_recv,
):
    rows, model = x_ref.shape
    local, cap = pack.shape[2], pack.shape[3]
    slots = n_sp * local * cap
    c = lax.axis_index("sp")
    t = lax.axis_index("tp")
    n_tp = n_z * CORES
    core = t % CORES
    partner = (c, t + 1 - 2 * core)
    loads = [
        pltpu.make_async_copy(a, b, w_sem.at[i])
        for i, (a, b) in enumerate(((gate_hbm, gate), (up_hbm, up), (down_hbm, down)))
    ]
    for load in loads:
        load.start()

    def column(d):
        return ((c + d) % n_sp, t)

    def layer(d):
        return (c, (t + CORES * d) % n_tp)

    barrier = pltpu.get_barrier_semaphore()
    for d in range(1, n_sp):
        pl.semaphore_signal(barrier, inc=1, device_id=column(d), device_id_type=MESH)
    for d in range(1, n_z):
        pl.semaphore_signal(barrier, inc=1, device_id=layer(d), device_id_type=MESH)
    pl.semaphore_signal(barrier, inc=1, device_id=partner, device_id_type=MESH)
    pl.semaphore_wait(barrier, n_sp + n_z - 1)

    def remote(src, dst, send, recv, target):
        return pltpu.make_async_remote_copy(
            src_ref=src,
            dst_ref=dst,
            send_sem=send,
            recv_sem=recv,
            device_id=target,
            device_id_type=MESH,
        )

    def z_copy(d):
        return remote(x_ref, zrows.at[d - 1], zs_send.at[d], zs_recv.at[d], layer(d))

    def pack_copy(d, s):
        return remote(
            pack.at[s, d - 1], arrived.at[0, s, d], ps_send.at[d, s], ps_recv.at[d, s], column(d)
        )

    def share_copy(d, s):
        return remote(
            arrived.at[0, s, d], arrived.at[1, s, d], fw_send.at[d, s], fw_recv.at[d, s], partner
        )

    def pair_copy(s):
        return remote(psend.at[s], precv.at[s], pp_send.at[s], pp_recv.at[s], partner)

    def back_copy(d, s):
        return remote(
            own.at[s, d], ret.at[s, d], rt_send.at[d, s], rt_recv.at[d, s], column(n_sp - d)
        )

    def z_back(d):
        return remote(
            zsend.at[d], zret.at[d], zr_send.at[d], zr_recv.at[d], layer(n_z - d)
        )

    for d in range(1, n_z):
        z_copy(d).start()

    def route_hits(s, r):
        target = lax.broadcasted_iota(jnp.int32, (slots, rows), 0).astype(jnp.float32)
        return target == meta_ref[s, r : r + 1, :rows]

    def pack_rows(s):
        if s:
            z_copy(s).wait_recv()
        hits = route_hits(s, 0) | route_hits(s, 1)
        pick = jnp.where(hits, 1.0, 0.0).astype(jnp.bfloat16)
        source = x_ref[...] if s == 0 else zrows[s - 1]
        packed = (
            jnp.dot(pick, source, preferred_element_type=jnp.float32)
            .astype(jnp.bfloat16)
            .reshape(n_sp, local, cap, model)
        )
        for d in range(1, n_sp):
            pack[s, d - 1] = packed[d]
            pack_copy(d, s).start()
        arrived[0, s, 0] = packed[0]
        share_copy(0, s).start()

    def run_experts(s):
        for d in range(1, n_sp):
            pack_copy(d, s).wait_recv()
            share_copy(d, s).start()
        for d in range(n_sp):
            share_copy(d, s).wait_recv()

        def expert_step(e, carry):
            x = arrived[:, s, :, e].reshape(2 * n_sp * cap, model)
            gated = jnp.dot(x, gate[e], preferred_element_type=jnp.float32)
            lifted = jnp.dot(x, up[e], preferred_element_type=jnp.float32)
            inner = (gated / (1.0 + jnp.exp(-gated)) * lifted).astype(jnp.bfloat16)
            y = jnp.dot(inner, down[e], preferred_element_type=jnp.float32)
            y = y.astype(jnp.bfloat16).reshape(2, n_sp, cap, model)
            own[s, :, e] = y[0]
            psend[s, :, e] = y[1]
            return carry

        lax.fori_loop(0, local, expert_step, 0)
        pair_copy(s).start()

    def reduce_pair(s):
        pair_copy(s).wait_recv()
        for d in list(range(1, n_sp)) + [0]:
            total = own[s, d].astype(jnp.float32) + precv[s, d].astype(jnp.float32)
            total = total.astype(jnp.bfloat16)
            if d == 0:
                ret[s, 0] = total
            else:
                own[s, d] = total
                back_copy(d, s).start()

    def mix_rows(s):
        for d in range(1, n_sp):
            back_copy(d, s).wait_recv()
        mixing = jnp.where(route_hits(s, 0), meta_ref[s, 2:3, :rows], 0.0) + jnp.where(
            route_hits(s, 1), meta_ref[s, 3:4, :rows], 0.0
        )
        high = mixing.astype(jnp.bfloat16)
        low = (mixing - high.astype(jnp.float32)).astype(jnp.bfloat16)
        back = ret[s].reshape(slots, model)
        numbers = (((0,), (0,)), ((), ()))
        merged = lax.dot_general(
            high, back, numbers, preferred_element_type=jnp.float32
        ) + lax.dot_general(low, back, numbers, preferred_element_type=jnp.float32)
        if s:
            zsend[s] = merged.astype(jnp.bfloat16)
            z_back(s).start()
        else:
            mine[...] = merged

    pack_rows(0)
    for load in loads:
        load.wait()
    if n_z > 1:
        pack_rows(1)
    for s in range(n_z):
        run_experts(s)
        if s + 2 < n_z:
            pack_rows(s + 2)
        elif s + 2 - n_z < n_z - 2:
            mix_rows(s + 2 - n_z)
        reduce_pair(s)
    for s in range(max(0, n_z - 2), n_z):
        mix_rows(s)
    merged = mine[...]
    for s in range(1, n_z):
        z_back(s).wait_recv()
        merged = merged + zret[s].astype(jnp.float32)
    out_ref[...] = (base_ref[...].astype(jnp.float32) + merged).astype(jnp.bfloat16)

    for d in range(1, n_z):
        z_copy(d).wait_send()
        z_back(d).wait_send()
    for s in range(n_z):
        for d in range(n_sp):
            if d:
                pack_copy(d, s).wait_send()
                back_copy(d, s).wait_send()
            share_copy(d, s).wait_send()
        pair_copy(s).wait_send()


def experts(normed, zmeta, updated, gate_weight, up_weight, down_weight, n_sp, n_z, cap):
    rows, model = normed.shape
    local = gate_weight.shape[0]
    dma = pltpu.SemaphoreType.DMA
    vmem = pl.BlockSpec(memory_space=pltpu.VMEM)
    hbm = pl.BlockSpec(memory_space=pl.ANY)
    block = (local, cap, model)

    def buffer(*shape):
        return pltpu.VMEM(shape, jnp.bfloat16)

    return pl.pallas_call(
        functools.partial(experts_kernel, n_sp, n_z),
        out_shape=jax.ShapeDtypeStruct((rows, model), jnp.bfloat16),
        in_specs=[vmem] * 3 + [hbm] * 3,
        out_specs=vmem,
        scratch_shapes=[
            buffer(*gate_weight.shape),
            buffer(*up_weight.shape),
            buffer(*down_weight.shape),
            buffer(n_z - 1, rows, model),
            buffer(n_z, n_sp - 1, *block),
            buffer(2, n_z, n_sp, *block),
            buffer(n_z, n_sp, *block),
            buffer(n_z, n_sp, *block),
            buffer(n_z, n_sp, *block),
            buffer(n_z, n_sp, *block),
            buffer(n_z, rows, model),
            buffer(n_z, rows, model),
            pltpu.VMEM((rows, model), jnp.float32),
            dma((3,)),
            dma((n_z,)),
            dma((n_z,)),
            dma((n_sp, n_z)),
            dma((n_sp, n_z)),
            dma((n_sp, n_z)),
            dma((n_sp, n_z)),
            dma((n_z,)),
            dma((n_z,)),
            dma((n_sp, n_z)),
            dma((n_sp, n_z)),
            dma((n_z,)),
            dma((n_z,)),
        ],
        compiler_params=pltpu.CompilerParams(
            collective_id=1, has_side_effects=True, vmem_limit_bytes=VMEM_BYTES
        ),
        name="experts",
    )(normed, zmeta, updated, gate_weight, up_weight, down_weight)


def layer_kernel(
    n_sp,
    n_tp,
    scale,
    lam_ref,
    raw_q,
    raw_k,
    raw_v,
    gain_ref,
    ids_ref,
    mix_ref,
    base_ref,
    norm_ref,
    w_hbm,
    gate_hbm,
    up_hbm,
    down_hbm,
    out_ref,
    q_ref,
    k_ref,
    v_ref,
    gathered,
    kvbuf,
    acc,
    top,
    att,
    bases,
    updated,
    x_ref,
    zmeta,
    gate,
    up,
    down,
    zrows,
    pack,
    arrived,
    psend,
    own,
    precv,
    ret,
    zsend,
    zret,
    fold,
    parts,
    kv_send,
    kv_recv,
    at_send,
    at_recv,
    ar_send,
    ar_recv,
    ba_send,
    ba_recv,
    me_send,
    me_recv,
    w_sem,
    ps_send,
    ps_recv,
    fw_send,
    fw_recv,
    pp_send,
    pp_recv,
    rt_send,
    rt_recv,
    zr_send,
    zr_recv,
    tw_send,
    tw_recv,
    fo_send,
    fo_recv,
    go,
):
    heads, tiles, wide, _ = q_ref.shape
    tile = wide // 2
    rows, model = base_ref.shape
    width = v_ref.shape[2]
    n_z = n_tp // CORES
    local, cap = pack.shape[2], pack.shape[3]
    slots = n_sp * local * cap
    span = n_sp * local * cap
    c = lax.axis_index("sp")
    t = lax.axis_index("tp")
    core = t % CORES
    partner = (c, t + 1 - 2 * core)

    def column(d):
        return ((c + d) % n_sp, t)

    z = t // CORES
    twin_z = z + 1 - 2 * (z % 2)
    far_z = (z + n_z // 2) % n_z
    twin = (c, twin_z * CORES + core)
    far = [
        None,
        (c, far_z * CORES + core),
        (c, (far_z + 1 - 2 * (far_z % 2)) * CORES + core),
        twin,
    ]
    split = fold.shape[3]

    weight = (psend, precv)
    loads = [
        pltpu.make_async_copy(a, b, w_sem.at[i])
        for i, (a, b) in enumerate(
            [
                (w_hbm.at[source, h], weight[h].at[source * width : (source + 1) * width])
                for h in range(heads)
                for source in range(n_tp)
            ]
            + [(gate_hbm, gate), (up_hbm, up), (down_hbm, down)]
        )
    ]
    for load in loads:
        load.start()
    barrier = pltpu.get_barrier_semaphore()
    for d in range(1, n_sp):
        pl.semaphore_signal(barrier, inc=1, device_id=column(d), device_id_type=MESH)
    for d in range(1, n_tp):
        pl.semaphore_signal(barrier, inc=1, device_id=(c, (t + d) % n_tp), device_id_type=MESH)
    for h in range(heads):
        k_ref[h] = raw_k[:, h, :]
        v_ref[h] = raw_v[:, h, :]
    pl.semaphore_wait(barrier, n_sp + n_tp - 2)

    def remote(src, dst, send, recv, target):
        return pltpu.make_async_remote_copy(
            src_ref=src,
            dst_ref=dst,
            send_sem=send,
            recv_sem=recv,
            device_id=target,
            device_id_type=MESH,
        )

    def kv_copies(slot, source, h, to, mine_too, parts=(0, 1)):
        return [
            remote(
                (k_ref, v_ref)[part].at[h] if mine_too else kvbuf.at[source, h, part],
                kvbuf.at[source, h, part],
                kv_send.at[slot, part],
                kv_recv.at[source, h, part],
                (to, t),
            )
            for part in parts
        ]

    def kv_wait(source, h):
        for part in range(2):
            remote(
                kvbuf.at[source, h, part],
                kvbuf.at[source, h, part],
                kv_send.at[0, part],
                kv_recv.at[source, h, part],
                partner,
            ).wait_recv()

    first_sends = [
        kv_copies(0, 0, 0, 2, True)
        + kv_copies(1, 0, 1, 1, True)
        + kv_copies(2, 0, 1, 2, True)
        + kv_copies(3, 0, 0, 1, True),
        kv_copies(0, 1, 0, 3, True) + kv_copies(1, 1, 1, 0, True) + kv_copies(2, 1, 1, 3, True),
        kv_copies(0, 2, 0, 3, True) + kv_copies(1, 2, 1, 3, True, (0,)),
        [],
    ]
    relayed = [(1, 1), (0, 1), (0, 0), (1, 0)]
    late_sends = [
        kv_copies(4, 1, 1, 2, False),
        kv_copies(3, 0, 1, 3, False),
        kv_copies(2, 0, 0, 3, False) + kv_copies(1, 2, 1, 3, True, (1,)),
        kv_copies(0, 1, 0, 2, False),
    ]

    def meta_copy(d):
        return remote(zmeta.at[0], zmeta.at[d], me_send.at[d], me_recv.at[d], far[d])

    for k in range(n_sp):
        @pl.when(c == k)
        def _():
            for copy in first_sends[k]:
                copy.start()

    def base_copy(d, side):
        columns = slice(side * (model // 2), (side + 1) * (model // 2))
        return remote(
            base_ref.at[:, columns] if d == 1 else bases.at[0, :, columns],
            bases.at[d - 1, :, columns],
            ba_send.at[d - 1, side],
            ba_recv.at[d - 1, side],
            far[1] if d == 1 else twin,
        )

    def pass_base(side):
        base_copy(1, side).wait_recv()
        base_copy(2, side).start()

    for side in range(2):
        base_copy(1, side).start()

    experts = n_sp * local
    shape = (experts, rows)
    names = lax.broadcasted_iota(jnp.int32, shape, 0)
    named = [names == ids_ref[r : r + 1, :] for r in range(2)]
    chosen = jnp.where(named[0] | named[1], 1.0, 0.0).astype(jnp.bfloat16)
    earlier = lax.broadcasted_iota(jnp.int32, (rows, rows), 0) < lax.broadcasted_iota(
        jnp.int32, (rows, rows), 1
    )
    ranks = jnp.dot(
        chosen, jnp.where(earlier, 1.0, 0.0).astype(jnp.bfloat16), preferred_element_type=jnp.float32
    )
    zmeta[0] = jnp.full(zmeta.shape[1:], -1.0, jnp.float32)
    for r in range(2):
        turned = ids_ref[r : r + 1, :] - c * local
        turned = jnp.where(turned < 0, turned + experts, turned)
        rank = jnp.sum(jnp.where(named[r], ranks, 0.0), axis=0, keepdims=True)
        zmeta[0, r : r + 1, :rows] = (turned * cap).astype(jnp.float32) + rank
        zmeta[0, 2 + r : 3 + r, :rows] = mix_ref[r : r + 1, :]
    for d in (1, 2, TWIN):
        meta_copy(d).start()

    side = lax.broadcasted_iota(jnp.int32, (tile, raw_q.shape[2]), 1) < raw_q.shape[2] // 2
    for h in range(heads):
        att[h] = raw_q[:, h, :]
        for i in range(tiles):
            part = att[h, i * tile : (i + 1) * tile]
            q_ref[h, i, :tile] = jnp.where(side, part, jnp.zeros_like(part))
            q_ref[h, i, tile:] = jnp.where(side, jnp.zeros_like(part), part)

    factor = scale * LOG2E

    def scores_of(h, i, keys):
        return (
            lax.dot_general(
                q_ref[h, i], keys, (((1,), (1,)), ((), ())), preferred_element_type=jnp.float32
            )
            * factor
        )

    def with_ones(values):
        return jnp.concatenate([values, jnp.ones_like(values)], axis=1)

    for i in range(tiles):
        extent = (i + 1) * tile
        for h in range(heads):
            s = scores_of(h, i, k_ref[h, :extent])
            row = lax.rem(lax.broadcasted_iota(jnp.int32, (wide, extent), 0), tile) + i * tile
            col = lax.broadcasted_iota(jnp.int32, (wide, extent), 1)
            s = jnp.where(col <= row, s, -jnp.inf)
            high = jnp.max(s, axis=1, keepdims=True)
            p = jnp.exp2(s - high)
            top[h, i] = high
            acc[h, i] = jnp.dot(
                p.astype(jnp.bfloat16),
                with_ones(v_ref[h, :extent]),
                preferred_element_type=jnp.float32,
            )

    for k in range(n_sp):
        @pl.when(c == k)
        def _():
            kv_wait(*relayed[k])
            for copy in late_sends[k]:
                copy.start()

    pass_base(0)

    def order_of(orders):
        codes = [sum((2 * s + h) * 8**j for j, (s, h) in enumerate(o)) for o in orders]
        code, count = jnp.int32(codes[0]), jnp.int32(len(orders[0]))
        for k in range(1, n_sp):
            code = jnp.where(c == k, codes[k], code)
            count = jnp.where(c == k, len(orders[k]), count)
        return code, count

    def absorb(orders, waited, passing=False):
        code, count = order_of(orders)

        def piece_step(j, code):
            piece = code % 8
            source, h = piece // 2, piece % 2

            @pl.when(j >= waited)
            def _():
                kv_wait(source, h)

            if passing:

                @pl.when(j == count - 1)
                def _():
                    pass_base(1)

            keys, values = kvbuf[source, h, 0], with_ones(kvbuf[source, h, 1])
            results = []
            for i in range(tiles):
                s = scores_of(h, i, keys)
                before = top[h, i]
                high = jnp.maximum(before, jnp.max(s, axis=1, keepdims=True))
                p = jnp.exp2(s - high)
                decay = jnp.exp2(before - high)
                summed = acc[h, i] * decay + jnp.dot(
                    p.astype(jnp.bfloat16), values, preferred_element_type=jnp.float32
                )
                results.append((high, summed))
            for i in range(tiles):
                top[h, i], acc[h, i] = results[i]
            return code // 8

        lax.fori_loop(0, count, piece_step, code)

    half = n_z // 2

    def block_rows(b, to_z, to_core):
        layer = to_z if b == 0 else (to_z + half) % n_z
        if b == 2:
            layer = layer + 1 - 2 * (layer % 2)
        return pl.ds(pl.multiple_of((layer * CORES + to_core) * rows, rows), rows)

    here = pl.ds(pl.multiple_of(t * width, width), width)

    def att_copy(h, b, d):
        to = (t + d) % n_tp
        return remote(
            att.at[h, block_rows(b, to // CORES, to % CORES)],
            gathered.at[h, b, :, here],
            at_send.at[h, b, d],
            at_recv.at[h, b, d],
            (c, to),
        )

    def relay_copy(h):
        side = half * CORES * width
        across = pl.ds(pl.multiple_of((1 - z // half) * side, side), side)
        return remote(
            gathered.at[h, 1, :, across],
            gathered.at[h, 2, :, across],
            ar_send.at[h],
            ar_recv.at[h],
            twin,
        )

    def near(d):
        return ((t + d) % n_tp) // CORES // half == z // half

    def finish(h):
        for i in range(tiles):
            both = acc[h, i, :, :width] / acc[h, i, :, width:]
            mixed = both[:tile] - lam_ref[h] * both[tile:]
            mean = jnp.mean(mixed * mixed, axis=1, keepdims=True)
            normed = mixed * lax.rsqrt(mean + 1e-06) * gain_ref[...]
            att[h, i * tile : (i + 1) * tile] = normed.astype(att.dtype)
        for d in range(1, n_tp):
            att_copy(h, 0, d).start()
        for b in range(3):
            gathered[h, b, :, here] = att[h, block_rows(b, z, core)]

    def finish_far():
        for h in range(heads):
            for d in range(1, n_tp):
                att_copy(h, 1, d).start()
        for h in range(heads):
            for d in range(1, n_tp):

                @pl.when(near(d))
                def _():
                    att_copy(h, 2, d).start()


    def await_rows(h, b):
        for d in range(1, n_tp):
            if b < 2:
                att_copy(h, b, d).wait_recv()
            else:

                @pl.when(near(n_tp - d))
                def _():
                    att_copy(h, b, d).wait_recv()

        if b == 1:
            relay_copy(h).start()
        if b == 2:
            relay_copy(h).wait_recv()

    def project(h, b):
        return jnp.dot(
            gathered[h, b], weight[h][: n_tp * width], preferred_element_type=jnp.float32
        )

    def normalize(base, projected):
        new = (base.astype(jnp.float32) + projected).astype(jnp.bfloat16)
        widened = new.astype(jnp.float32)
        mean = jnp.mean(widened * widened, axis=1, keepdims=True)
        return new, (widened * lax.rsqrt(mean + 1e-06) * norm_ref[...]).astype(jnp.bfloat16)

    def far_rows(b):
        await_rows(0, b)
        parts[b] = project(0, b)
        await_rows(1, b)
        if b == 2:
            for part in range(2):
                base_copy(2, part).wait_recv()
        _, normed = normalize(bases[b - 1], parts[b] + project(1, b))
        zrows[b - 1] = normed

    absorb([[], [(0, 1), (0, 0)], [(0, 0), (0, 1), (1, 0)], [(1, 0), (2, 0), (1, 1), (0, 0)]], 1, True)

    @pl.when(c == 0)
    def _():
        pass_base(1)

    finish(0)
    absorb([[], [], [(1, 1)], [(2, 1), (0, 1)]], 0)

    @pl.when(c == n_sp - 1)
    def _():
        for d in range(1, n_sp):
            pl.semaphore_signal(go, inc=1, device_id=column(d), device_id_type=MESH)

    finish(1)
    finish_far()
    for load in loads[: heads * n_tp]:
        load.wait()
    await_rows(0, 0)
    parts[0] = project(0, 0)
    await_rows(1, 0)
    new, normed = normalize(base_ref[...], parts[0] + project(1, 0))
    updated[...] = new
    x_ref[...] = normed

    def pack_copy(d, s):
        return remote(
            pack.at[s, d - 1], arrived.at[0, s, d], ps_send.at[d, s], ps_recv.at[d, s], column(d)
        )

    def share_copy(d, s):
        return remote(
            arrived.at[0, s, d], arrived.at[1, s, d], fw_send.at[d, s], fw_recv.at[d, s], partner
        )

    def twin_copy(d):
        return remote(
            arrived.at[0, 0, d], arrived.at[0, TWIN, d], tw_send.at[d], tw_recv.at[d], twin
        )

    def pair_copy(s):
        block = pl.ds(s * span, span)
        return remote(psend.at[block], precv.at[block], pp_send.at[s], pp_recv.at[s], partner)

    def fold_copy(d):
        return remote(
            own.at[TWIN, d, :, :, :split], fold.at[d], fo_send.at[d], fo_recv.at[d], twin
        )

    def columns_of(part):
        if part == 2:
            return slice(split, model)
        return slice(part * (model // 2), (part + 1) * (model // 2))

    def back_copy(d, s, part):
        return remote(
            own.at[s, d, :, :, columns_of(part)],
            ret.at[s, d, :, :, columns_of(part)],
            rt_send.at[d, s, part],
            rt_recv.at[d, s, part],
            column(n_sp - d),
        )

    def z_part(d, part, target):
        return remote(
            zsend.at[d - 1, :, columns_of(part)],
            zret.at[d - 1, :, columns_of(part)],
            zr_send.at[d, part],
            zr_recv.at[d, part],
            target,
        )

    def z_back(d, part):
        return z_part(d, part, far[d])

    def z_join(part):
        return remote(
            zsend.at[0, :, columns_of(part)],
            zret.at[0, :, columns_of(part)],
            zr_send.at[0, part],
            zr_recv.at[0, part],
            twin,
        )

    outer = (z == 0) | (z == n_z - 1)
    for d in (1, 2, TWIN):
        meta_copy(d).wait()

    def route_hits(s, r):
        target = lax.broadcasted_iota(jnp.int32, (slots, rows), 0).astype(jnp.float32)
        return target == zmeta[s, r : r + 1, :rows]

    def pack_rows(s):
        hits = route_hits(s, 0) | route_hits(s, 1)
        pick = jnp.where(hits, 1.0, 0.0).astype(jnp.bfloat16)
        source = x_ref[...] if s == 0 else zrows[s - 1]
        packed = (
            jnp.dot(pick, source, preferred_element_type=jnp.float32)
            .astype(jnp.bfloat16)
            .reshape(n_sp, local, cap, model)
        )
        if s == 0:
            arrived[0, 0, 0] = packed[0]
            twin_copy(0).start()
        for d in range(1, n_sp):
            pack[s, d - 1] = packed[d]
            pack_copy(d, s).start()
        if s:
            arrived[0, s, 0] = packed[0]
        share_copy(0, s).start()

    def rows_here(s):
        for d in range(n_sp):
            if s == TWIN:
                twin_copy(d).wait_recv()
            elif s and d:
                pack_copy(d, s).wait_recv()
            if s == TWIN or d:
                share_copy(d, s).start()
        for d in range(n_sp):
            share_copy(d, s).wait_recv()

    def run_experts(s):
        rows_here(s)

        def expert_step(e, carry):
            x = arrived[:, s, :, e].reshape(2 * n_sp * cap, model)
            gated = jnp.dot(x, gate[e], preferred_element_type=jnp.float32)
            lifted = jnp.dot(x, up[e], preferred_element_type=jnp.float32)
            inner = (gated / (1.0 + jnp.exp(-gated)) * lifted).astype(jnp.bfloat16)
            y = jnp.dot(inner, down[e], preferred_element_type=jnp.float32)
            y = y.astype(jnp.bfloat16).reshape(2, n_sp, cap, model)
            own[s, :, e] = y[0]
            for d in range(n_sp):
                place = pl.multiple_of(s * span + (d * local + e) * cap, cap)
                psend[pl.ds(place, cap)] = y[1, d]
            return carry

        lax.fori_loop(0, local, expert_step, 0)
        pair_copy(s).start()

    def reduce_pair(s):
        pair_copy(s).wait_recv()
        for d in list(range(1, n_sp)) + [0]:
            other = precv[s * span + d * local * cap : s * span + (d + 1) * local * cap]
            total = own[s, d].astype(jnp.float32) + other.reshape(local, cap, model).astype(
                jnp.float32
            )
            if s == 0:
                fold_copy(d).wait_recv()
                total = jnp.concatenate(
                    [total[:, :, :split] + fold[d].astype(jnp.float32), total[:, :, split:]], axis=2
                )
            total = total.astype(jnp.bfloat16)
            if s == TWIN:
                own[s, d] = total
                if d:
                    fold_copy(d).start()
                else:

                    @pl.when(jnp.logical_not(outer))
                    def _():
                        fold_copy(d).start()

                if d:
                    back_copy(d, TWIN, 2).start()
                else:
                    ret[TWIN, 0, :, :, split:] = total[:, :, split:]
            elif d == 0:
                ret[s, 0] = total
            else:
                own[s, d] = total
                back_copy(d, s, 0).start()
                if s == 0:
                    back_copy(d, s, 1).start()
        if s in (1, 2):
            for d in range(1, n_sp):
                back_copy(d, s, 1).start()

    def mix_rows(s, part):
        for d in range(1, n_sp):
            back_copy(d, s, part).wait_recv()
        columns = columns_of(part)
        mixing = jnp.where(route_hits(s, 0), zmeta[s, 2:3, :rows], 0.0) + jnp.where(
            route_hits(s, 1), zmeta[s, 3:4, :rows], 0.0
        )
        high = mixing.astype(jnp.bfloat16)
        low = (mixing - high.astype(jnp.float32)).astype(jnp.bfloat16)
        back = ret[s, :, :, :, columns].reshape(slots, -1)
        numbers = (((0,), (0,)), ((), ()))
        merged = lax.dot_general(
            high, back, numbers, preferred_element_type=jnp.float32
        ) + lax.dot_general(low, back, numbers, preferred_element_type=jnp.float32)
        if s == 1:
            zsend[0, :, columns] = merged.astype(jnp.bfloat16)

            @pl.when(outer)
            def _():
                z_join(part).start()

            @pl.when(jnp.logical_not(outer))
            def _():
                z_back(1, part).start()

        if s == TWIN:
            zsend[TWIN - 1, :, columns] = merged.astype(jnp.bfloat16)
            z_back(TWIN, 2).start()
        if s == 2:
            parts[0, :, columns] = merged

            @pl.when(jnp.logical_not(outer))
            def _():
                z_join(part).wait_recv()
                parts[0, :, columns] = parts[0, :, columns] + zret[0, :, columns].astype(jnp.float32)

            zsend[1, :, columns] = parts[0, :, columns].astype(jnp.bfloat16)
            z_back(2, part).start()
        return merged

    def sent_early():
        for k in range(n_sp):
            @pl.when(c == k)
            def _():
                for copy in first_sends[k] + late_sends[k]:
                    copy.wait_send()

        for h in range(heads):
            for d in range(1, n_tp):
                for b in range(2):
                    att_copy(h, b, d).wait_send()

                @pl.when(near(d))
                def _():
                    att_copy(h, 2, d).wait_send()

            relay_copy(h).wait_send()
        for d in (1, 2):
            for side in range(2):
                base_copy(d, side).wait_send()

    def sent_later():
        for s in range(n_z):
            for d in range(n_sp):
                if d and s != TWIN:
                    pack_copy(d, s).wait_send()
                if d and s in (1, 2):
                    for part in range(2):
                        back_copy(d, s, part).wait_send()
                if d and s == TWIN:
                    back_copy(d, s, 2).wait_send()
                share_copy(d, s).wait_send()
            pair_copy(s).wait_send()
        for d in range(n_sp):
            twin_copy(d).wait_send()

    @pl.when(c != n_sp - 1)
    def _():
        pl.semaphore_wait(go, 1)

    pack_rows(0)
    for load in loads[heads * n_tp :]:
        load.wait()
    far_rows(1)
    pack_rows(1)
    for d in range(1, n_sp):
        pack_copy(d, 0).wait_recv()
        twin_copy(d).start()
    far_rows(2)
    pack_rows(2)
    run_experts(0)
    sent_early()
    run_experts(1)
    reduce_pair(1)
    run_experts(TWIN)
    reduce_pair(TWIN)
    run_experts(2)
    reduce_pair(2)
    mix_rows(1, 0)
    mix_rows(1, 1)

    @pl.when(outer)
    def _():
        fold_copy(0).start()

    mix_rows(TWIN, 2)
    mix_rows(2, 0)
    mix_rows(2, 1)
    sent_later()
    reduce_pair(0)
    parts[0] = updated[...].astype(jnp.float32)
    for part in range(2):
        columns = columns_of(part)

        @pl.when(outer)
        def _():
            z_back(1, part).wait_recv()
            parts[0, :, columns] = parts[0, :, columns] + zret[0, :, columns].astype(jnp.float32)

        z_back(2, part).wait_recv()
        parts[0, :, columns] = parts[0, :, columns] + zret[1, :, columns].astype(jnp.float32)
    z_back(TWIN, 2).wait_recv()
    parts[0, :, split:] = parts[0, :, split:] + zret[TWIN - 1, :, split:].astype(jnp.float32)
    for part in range(2):
        columns = columns_of(part)
        out_ref[:, columns] = (parts[0, :, columns] + mix_rows(0, part)).astype(jnp.bfloat16)

    for part in range(2):

        @pl.when(outer)
        def _():
            z_join(part).wait_send()

        @pl.when(jnp.logical_not(outer))
        def _():
            z_back(1, part).wait_send()

        z_back(2, part).wait_send()
    z_back(TWIN, 2).wait_send()
    for d in range(n_sp):
        fold_copy(d).wait_send()
        if d:
            for part in range(2):
                back_copy(d, 0, part).wait_send()


def whole_layer(
    queries,
    key_pairs,
    head_values,
    lambdas,
    head_gain,
    expert_ids,
    route_weights,
    residual,
    norm_gain,
    out_weight,
    gate_weight,
    up_weight,
    down_weight,
    n_sp,
    n_tp,
    cap,
):
    tokens, heads, pair = queries.shape
    rows, model = residual.shape
    width = head_values.shape[2]
    local = gate_weight.shape[0]
    n_z = n_tp // CORES
    tile = math.gcd(tokens, 256)
    tiles = tokens // tile
    dma = pltpu.SemaphoreType.DMA
    vmem = pl.BlockSpec(memory_space=pltpu.VMEM)
    hbm = pl.BlockSpec(memory_space=pl.ANY)
    block = (local, cap, model)
    flat = max(n_tp * width, n_z * n_sp * local * cap)

    def buffer(*shape):
        return pltpu.VMEM(shape, jnp.bfloat16)

    def single(*shape):
        return pltpu.VMEM(shape, jnp.float32)

    return pl.pallas_call(
        functools.partial(layer_kernel, n_sp, n_tp, (pair // 2) ** (-0.5)),
        out_shape=jax.ShapeDtypeStruct((rows, model), jnp.bfloat16),
        in_specs=[pl.BlockSpec(memory_space=pltpu.SMEM)] + [vmem] * 8 + [hbm] * 4,
        out_specs=vmem,
        scratch_shapes=[
            buffer(heads, tiles, 2 * tile, pair),
            buffer(heads, tokens, pair),
            buffer(heads, tokens, width),
            buffer(heads, 3, rows, n_tp * width),
            buffer(n_sp - 1, heads, 2, tokens, width),
            single(heads, tiles, 2 * tile, 2 * width),
            single(heads, tiles, 2 * tile, 1),
            buffer(heads, tokens, width),
            buffer(2, rows, model),
            buffer(rows, model),
            buffer(rows, model),
            single(4, 8, rows + -rows % 128),
            buffer(*gate_weight.shape),
            buffer(*up_weight.shape),
            buffer(*down_weight.shape),
            buffer(2, rows, model),
            buffer(3, n_sp - 1, *block),
            buffer(2, n_z, n_sp, *block),
            buffer(flat, model),
            buffer(n_z, n_sp, *block),
            buffer(flat, model),
            buffer(n_z, n_sp, *block),
            buffer(3, rows, model),
            buffer(3, rows, model),
            buffer(n_sp, local, cap, model - model // 4),
            single(3, rows, model),
            dma((n_sp + 1, 2)),
            dma((n_sp - 1, heads, 2)),
            dma((heads, 3, n_tp)),
            dma((heads, 3, n_tp)),
            dma((heads,)),
            dma((heads,)),
            dma((2, 2)),
            dma((2, 2)),
            dma((n_z,)),
            dma((n_z,)),
            dma((heads * n_tp + 3,)),
            dma((n_sp, n_z)),
            dma((n_sp, n_z)),
            dma((n_sp, n_z)),
            dma((n_sp, n_z)),
            dma((n_z,)),
            dma((n_z,)),
            dma((n_sp, n_z, 3)),
            dma((n_sp, n_z, 3)),
            dma((n_z, 3)),
            dma((n_z, 3)),
            dma((n_sp,)),
            dma((n_sp,)),
            dma((n_sp,)),
            dma((n_sp,)),
            pltpu.SemaphoreType.REGULAR,
        ],
        compiler_params=pltpu.CompilerParams(
            collective_id=2, has_side_effects=True, vmem_limit_bytes=VMEM_BYTES
        ),
        name="layer",
    )(
        lambdas,
        queries,
        key_pairs,
        head_values,
        head_gain.reshape(1, -1),
        expert_ids.T,
        route_weights.T,
        residual,
        norm_gain.reshape(1, -1),
        out_weight.reshape(n_tp, heads, width, model),
        gate_weight,
        up_weight,
        down_weight,
    )


def shards(
    queries,
    key_pairs,
    head_values,
    lambdas,
    head_gain,
    out_weight,
    residual,
    norm_gain,
    expert_ids,
    route_weights,
    gate_weight,
    up_weight,
    down_weight,
):
    tokens_here, heads_here, pair_width = queries.shape
    value_width = head_values.shape[2]
    rows_here = residual.shape[0]
    sp_count = lax.axis_size("sp")
    tp_count = lax.axis_size("tp")
    z_count = tp_count // CORES
    route_count = expert_ids.shape[1]
    local_experts = gate_weight.shape[0]
    expert_count = local_experts * sp_count
    capacity = max(2, 4 * rows_here * route_count // (3 * expert_count))
    model_width = residual.shape[1]
    block_bytes = z_count * local_experts * capacity * model_width * 2
    if sp_count == PLANE and z_count == LAYERS and heads_here == HEADS_HERE and pair_width == value_width and (
        capacity % 16 == 0 and rows_here <= 128 and route_count == 2
        and (7 * sp_count - 1) * block_bytes <= 3 * VMEM_BYTES // 5
    ):
        return whole_layer(
            queries,
            key_pairs,
            head_values,
            lambdas,
            head_gain,
            expert_ids,
            route_weights,
            residual,
            norm_gain,
            out_weight,
            gate_weight,
            up_weight,
            down_weight,
            sp_count,
            tp_count,
            capacity,
        )
    flat_ids = expert_ids.reshape(-1)
    indicator = (flat_ids[:, None] == jnp.arange(expert_count, dtype=jnp.int32)[None, :]).astype(
        jnp.int32
    )
    ranking = jnp.sum(jnp.cumsum(indicator, axis=0) * indicator, axis=1) - 1
    turned = (flat_ids - lax.axis_index("sp") * local_experts) % expert_count
    near_slots = (turned * capacity + ranking).reshape(rows_here, route_count)
    slots = flat_ids * capacity + ranking
    meta = jnp.concatenate([near_slots.astype(jnp.float32), route_weights], axis=1).T
    meta = jnp.pad(meta, ((0, 8 - 2 * route_count), (0, -rows_here % 128)), constant_values=-1.0)
    updated, normed, zmeta = attend(
        queries,
        key_pairs,
        head_values,
        lambdas,
        head_gain,
        meta,
        residual,
        norm_gain,
        out_weight,
        sp_count,
        tp_count,
    )
    if capacity % 16 == 0 and rows_here <= 128 and route_count == 2 and (
        (7 * sp_count - 1) * block_bytes <= 3 * VMEM_BYTES // 5
    ):
        return experts(
            normed, zmeta, updated, gate_weight, up_weight, down_weight, sp_count, z_count, capacity
        )
    sources = jnp.arange(rows_here * route_count, dtype=jnp.int32) // route_count
    outgoing = (
        jnp.zeros((expert_count * capacity, model_width), jnp.bfloat16)
        .at[slots]
        .set(normed[sources])
    )
    arrived = lax.all_to_all(
        outgoing.reshape(sp_count, local_experts, capacity, model_width),
        "sp",
        split_axis=0,
        concat_axis=0,
        tiled=True,
    )
    piece_rows = lax.all_gather(arrived[None], "tp", axis=0, tiled=True)
    gate_part = jnp.einsum(
        "tsecd,edf->tsecf", piece_rows, gate_weight, preferred_element_type=jnp.float32
    )
    up_part = jnp.einsum(
        "tsecd,edf->tsecf", piece_rows, up_weight, preferred_element_type=jnp.float32
    )
    inner_rows = (jax.nn.silu(gate_part) * up_part).astype(jnp.bfloat16)
    partial_value = jnp.einsum(
        "tsecf,efd->tsecd", inner_rows, down_weight, preferred_element_type=jnp.float32
    )
    reduced = lax.psum_scatter(
        partial_value.astype(jnp.bfloat16), "tp", scatter_dimension=0, tiled=True
    )
    returned = lax.all_to_all(reduced[0], "sp", split_axis=0, concat_axis=0, tiled=True)
    picked = (
        returned.reshape(expert_count * capacity, model_width)[slots]
        .astype(jnp.float32)
        .reshape(rows_here, route_count, model_width)
    )
    moe_sum = jnp.sum(picked * route_weights[:, :, None], axis=1)
    return (updated.astype(jnp.float32) + moe_sum).astype(jnp.bfloat16)


def solution(mesh):
    placed = (
        P("sp", "tp", None),
        P("sp", "tp", None),
        P("sp", "tp", None),
        P("tp"),
        P(),
        P(),
        P(("sp", "tp"), None),
        P(),
        P(("sp", "tp"), None),
        P(("sp", "tp"), None),
        P("sp", None, "tp"),
        P("sp", None, "tp"),
        P("sp", "tp", None),
    )
    return jax.shard_map(
        shards, mesh=mesh, in_specs=placed, out_specs=P(("sp", "tp"), None), check_vma=False
    )
```
